32 devices in a mesh: sp: 8 (over z, y), tp: 4 (over x, core).
Axes of the slice: x: 2, y: 2, z: 4, core: 2. Of those that a mesh axis runs over, the one named last changes fastest.
Arguments:
- inputs: bfloat16 [8192, 2048], P(('sp', 'tp')), may hold values from -90 to 90
- in_gain: float32 [2048], replicated, may hold values from 0.1 to 1.9
- w_query: bfloat16 [2048, 1024], replicated, may hold values from -2 to 2
- w_key: bfloat16 [2048, 128], replicated, may hold values from -2 to 2
- w_value: bfloat16 [2048, 128], replicated, may hold values from -0.125 to 0.125
- query_gain: float32 [64], replicated, may hold values from 0 to 8, as said below
- key_gain: float32 [64], replicated, may hold values from 0 to 8, as said below
- decay_sums: float32 [8192, 16], P('sp', 'tp'), may hold values from -1173 to 0, as said below
- w_out: bfloat16 [1024, 2048], replicated, may hold values from -0.1875 to 0.1875
Outputs:
- result: bfloat16 [8192, 2048], P(('sp', 'tp'))
The draws below stay inside these ranges and needn't reach their ends.
Inputs may be any that keep to these rules, and one draw needn't show every extreme that they name: `decay_sums`: along positions, each head's entries never rise. `query_gain`: every entry is positive. `key_gain`: every entry is positive.
All inputs are finite; a program needn't handle non-finite values.
Results may differ from the reference program's by a relative error of at most 0.015.
The reference program's roundings to bfloat16 on the way count: a program that leaves them out, or rounds other values in their place, can miss the bound.
Values may be sent and summed in bfloat16 or wider, within the bound.
A program may use at most 64 MiB of HBM per device.

```python
import math
import jax
import jax.numpy as jnp
from jax import lax

D = 2048
QUERY_HEADS = 16
DH = 64
KV = 2
TOK_DEV = 1024
SEQUENCE_LENGTH = 8192


def draw_inputs(key, part):
    key_noise, key_shift = jax.random.split(jax.random.fold_in(key, 13), 2)
    noise = jax.random.truncated_normal(key_noise, -5.0, 5.0, (SEQUENCE_LENGTH, D), jnp.float32)
    shift = jax.random.truncated_normal(key_shift, -4.0, 4.0, (SEQUENCE_LENGTH // TOK_DEV, D), jnp.float32)
    shifted = noise + jnp.repeat(shift, TOK_DEV, axis=0)
    return shifted.astype(jnp.bfloat16)


def draw_w_query(key, part):
    noise = jax.random.truncated_normal(jax.random.fold_in(key, 31), -6.0, 6.0, (D, QUERY_HEADS * DH), jnp.float32) * D ** (-0.5)
    return noise.astype(jnp.bfloat16)


def draw_w_key(key, part):
    noise = jax.random.truncated_normal(jax.random.fold_in(key, 32), -6.0, 6.0, (D, KV * DH), jnp.float32) * D ** (-0.5)
    return noise.astype(jnp.bfloat16)


def draw_query_gain(key, part):
    return jax.random.uniform(jax.random.fold_in(key, 11), (DH,), jnp.float32, 0.4, 1.6)


def draw_key_gain(key, part):
    return jax.random.uniform(jax.random.fold_in(key, 12), (DH,), jnp.float32, 0.4, 1.6)


def draw_decay_sums(key, part):
    random_part_keys = jax.random.split(jax.random.fold_in(key, 14), 7)
    order = jax.random.permutation(random_part_keys[0], QUERY_HEADS)
    fast_count = QUERY_HEADS // 2
    fast = (order < fast_count)[None, :]
    slow_rate = jax.random.uniform(random_part_keys[1], (1, QUERY_HEADS), jnp.float32, 0.2, 0.6) / SEQUENCE_LENGTH
    fast_rate = jax.random.uniform(random_part_keys[2], (1, QUERY_HEADS), jnp.float32, 1.0 / 60.0, 1.0 / 25.0)
    base_offset = jnp.where(fast, fast_rate, slow_rate)
    coarse_estimate = jax.random.uniform(random_part_keys[3], (SEQUENCE_LENGTH, QUERY_HEADS), jnp.float32, 0.3, 1.7)
    block_multiple = jnp.exp(jax.random.uniform(random_part_keys[4], (SEQUENCE_LENGTH // TOK_DEV, QUERY_HEADS), jnp.float32, -math.log(2.0), math.log(2.0)))
    block_multiple = jnp.repeat(block_multiple, TOK_DEV, axis=0)
    spike_position = jax.random.randint(random_part_keys[5], (3,), 0, SEQUENCE_LENGTH)
    spike_depth = jnp.log(jax.random.uniform(random_part_keys[6], (3, QUERY_HEADS), jnp.float32, 0.5, 0.8))
    match_count = (jnp.arange(SEQUENCE_LENGTH, dtype=jnp.int32)[:, None] == spike_position[None, :]).astype(jnp.float32)
    spike_list = jnp.dot(match_count, spike_depth, precision=lax.Precision.HIGHEST)
    step_log_gates = -base_offset * coarse_estimate * block_multiple + spike_list
    return jnp.cumsum(step_log_gates, axis=0)


def gaussian(rng, shape, spread, most, kind=jnp.bfloat16):
    drawn = jax.random.normal(rng, shape, jnp.float32) * spread
    return jnp.minimum(jnp.maximum(drawn, -most), most).astype(kind)


def setup_inputs(seed: int = 0) -> dict:
    arg_keys = jax.random.split(jax.random.key(seed), 10)
    inputs = draw_inputs(jax.random.fold_in(arg_keys[9], 71), 0)
    in_gain = jnp.clip(1.0 + 0.18 * jax.random.normal(arg_keys[1], (D,), jnp.float32), 0.1, 1.9)
    w_query = draw_w_query(jax.random.fold_in(arg_keys[9], 71), 0)
    w_key = draw_w_key(jax.random.fold_in(arg_keys[9], 71), 0)
    w_value = gaussian(arg_keys[4], (D, KV * DH), D ** -0.5, 0.125)
    query_gain = draw_query_gain(jax.random.fold_in(arg_keys[9], 71), 0)
    key_gain = draw_key_gain(jax.random.fold_in(arg_keys[9], 71), 0)
    decay_sums = draw_decay_sums(jax.random.fold_in(arg_keys[9], 71), 0)
    w_out = gaussian(arg_keys[8], (QUERY_HEADS * DH, D), (QUERY_HEADS * DH) ** -0.5, 0.1875)
    return dict(inputs=inputs, in_gain=in_gain, w_query=w_query, w_key=w_key, w_value=w_value, query_gain=query_gain, key_gain=key_gain, decay_sums=decay_sums, w_out=w_out)


epsilon = 1e-06

def rms_norm(vector, gain_vec):
    return vector * lax.rsqrt(lax.optimization_barrier(jnp.mean(vector * vector, axis=-1, keepdims=True)) + epsilon) * gain_vec

def reference(inputs, in_gain, w_query, w_key, w_value, query_gain, key_gain, decay_sums, w_out):
    length = inputs.shape[0]
    normed = rms_norm(inputs.astype(jnp.float32), in_gain).astype(jnp.bfloat16)
    queries = rms_norm(jnp.dot(normed, w_query, preferred_element_type=jnp.float32).reshape(length, QUERY_HEADS, DH), query_gain).astype(jnp.bfloat16)
    keys = rms_norm(jnp.dot(normed, w_key, preferred_element_type=jnp.float32).reshape(length, KV, DH), key_gain).astype(jnp.bfloat16)
    values = jnp.dot(normed, w_value, preferred_element_type=jnp.float32).astype(jnp.bfloat16).reshape(length, KV, DH)
    group_size = QUERY_HEADS // KV
    keys_wide = jnp.repeat(keys, group_size, axis=1).astype(jnp.float32)
    values_wide = jnp.repeat(values, group_size, axis=1).astype(jnp.float32)
    block_rows = math.gcd(length, 512)
    block_count = length // block_rows
    key_pos = jnp.arange(length, dtype=jnp.int32)
    key_decay = decay_sums.T
    score_scale = DH ** (-0.5)

    def attend_block(block_index):
        offset = (block_index * block_rows).astype(jnp.int32)
        query_rows = lax.dynamic_slice_in_dim(queries, offset, block_rows, 0).astype(jnp.float32)
        query_decay = lax.dynamic_slice_in_dim(decay_sums, offset, block_rows, 0)
        scores = jnp.einsum('qhd,khd->hqk', query_rows, keys_wide) * score_scale
        scores = scores + query_decay.T[:, :, None] - key_decay[:, None, :]
        query_pos = offset + jnp.arange(block_rows, dtype=jnp.int32)
        visible = key_pos[None, :] <= query_pos[:, None]
        scores = jnp.where(visible[None], scores, -1e+30)
        peak = lax.optimization_barrier(jnp.max(scores, axis=-1, keepdims=True))
        weights_exp = jnp.where(visible[None], jnp.exp(scores - peak), 0.0)
        total = lax.optimization_barrier(jnp.sum(weights_exp, axis=-1))
        rounded = lax.optimization_barrier(weights_exp.astype(jnp.bfloat16)).astype(jnp.float32)
        mixed = jnp.einsum('hqk,khd->qhd', rounded, values_wide)
        return (mixed / total.T[:, :, None]).astype(jnp.bfloat16)
    blocks = lax.map(attend_block, jnp.arange(block_count, dtype=jnp.int32))
    attended = blocks.reshape(length, QUERY_HEADS * DH)
    return jnp.dot(attended, w_out, preferred_element_type=jnp.float32).astype(jnp.bfloat16)
```

```python
import math

import jax
import jax.numpy as jnp
from jax import lax
from jax.experimental import pallas as pl
from jax.experimental.pallas import tpu as pltpu
from jax.sharding import Mesh, PartitionSpec as P

epsilon = 1e-06
LOG2E = math.log2(math.e)
ALL = ("sp", "kv", "half")
HEADS_PER_DOT = 2
KEY_BLOCK = 512
SMALL = 60.0


def rms_norm(vector, gain_vec):
    return (
        vector * lax.rsqrt(jnp.mean(vector * vector, axis=-1, keepdims=True) + epsilon) * gain_vec
    )


def exchange_kernel(
    kv_ref, q_ref, decay_ref, kv_out, q_out, decay_out, own_sems, kv_send, kv_recv, kv_relay,
    decay_send, decay_recv, decay_relay, q_send, q_recv, *, rows, sizes
):
    sp_count, kv_heads, half_count = sizes
    sp, group, half = lax.axis_index("sp"), lax.axis_index("kv"), lax.axis_index("half")
    core, chips = half % 2, half_count // 2
    partner = (sp, group, half + 1 - 2 * core)

    def device_of(chip):
        return (chip // (kv_heads * chips), (chip // chips) % kv_heads, (chip % chips) * 2 + core)

    def block_of(place):
        return (place[0] * kv_heads + place[1]) * half_count + place[2]

    def kv_copy(source, block, send, device):
        return pltpu.make_async_remote_copy(
            src_ref=source, dst_ref=kv_out.at[pl.ds(pl.multiple_of(block * rows, rows), rows)],
            send_sem=send, recv_sem=kv_recv.at[block], device_id=device,
            device_id_type=pl.DeviceIdType.MESH,
        )

    def decay_copy(source, member, send, device):
        return pltpu.make_async_remote_copy(
            src_ref=source, dst_ref=decay_out.at[member], send_sem=send,
            recv_sem=decay_recv.at[member], device_id=device,
            device_id_type=pl.DeviceIdType.MESH,
        )

    me = block_of((sp, group, half))
    chip = (sp * kv_heads + group) * chips + half // 2
    total = sp_count * kv_heads * chips
    member = sp * half_count + half
    cluster = sp * chips + half // 2
    clusters = sp_count * chips
    started = []
    for k in range(1, total):
        place = device_of((chip + k) % total)
        started.append(kv_copy(kv_ref.at[place[1]], me, kv_send.at[k], place))
        started[-1].start()
    for k in range(1, clusters):
        other = (cluster + k) % clusters
        place = (other // chips, group, (other % chips) * 2 + core)
        started.append(decay_copy(decay_ref, member, decay_send.at[k], place))
        started[-1].start()
    q_copy = pltpu.make_async_remote_copy(
        src_ref=q_ref, dst_ref=q_out, send_sem=q_send, recv_sem=q_recv,
        device_id=(sp_count - 1 - sp, kv_heads - 1 - group, half_count - 1 - half),
        device_id_type=pl.DeviceIdType.MESH,
    )
    q_copy.start()
    started.append(kv_copy(kv_ref.at[group], me, kv_relay.at[0], partner))
    started[-1].start()
    started.append(decay_copy(decay_ref, member, decay_relay.at[0], partner))
    started[-1].start()
    own_kv = pltpu.make_async_copy(
        kv_ref.at[group], kv_out.at[pl.ds(pl.multiple_of(me * rows, rows), rows)], own_sems.at[0]
    )
    own_kv.start()
    own_decay = pltpu.make_async_copy(decay_ref, decay_out.at[member], own_sems.at[1])
    own_decay.start()
    for k in range(1, clusters):
        other = (cluster + clusters - k) % clusters
        which = (other // chips) * half_count + (other % chips) * 2 + core
        landed = decay_out.at[which]
        relay = decay_copy(landed, which, decay_relay.at[k], partner)
        relay.wait_recv()
        relay.start()
        started.append(relay)
    for k in range(1, total):
        block = block_of(device_of((chip + total - k) % total))
        landed = kv_out.at[pl.ds(pl.multiple_of(block * rows, rows), rows)]
        relay = kv_copy(landed, block, kv_relay.at[k], partner)
        relay.wait_recv()
        relay.start()
        started.append(relay)
    for k in range(clusters):
        other = (cluster + clusters - k) % clusters
        which = (other // chips) * half_count + (other % chips) * 2 + 1 - core
        decay_copy(decay_out.at[which], which, decay_relay.at[k], partner).wait_recv()
    for k in range(total):
        place = device_of((chip + total - k) % total)
        block = block_of((place[0], place[1], place[2] + 1 - 2 * core))
        landed = kv_out.at[pl.ds(pl.multiple_of(block * rows, rows), rows)]
        kv_copy(landed, block, kv_relay.at[k], partner).wait_recv()
    for copy in started:
        copy.wait_send()
    own_kv.wait()
    own_decay.wait()
    q_copy.wait()


def attend_kernel(
    place_ref, near_ref, far_ref, row_ref, decay_ref, kv_ref, out_ref, ones_ref, q_ref, peak_ref,
    acc_ref, *, rows, heads, key_block, small
):
    lane = lax.broadcasted_iota(jnp.int32, (rows, 128), 1)
    low = lane < 64
    for r, ref in enumerate((near_ref, far_ref)):
        for pair in range(heads // 2):
            both = ref[:, pair * 128 : (pair + 1) * 128].astype(jnp.float32)
            even = jnp.where(low, both, 0.0)
            odd = jnp.where(low, pltpu.roll(both, 64, 1), 0.0)
            q_ref[r, (2 * pair) * rows : (2 * pair + 1) * rows] = even.astype(jnp.bfloat16)
            q_ref[r, (2 * pair + 1) * rows : (2 * pair + 2) * rows] = odd.astype(jnp.bfloat16)

    def fill(i, carry):
        at = pl.ds(pl.multiple_of(i * key_block, key_block), key_block)
        wide = lax.broadcasted_iota(jnp.int32, (key_block, 128), 1) < 64
        ones_ref[at] = jnp.where(wide, 1.0, kv_ref[at].astype(jnp.float32)).astype(jnp.bfloat16)
        return carry

    lax.fori_loop(0, kv_ref.shape[0] // key_block, fill, 0)
    span = HEADS_PER_DOT * rows

    for r in range(2):
        first = place_ref[r]
        for head in range(heads):
            part = pl.ds(head * rows, rows)
            if small:
                peak_ref[part] = jnp.broadcast_to(row_ref[r, :, head : head + 1], (rows, 128))
            else:
                peak_ref[part] = jnp.full((rows, 128), -1e30, jnp.float32)
        acc_ref[...] = jnp.zeros_like(acc_ref)

        def step(index, masked):
            at = pl.ds(pl.multiple_of(index * key_block, key_block), key_block)
            keys = kv_ref[at]
            values = ones_ref[at]
            for start in range(0, heads, HEADS_PER_DOT):
                part = pl.ds(start * rows, span)
                before = peak_ref[part]
                scores = lax.dot_general(
                    q_ref[r, part], keys, (((1,), (1,)), ((), ())),
                    preferred_element_type=jnp.float32,
                )
                if small:
                    scores = scores + jnp.concatenate([before] * (key_block // 128), axis=1)
                scores = scores.reshape(HEADS_PER_DOT, rows, key_block)
                scores = scores - decay_ref[index, start : start + HEADS_PER_DOT][:, None, :]
                if masked:
                    row = first + lax.broadcasted_iota(jnp.int32, (rows, key_block), 0)
                    col = index * key_block + lax.broadcasted_iota(
                        jnp.int32, (rows, key_block), 1
                    )
                    scores = jnp.where((col <= row)[None], scores, -1e30)
                scores = scores.reshape(span, key_block)
                if small:
                    weights = jnp.exp2(scores).astype(jnp.bfloat16)
                    acc_ref[part] += jnp.dot(weights, values, preferred_element_type=jnp.float32)
                else:
                    after = jnp.maximum(before, jnp.max(scores, axis=1, keepdims=True))
                    weights = jnp.exp2(scores - after[:, :1]).astype(jnp.bfloat16)
                    acc_ref[part] = acc_ref[part] * jnp.exp2(before - after) + jnp.dot(
                        weights, values, preferred_element_type=jnp.float32
                    )
                    peak_ref[part] = after

        full = first // key_block

        def body(index, carry):
            step(index, False)
            return carry

        lax.fori_loop(0, full, body, 0)
        step(full, True)
        for pair in range(heads // 2):
            even = acc_ref[(2 * pair) * rows : (2 * pair + 1) * rows]
            odd = acc_ref[(2 * pair + 1) * rows : (2 * pair + 2) * rows]
            done = jnp.where(low, pltpu.roll(even, 64, 1), odd) / jnp.where(
                low, even, pltpu.roll(odd, 64, 1)
            )
            out_ref[r, :, pair * 128 : (pair + 1) * 128] = done.astype(jnp.bfloat16)


def attend(place, near, far, row_decay, decays, kv, small):
    length = kv.shape[0]
    rows, width = near.shape
    heads, key_block = decays.shape[1:]
    vmem = pl.BlockSpec(memory_space=pltpu.VMEM)
    return pl.pallas_call(
        lambda *refs: attend_kernel(
            *refs, rows=rows, heads=heads, key_block=key_block, small=small
        ),
        out_shape=jax.ShapeDtypeStruct((2, rows, width), jnp.bfloat16),
        in_specs=[pl.BlockSpec(memory_space=pltpu.SMEM)] + [vmem] * 5,
        out_specs=vmem,
        scratch_shapes=[
            pltpu.VMEM((length, 128), jnp.bfloat16),
            pltpu.VMEM((2, heads * rows, 128), jnp.bfloat16),
            pltpu.VMEM((heads * rows, 128), jnp.float32),
            pltpu.VMEM((heads * rows, 128), jnp.float32),
        ],
        compiler_params=pltpu.CompilerParams(vmem_limit_bytes=40 * 1024 * 1024),
        name="attend_small" if small else "attend_any",
    )(place, near, far, row_decay, decays, kv)


def stream_kernel(
    kv_ref, query_ref, decay_ref, out_ref, kv_all, decay_all, far_decay, far_q, q_ref, peak_ref,
    acc_ref, res_ref, kv_recv, decay_recv, x_send, own_send, round_send, far_send, far_recv,
    q_send, q_recv, back_send, back_recv, *, sizes, lines, rows, heads, key_block
):
    sp_count, kv_heads, half_count = sizes
    zs, ys = lines
    pairs = heads // 2
    width = heads * 64
    local, chunk_rows = decay_ref.shape
    blocks = chunk_rows // key_block
    s, g, j = lax.axis_index("sp"), lax.axis_index("kv"), lax.axis_index("half")
    z, y = s // ys, s % ys
    mirror = (sp_count - 1 - s, kv_heads - 1 - g, half_count - 1 - j)
    offset = (g * half_count + j) * rows
    far_offset = (mirror[1] * half_count + mirror[2]) * rows

    def block_at(s_, x_, j_):
        return (s_ * kv_heads + x_) * half_count + j_

    def rows_of(block):
        return pl.ds(pl.multiple_of(block * rows, rows), rows)

    def remote(source, target, send, recv, device):
        return pltpu.make_async_remote_copy(
            src_ref=source, dst_ref=target, send_sem=send, recv_sem=recv, device_id=device,
            device_id_type=pl.DeviceIdType.MESH,
        )

    def kv_copy(source, block, send, device):
        return remote(source, kv_all.at[rows_of(block)], send, kv_recv.at[block], device)

    def decay_copy(source, member, send, device):
        return remote(source, decay_all.at[member], send, decay_recv.at[member], device)

    here = (s, g, j)

    def package(s_, j_, base, device, sems):
        copies = []
        for x_ in range(kv_heads):
            block = block_at(s_, x_, j_)
            copies.append(
                kv_copy(kv_all.at[rows_of(block)], block, sems.at[base + x_], device)
            )
        member = s_ * half_count + j_
        copies.append(
            decay_copy(decay_all.at[member], member, sems.at[base + kv_heads], device)
        )
        return copies

    each = kv_heads + 1
    per = 1 + (ys - 1) + (half_count - 1) + (ys - 1) * (half_count - 1)

    def arrived(s_, j_):
        for copy in package(s_, j_, 0, here, own_send):
            copy.wait_recv()

    def start_all(copies):
        for copy in copies:
            copy.start()

    def drain_all(copies):
        for copy in copies:
            copy.wait_send()

    def inside(z_):
        return (z_ >= 0) & (z_ < zs)

    def round_of(k, go):
        act = start_all if go else drain_all
        for d, way in enumerate((1, -1)):
            base = ((k - 1) * 2 + d) * per * each

            @pl.when(inside(z - way * k))
            def _():
                s_ = (z - way * k) * ys + y
                if go:
                    arrived(s_, j)

                @pl.when(inside(z + way))
                def _():
                    act(package(s_, j, base, ((z + way) * ys + y, g, j), round_send))

                slot = 1
                for n in range(1, ys):
                    to = (z * ys + (y + n) % ys, g, j)
                    act(package(s_, j, base + slot * each, to, round_send))
                    slot += 1
                for n in range(1, half_count):
                    to = (s, g, (j + n) % half_count)
                    act(package(s_, j, base + slot * each, to, round_send))
                    slot += 1

            reach = inside(z - way * (k - 1))
            if way < 0:
                reach = reach & (k != 1)

            @pl.when(reach)
            def _():
                slot = ys + half_count - 1
                for m in range(1, ys):
                    s_ = (z - way * (k - 1)) * ys + (y + m) % ys
                    if go:
                        arrived(s_, j)
                    for n in range(1, half_count):
                        to = (s, g, (j + n) % half_count)
                        act(package(s_, j, base + slot * each, to, round_send))
                        slot += 1

    def lanes_of(k):
        for way in (1, -1):

            @pl.when(inside(z - way * k))
            def _():
                for n in range(1, half_count):
                    arrived((z - way * k) * ys + y, (j + n) % half_count)

            reach = inside(z - way * (k - 1))
            if way < 0:
                reach = reach & (k != 1)

            @pl.when(reach)
            def _():
                for m in range(1, ys):
                    for n in range(1, half_count):
                        arrived(
                            (z - way * (k - 1)) * ys + (y + m) % ys, (j + n) % half_count
                        )

    def q_lanes(group, pair):
        return pl.ds(pl.multiple_of(group * width + pair * 128, 128), 128)

    own_block = block_at(s, g, j)
    other_block = block_at(s, 1 - g, j)
    member = s * half_count + j
    x_copy = kv_copy(kv_ref.at[1 - g], own_block, x_send, (s, 1 - g, j))
    x_copy.start()

    def own_to(act):
        slot = 0
        targets = []
        for n in range(1, half_count):
            targets.append((None, (s, g, (j + n) % half_count)))
        for way in (1, -1):
            targets.append((inside(z + way), ((z + way) * ys + y, g, j)))
        for n in range(1, ys):
            targets.append((None, (z * ys + (y + n) % ys, g, j)))
        for condition, device in targets:
            base = slot * each

            def run():
                act(base, device)

            if condition is None:
                run()
            else:
                pl.when(condition)(run)
            slot += 1

    def own_first(base, device):
        kv_copy(kv_ref.at[g], own_block, own_send.at[base], device).start()
        decay_copy(decay_ref, member, own_send.at[base + 1], device).start()

    def own_second(base, device):
        landed = kv_all.at[rows_of(other_block)]
        kv_copy(landed, other_block, own_send.at[base + 2], device).start()

    def own_drain(base, device):
        kv_copy(kv_ref.at[g], own_block, own_send.at[base], device).wait_send()
        decay_copy(decay_ref, member, own_send.at[base + 1], device).wait_send()
        landed = kv_all.at[rows_of(other_block)]
        kv_copy(landed, other_block, own_send.at[base + 2], device).wait_send()

    own_to(own_first)

    def far_copy(n):
        source = decay_ref.at[
            :, pl.ds(pl.multiple_of(((1 - g) * half_count + half_count - 1 - n) * rows, rows), rows)
        ]
        return remote(
            source, far_decay.at[j], far_send.at[n], far_recv.at[j], (mirror[0], g, n)
        )

    for n in range(half_count):
        far_copy(n).start()

    def q_copy(pair):
        return remote(
            query_ref.at[:, q_lanes(1 - g, pair)], far_q.at[pair], q_send.at[pair],
            q_recv.at[pair], mirror,
        )

    q_copy(0).start()

    kv_all[rows_of(own_block)] = kv_ref[g]
    decay_all[member] = decay_ref[...]
    acc_ref[...] = jnp.zeros_like(acc_ref)
    low = lax.broadcasted_iota(jnp.int32, (rows, 128), 1) < 64

    def unpack(r, pair, both):
        both = both.astype(jnp.float32)
        even = jnp.where(low, both, 0.0)
        odd = jnp.where(low, pltpu.roll(both, 64, 1), 0.0)
        q_ref[r, (2 * pair) * rows : (2 * pair + 1) * rows] = even.astype(jnp.bfloat16)
        q_ref[r, (2 * pair + 1) * rows : (2 * pair + 2) * rows] = odd.astype(jnp.bfloat16)

    def shifts(r, pair, values):
        turned = values.T
        for n in range(2):
            part = pl.ds((2 * pair + n) * rows, rows)
            peak_ref[r, part] = jnp.broadcast_to(turned[:, n : n + 1], (rows, 128))

    def eight(two):
        return jnp.concatenate([two, two, two, two], axis=0)

    for pair in range(pairs):
        unpack(0, pair, query_ref[:, q_lanes(g, pair)])

    kv_copy(kv_ref.at[g], other_block, x_send, here).wait_recv()
    own_to(own_second)
    for pair in range(1, pairs):
        q_copy(pair).start()
    for n in range(1, half_count):
        arrived(s, (j + n) % half_count)

    for pair in range(pairs):
        first = (2 * pair) % local
        span = pl.ds(pl.multiple_of(offset, rows), rows)
        two = decay_all[s * half_count + (2 * pair) // local, first : first + 2, span]
        shifts(0, pair, eight(two))

    def pair_step(r, chunk, block, pair, masked, start):
        at = pl.ds(pl.multiple_of((chunk * blocks + block) * key_block, key_block), key_block)
        keys = kv_all[at]
        upper = lax.broadcasted_iota(jnp.int32, (key_block, 128), 1) >= 64
        pick = jnp.where(upper, 1.0, 0.0).astype(jnp.bfloat16)
        ones = jnp.where(upper, 0.0, 1.0).astype(jnp.bfloat16)
        values = keys * pick + ones
        part = pl.ds(pair * 2 * rows, 2 * rows)
        if not isinstance(pair, int):
            part = pl.ds(pl.multiple_of(pair * 2 * rows, 2 * rows), 2 * rows)
        scores = lax.dot_general(
            q_ref[r, part], keys, (((1,), (1,)), ((), ())), preferred_element_type=jnp.float32
        )
        before = peak_ref[r, part]
        scores = scores + jnp.concatenate([before] * (key_block // 128), axis=1)
        first = (2 * pair) % local
        lanes = pl.ds(pl.multiple_of(block * key_block, key_block), key_block)
        decays = decay_all[chunk * half_count + (2 * pair) // local, pl.ds(first, 2), lanes]
        scores = scores.reshape(2, rows, key_block) - decays[:, None, :]
        if masked:
            row = start + lax.broadcasted_iota(jnp.int32, (rows, key_block), 0)
            col = block * key_block + lax.broadcasted_iota(jnp.int32, (rows, key_block), 1)
            scores = jnp.where((col <= row)[None], scores, -1e30)
        weights = jnp.exp2(scores.reshape(2 * rows, key_block)).astype(jnp.bfloat16)
        acc_ref[r, part] += jnp.dot(weights, values, preferred_element_type=jnp.float32)

    def diagonal(r, chunk, some, start):
        full = start // key_block

        def whole(block, carry):
            for pair in some:
                pair_step(r, chunk, block, pair, False, start)
            return carry

        lax.fori_loop(0, full, whole, 0)
        for pair in some:
            pair_step(r, chunk, full, pair, True, start)

    def finished(r, pair):
        at = 2 * pair * rows
        even = acc_ref[r, pl.ds(at, rows)]
        odd = acc_ref[r, pl.ds(at + rows, rows)]
        done = jnp.where(low, pltpu.roll(even, 64, 1), odd) / jnp.where(
            low, even, pltpu.roll(odd, 64, 1)
        )
        return done.astype(jnp.bfloat16)

    def prepare(some):
        for pair in some:
            remote(
                query_ref.at[:, q_lanes(1 - g, pair)], far_q.at[pair], q_send.at[pair],
                q_recv.at[pair], here,
            ).wait_recv()
            unpack(1, pair, far_q[pair])
            first = (2 * pair) % local
            two = far_decay[(2 * pair) // local, first : first + 2]
            shifts(1, pair, eight(two))

    def far_ready():
        for n in range(half_count):
            remote(
                decay_ref.at[:, pl.ds(0, rows)], far_decay.at[n], far_send.at[n],
                far_recv.at[n], here,
            ).wait_recv()

    halves = (tuple(range(pairs // 2)), tuple(range(pairs // 2, pairs)))
    diagonal(0, s, halves[0], offset)
    round_of(1, True)
    diagonal(0, s, halves[1], offset)

    def item(k, carry):
        lanes_of(k)
        far = k > s
        r = jnp.where(far, 1, 0)
        back = jnp.where(y == 0, jnp.where(k == 1, ys, jnp.where(k == ys, 1, k)), k)
        chunk = jnp.where(far, k - s - 1, s - back)

        @pl.when(k == s + 1)
        def _():
            far_ready()
            prepare(halves[0])

        for block in range(blocks):
            for pair in halves[0]:
                pair_step(r, chunk, block, pair, False, 0)

        @pl.when(k < zs)
        def _():
            round_of(k + 1, True)

        @pl.when(k == s + 1)
        def _():
            prepare(halves[1])

        for block in range(blocks):
            for pair in halves[1]:
                pair_step(r, chunk, block, pair, False, 0)
        return carry

    lax.fori_loop(1, zs + 1, item, 0)

    @pl.when(s >= zs)
    def _():
        far_ready()
        prepare(range(pairs))

    far_chunk = sp_count - 1 - s

    def back_copy(pair, device):
        return remote(
            res_ref.at[pair], out_ref.at[:, q_lanes(g, pair)], back_send.at[pair],
            back_recv.at[pair], device,
        )

    for pair in range(pairs):

        def far_item(chunk, carry):
            for block in range(blocks):
                pair_step(1, chunk, block, pair, False, 0)
            return carry

        lax.fori_loop(jnp.maximum(zs - s, 0), far_chunk, far_item, 0)
        diagonal(1, far_chunk, (pair,), far_offset)
        res_ref[pair] = finished(1, pair)
        back_copy(pair, mirror).start()

    def last_item(index, carry):
        for pair in range(pairs):
            pair_step(0, index // blocks, index % blocks, pair, False, 0)
        return carry

    lax.fori_loop(0, jnp.maximum(s - zs, 0) * blocks, last_item, 0)
    for pair in range(pairs):
        out_ref[:, q_lanes(g, pair)] = finished(0, pair)

    x_copy.wait_send()
    own_to(own_drain)

    def drain(k, carry):
        round_of(k, False)
        return carry

    lax.fori_loop(1, zs + 1, drain, 0)
    for n in range(half_count):
        far_copy(n).wait_send()
    for pair in range(pairs):
        q_copy(pair).wait_send()
        back_copy(pair, mirror).wait_send()
        remote(
            res_ref.at[pair], out_ref.at[:, q_lanes(1 - g, pair)], back_send.at[pair],
            back_recv.at[pair], here,
        ).wait_recv()


def lines_of(sp_count):
    ys = 1 << ((sp_count.bit_length() - 1) // 2)
    return sp_count // ys, ys


def stream(queries, kv_blocks, decays, sizes):
    sp_count, kv_heads, half_count = sizes
    rows = queries.shape[0]
    heads = queries.shape[1] // 64 // kv_heads
    local, chunk_rows = decays.shape
    zs, ys = lines_of(sp_count)
    pairs = heads // 2
    count = sp_count * kv_heads * half_count
    members = sp_count * half_count
    per = 1 + (ys - 1) + (half_count - 1) + (ys - 1) * (half_count - 1)
    each = kv_heads + 1
    vmem = pl.BlockSpec(memory_space=pltpu.VMEM)
    dma = pltpu.SemaphoreType.DMA
    return pl.pallas_call(
        lambda *refs: stream_kernel(
            *refs, sizes=sizes, lines=(zs, ys), rows=rows, heads=heads,
            key_block=math.gcd(chunk_rows, KEY_BLOCK),
        ),
        out_shape=jax.ShapeDtypeStruct(queries.shape, jnp.bfloat16),
        in_specs=[vmem] * 3,
        out_specs=vmem,
        scratch_shapes=[
            pltpu.VMEM((rows * count, 128), jnp.bfloat16),
            pltpu.VMEM((members, local, chunk_rows), jnp.float32),
            pltpu.VMEM((half_count, local, rows), jnp.float32),
            pltpu.VMEM((pairs, rows, 128), jnp.bfloat16),
            pltpu.VMEM((2, heads * rows, 128), jnp.bfloat16),
            pltpu.VMEM((2, heads * rows, 128), jnp.float32),
            pltpu.VMEM((2, heads * rows, 128), jnp.float32),
            pltpu.VMEM((pairs, rows, 128), jnp.bfloat16),
            dma((count,)), dma((members,)), dma, dma(((ys + half_count) * each,)),
            dma((zs * 2 * per * each,)), dma((half_count,)), dma((half_count,)),
            dma((pairs,)), dma((pairs,)), dma((pairs,)), dma((pairs,)),
        ],
        compiler_params=pltpu.CompilerParams(
            has_side_effects=True, vmem_limit_bytes=44 * 1024 * 1024
        ),
        name="stream",
    )(kv_blocks, queries, decays)


def any_scores(queries, kv_blocks, decays, sizes):
    sp_count, kv_heads, half_count = sizes
    group = lax.axis_index("kv")
    me = (lax.axis_index("sp") * kv_heads + group) * half_count + lax.axis_index("half")
    count = sp_count * kv_heads * half_count
    mirror = [(i, count - 1 - i) for i in range(count)]
    rows = queries.shape[0]
    length = rows * count
    heads = queries.shape[1] // 64 // kv_heads
    width = heads * 64
    members = sp_count * half_count
    key_block = math.gcd(length, KEY_BLOCK)

    def choose(a, b):
        return jnp.where(group == 0, a, b)

    decay_rows = decays.reshape(-1, 128)
    own_q = choose(queries[:, :width], queries[:, width:])
    sent_q = choose(queries[:, width:], queries[:, :width])
    vmem = pl.BlockSpec(memory_space=pltpu.VMEM)
    chips = count // 2
    dma = pltpu.SemaphoreType.DMA
    kv, far_q, decay_all = pl.pallas_call(
        lambda *refs: exchange_kernel(*refs, rows=rows, sizes=sizes),
        out_shape=(
            jax.ShapeDtypeStruct((length, 128), jnp.bfloat16),
            jax.ShapeDtypeStruct((rows, width), jnp.bfloat16),
            jax.ShapeDtypeStruct((members, *decay_rows.shape), jnp.float32),
        ),
        in_specs=[vmem] * 3,
        out_specs=(vmem,) * 3,
        scratch_shapes=[
            dma((2,)), dma((chips,)), dma((count,)), dma((chips,)), dma((members // 2,)),
            dma((members,)), dma((members // 2,)), dma, dma,
        ],
        compiler_params=pltpu.CompilerParams(has_side_effects=True),
        name="exchange",
    )(kv_blocks, sent_q, decay_rows)
    decay_all = decay_all.reshape(sp_count, heads, -1, key_block)
    decay_all = decay_all.transpose(0, 2, 1, 3).reshape(length // key_block, heads, key_block)
    firsts = (me * rows, (count - 1 - me) * rows)
    place = jnp.stack(firsts).astype(jnp.int32)
    row_decay = jnp.stack(
        [
            lax.dynamic_slice(
                decay_all, (first // key_block, 0, first % key_block), (1, heads, rows)
            )[0].T
            for first in firsts
        ]
    )
    attended = attend(place, own_q, far_q, row_decay, decay_all, kv, False)
    back = lax.ppermute(attended[1], ALL, mirror)
    return choose(
        jnp.concatenate([attended[0], back], axis=1), jnp.concatenate([back, attended[0]], axis=1)
    )


def per_device(inputs, in_gain, w_query, w_key, w_value, query_gain, key_gain, decay_sums, w_out):
    kv_heads = lax.axis_size("kv")
    sizes = (lax.axis_size("sp"), kv_heads, lax.axis_size("half"))
    head_size = query_gain.shape[0]
    rows = inputs.shape[0]
    all_heads = w_query.shape[1] // head_size

    normed = rms_norm(inputs.astype(jnp.float32), in_gain).astype(jnp.bfloat16)
    keys = rms_norm(
        jnp.dot(normed, w_key, preferred_element_type=jnp.float32).reshape(
            rows, kv_heads, head_size
        ),
        key_gain,
    ).astype(jnp.bfloat16)
    values = (
        jnp.dot(normed, w_value, preferred_element_type=jnp.float32)
        .astype(jnp.bfloat16)
        .reshape(rows, kv_heads, head_size)
    )
    pairs = jnp.concatenate([keys, values], axis=2)
    kv_blocks = pairs.transpose(1, 0, 2)
    decays = decay_sums.T * LOG2E

    queries = rms_norm(
        jnp.dot(normed, w_query, preferred_element_type=jnp.float32).reshape(
            rows, all_heads, head_size
        ),
        query_gain * (LOG2E * head_size ** (-0.5)),
    ).astype(jnp.bfloat16).reshape(rows, all_heads * head_size)
    bound = head_size**0.5 * LOG2E * jnp.max(query_gain) * jnp.max(key_gain)
    whole = lax.cond(
        bound <= SMALL,
        lambda *given: stream(*given, sizes),
        lambda *given: any_scores(*given, sizes),
        queries, kv_blocks, decays,
    )
    return jnp.dot(whole, w_out, preferred_element_type=jnp.float32).astype(jnp.bfloat16)


def solution(mesh):
    sp_count, tp_count = mesh.devices.shape
    split = Mesh(mesh.devices.reshape(sp_count, 2, tp_count // 2), ALL)
    placed = (P(ALL, None), P(), P(), P(), P(), P(), P(), P("sp", ("kv", "half")), P())
    return jax.shard_map(
        per_device, mesh=split, in_specs=placed, out_specs=P(ALL, None), check_vma=False
    )
```

```python
import math

import jax
import jax.numpy as jnp
from jax import lax
from jax.experimental import pallas as pl
from jax.experimental.pallas import tpu as pltpu
from jax.sharding import Mesh, PartitionSpec as P

epsilon = 1e-06
LOG2E = math.log2(math.e)
ALL = ("sp", "kv", "half")
HEADS_PER_DOT = 2
KEY_BLOCK = 512
SMALL = 60.0


def rms_norm(vector, gain_vec):
    return (
        vector * lax.rsqrt(jnp.mean(vector * vector, axis=-1, keepdims=True) + epsilon) * gain_vec
    )


def exchange_kernel(
    kv_ref, q_ref, decay_ref, kv_out, q_out, decay_out, own_sems, kv_send, kv_recv, kv_relay,
    decay_send, decay_recv, decay_relay, q_send, q_recv, *, rows, sizes
):
    sp_count, kv_heads, half_count = sizes
    sp, group, half = lax.axis_index("sp"), lax.axis_index("kv"), lax.axis_index("half")
    core, chips = half % 2, half_count // 2
    partner = (sp, group, half + 1 - 2 * core)

    def device_of(chip):
        return (chip // (kv_heads * chips), (chip // chips) % kv_heads, (chip % chips) * 2 + core)

    def block_of(place):
        return (place[0] * kv_heads + place[1]) * half_count + place[2]

    def kv_copy(source, block, send, device):
        return pltpu.make_async_remote_copy(
            src_ref=source, dst_ref=kv_out.at[pl.ds(pl.multiple_of(block * rows, rows), rows)],
            send_sem=send, recv_sem=kv_recv.at[block], device_id=device,
            device_id_type=pl.DeviceIdType.MESH,
        )

    def decay_copy(source, member, send, device):
        return pltpu.make_async_remote_copy(
            src_ref=source, dst_ref=decay_out.at[member], send_sem=send,
            recv_sem=decay_recv.at[member], device_id=device,
            device_id_type=pl.DeviceIdType.MESH,
        )

    me = block_of((sp, group, half))
    chip = (sp * kv_heads + group) * chips + half // 2
    total = sp_count * kv_heads * chips
    member = sp * half_count + half
    cluster = sp * chips + half // 2
    clusters = sp_count * chips
    started = []
    for k in range(1, total):
        place = device_of((chip + k) % total)
        started.append(kv_copy(kv_ref.at[place[1]], me, kv_send.at[k], place))
        started[-1].start()
    for k in range(1, clusters):
        other = (cluster + k) % clusters
        place = (other // chips, group, (other % chips) * 2 + core)
        started.append(decay_copy(decay_ref, member, decay_send.at[k], place))
        started[-1].start()
    q_copy = pltpu.make_async_remote_copy(
        src_ref=q_ref, dst_ref=q_out, send_sem=q_send, recv_sem=q_recv,
        device_id=(sp_count - 1 - sp, kv_heads - 1 - group, half_count - 1 - half),
        device_id_type=pl.DeviceIdType.MESH,
    )
    q_copy.start()
    started.append(kv_copy(kv_ref.at[group], me, kv_relay.at[0], partner))
    started[-1].start()
    started.append(decay_copy(decay_ref, member, decay_relay.at[0], partner))
    started[-1].start()
    own_kv = pltpu.make_async_copy(
        kv_ref.at[group], kv_out.at[pl.ds(pl.multiple_of(me * rows, rows), rows)], own_sems.at[0]
    )
    own_kv.start()
    own_decay = pltpu.make_async_copy(decay_ref, decay_out.at[member], own_sems.at[1])
    own_decay.start()
    for k in range(1, clusters):
        other = (cluster + clusters - k) % clusters
        which = (other // chips) * half_count + (other % chips) * 2 + core
        landed = decay_out.at[which]
        relay = decay_copy(landed, which, decay_relay.at[k], partner)
        relay.wait_recv()
        relay.start()
        started.append(relay)
    for k in range(1, total):
        block = block_of(device_of((chip + total - k) % total))
        landed = kv_out.at[pl.ds(pl.multiple_of(block * rows, rows), rows)]
        relay = kv_copy(landed, block, kv_relay.at[k], partner)
        relay.wait_recv()
        relay.start()
        started.append(relay)
    for k in range(clusters):
        other = (cluster + clusters - k) % clusters
        which = (other // chips) * half_count + (other % chips) * 2 + 1 - core
        decay_copy(decay_out.at[which], which, decay_relay.at[k], partner).wait_recv()
    for k in range(total):
        place = device_of((chip + total - k) % total)
        block = block_of((place[0], place[1], place[2] + 1 - 2 * core))
        landed = kv_out.at[pl.ds(pl.multiple_of(block * rows, rows), rows)]
        kv_copy(landed, block, kv_relay.at[k], partner).wait_recv()
    for copy in started:
        copy.wait_send()
    own_kv.wait()
    own_decay.wait()
    q_copy.wait()


def attend_kernel(
    place_ref, near_ref, far_ref, row_ref, decay_ref, kv_ref, out_ref, ones_ref, q_ref, peak_ref,
    acc_ref, *, rows, heads, key_block, small
):
    lane = lax.broadcasted_iota(jnp.int32, (rows, 128), 1)
    low = lane < 64
    for r, ref in enumerate((near_ref, far_ref)):
        for pair in range(heads // 2):
            both = ref[:, pair * 128 : (pair + 1) * 128].astype(jnp.float32)
            even = jnp.where(low, both, 0.0)
            odd = jnp.where(low, pltpu.roll(both, 64, 1), 0.0)
            q_ref[r, (2 * pair) * rows : (2 * pair + 1) * rows] = even.astype(jnp.bfloat16)
            q_ref[r, (2 * pair + 1) * rows : (2 * pair + 2) * rows] = odd.astype(jnp.bfloat16)

    def fill(i, carry):
        at = pl.ds(pl.multiple_of(i * key_block, key_block), key_block)
        wide = lax.broadcasted_iota(jnp.int32, (key_block, 128), 1) < 64
        ones_ref[at] = jnp.where(wide, 1.0, kv_ref[at].astype(jnp.float32)).astype(jnp.bfloat16)
        return carry

    lax.fori_loop(0, kv_ref.shape[0] // key_block, fill, 0)
    span = HEADS_PER_DOT * rows

    for r in range(2):
        first = place_ref[r]
        for head in range(heads):
            part = pl.ds(head * rows, rows)
            if small:
                peak_ref[part] = jnp.broadcast_to(row_ref[r, :, head : head + 1], (rows, 128))
            else:
                peak_ref[part] = jnp.full((rows, 128), -1e30, jnp.float32)
        acc_ref[...] = jnp.zeros_like(acc_ref)

        def step(index, masked):
            at = pl.ds(pl.multiple_of(index * key_block, key_block), key_block)
            keys = kv_ref[at]
            values = ones_ref[at]
            for start in range(0, heads, HEADS_PER_DOT):
                part = pl.ds(start * rows, span)
                before = peak_ref[part]
                scores = lax.dot_general(
                    q_ref[r, part], keys, (((1,), (1,)), ((), ())),
                    preferred_element_type=jnp.float32,
                )
                if small:
                    scores = scores + jnp.concatenate([before] * (key_block // 128), axis=1)
                scores = scores.reshape(HEADS_PER_DOT, rows, key_block)
                scores = scores - decay_ref[index, start : start + HEADS_PER_DOT][:, None, :]
                if masked:
                    row = first + lax.broadcasted_iota(jnp.int32, (rows, key_block), 0)
                    col = index * key_block + lax.broadcasted_iota(
                        jnp.int32, (rows, key_block), 1
                    )
                    scores = jnp.where((col <= row)[None], scores, -1e30)
                scores = scores.reshape(span, key_block)
                if small:
                    weights = jnp.exp2(scores).astype(jnp.bfloat16)
                    acc_ref[part] += jnp.dot(weights, values, preferred_element_type=jnp.float32)
                else:
                    after = jnp.maximum(before, jnp.max(scores, axis=1, keepdims=True))
                    weights = jnp.exp2(scores - after[:, :1]).astype(jnp.bfloat16)
                    acc_ref[part] = acc_ref[part] * jnp.exp2(before - after) + jnp.dot(
                        weights, values, preferred_element_type=jnp.float32
                    )
                    peak_ref[part] = after

        full = first // key_block

        def body(index, carry):
            step(index, False)
            return carry

        lax.fori_loop(0, full, body, 0)
        step(full, True)
        for pair in range(heads // 2):
            even = acc_ref[(2 * pair) * rows : (2 * pair + 1) * rows]
            odd = acc_ref[(2 * pair + 1) * rows : (2 * pair + 2) * rows]
            done = jnp.where(low, pltpu.roll(even, 64, 1), odd) / jnp.where(
                low, even, pltpu.roll(odd, 64, 1)
            )
            out_ref[r, :, pair * 128 : (pair + 1) * 128] = done.astype(jnp.bfloat16)


def attend(place, near, far, row_decay, decays, kv, small):
    length = kv.shape[0]
    rows, width = near.shape
    heads, key_block = decays.shape[1:]
    vmem = pl.BlockSpec(memory_space=pltpu.VMEM)
    return pl.pallas_call(
        lambda *refs: attend_kernel(
            *refs, rows=rows, heads=heads, key_block=key_block, small=small
        ),
        out_shape=jax.ShapeDtypeStruct((2, rows, width), jnp.bfloat16),
        in_specs=[pl.BlockSpec(memory_space=pltpu.SMEM)] + [vmem] * 5,
        out_specs=vmem,
        scratch_shapes=[
            pltpu.VMEM((length, 128), jnp.bfloat16),
            pltpu.VMEM((2, heads * rows, 128), jnp.bfloat16),
            pltpu.VMEM((heads * rows, 128), jnp.float32),
            pltpu.VMEM((heads * rows, 128), jnp.float32),
        ],
        compiler_params=pltpu.CompilerParams(vmem_limit_bytes=40 * 1024 * 1024),
        name="attend_small" if small else "attend_any",
    )(place, near, far, row_decay, decays, kv)


def stream_kernel(
    kvt_ref, query_ref, decay_ref, out_ref, kvt_all, decay_all, far_decay, in_q, qt_ref, acc_ref,
    kp_all, vt_all, res_ref, kv_recv, decay_recv, x_send, own_send, round_send, late_send,
    far_send, far_recv, q_send, q_recv, back_send, back_recv, *, sizes, lines, rows, heads
):
    sp_count, kv_heads, half_count = sizes
    zs, ys = lines
    zh = zs // 2
    upper = sp_count // 2
    pairs = heads // 2
    units = pairs * kv_heads
    width = heads * 64
    span = 2 * rows
    local, chunk_rows = decay_ref.shape
    s, g, j = lax.axis_index("sp"), lax.axis_index("kv"), lax.axis_index("half")
    z, y = s // ys, s % ys
    partner_x = 1 - g
    s_far = sp_count - 1 - s
    is_high = s >= upper

    def share(s_):
        return (2 * units * (2 * s_ + 1 - sp_count) + 2 * s_ + 1) // (2 * (2 * s_ + 1))

    given = jnp.where(is_high, share(jnp.maximum(s, upper)), 0)
    taken = jnp.where(is_high, 0, share(jnp.maximum(s_far, upper)))

    def kept_from(x_):
        return (jnp.maximum(given - x_, 0) + kv_heads - 1) // kv_heads

    def block_at(s_, x_, j_):
        return (s_ * kv_heads + x_) * half_count + j_

    def remote(source, target, send, recv, device):
        return pltpu.make_async_remote_copy(
            src_ref=source, dst_ref=target, send_sem=send, recv_sem=recv, device_id=device,
            device_id_type=pl.DeviceIdType.MESH,
        )

    def kv_copy(source, block, send, device):
        return remote(source, kvt_all.at[block], send, kv_recv.at[block], device)

    def decay_copy(source, member, send, device):
        return remote(source, decay_all.at[member], send, decay_recv.at[member], device)

    here = (s, g, j)
    each = kv_heads + 1

    def package(s_, j_, base, device, sems):
        copies = []
        for x_ in range(kv_heads):
            block = block_at(s_, x_, j_)
            copies.append(kv_copy(kvt_all.at[block], block, sems.at[base + x_], device))
        member = s_ * half_count + j_
        copies.append(
            decay_copy(decay_all.at[member], member, sems.at[base + kv_heads], device)
        )
        return copies

    def arrived(s_, j_):
        for copy in package(s_, j_, 0, here, own_send):
            copy.wait_recv()

    def start_all(copies):
        for copy in copies:
            copy.start()

    def drain_all(copies):
        for copy in copies:
            copy.wait_send()

    def inside(z_):
        return (z_ >= 0) & (z_ < zs)

    def others(s_, base, sems, act, z_=None):
        slot = 0
        if z_ is None:
            for n in range(1, ys):
                to = (z * ys + (y + n) % ys, g, j)
                act(package(s_, j, base + slot * each, to, sems))
                slot += 1
        for n in range(1, half_count):
            to = (s, g, (j + n) % half_count)
            act(package(s_, j, base + slot * each, to, sems))
            slot += 1

    per = 1 + (ys - 1) + (half_count - 1) + (ys - 1) * (half_count - 1)

    def near_from(z_, way):
        return inside(z_) if way > 0 else inside(z_) & (z_ < zh)

    def round_of(k, go):
        act = start_all if go else drain_all
        for d, way in enumerate((1, -1)):
            base = ((k - 1) * 2 + d) * per * each

            @pl.when(near_from(z - way * k, way))
            def _():
                s_ = (z - way * k) * ys + y
                if go:
                    arrived(s_, j)

                @pl.when(inside(z + way))
                def _():
                    act(package(s_, j, base, ((z + way) * ys + y, g, j), round_send))

                others(s_, base + each, round_send, act)

            reach = near_from(z - way * (k - 1), way)
            if way < 0:
                reach = reach & (k != 1)

            @pl.when(reach)
            def _():
                for m in range(1, ys):
                    s_ = (z - way * (k - 1)) * ys + (y + m) % ys
                    if go:
                        arrived(s_, j)
                    slot = ys + half_count - 1 + (m - 1) * (half_count - 1)
                    others(s_, base + slot * each, round_send, act, z)

    def late(zo, go):
        act = start_all if go else drain_all
        base = (zo - zh) * per * each

        @pl.when((zo > z) & (zo < zs))
        def _():
            s_ = zo * ys + y
            if go:
                arrived(s_, j)

            @pl.when(z > 0)
            def _():
                act(package(s_, j, base, ((z - 1) * ys + y, g, j), late_send))

            @pl.when(zo <= zs - 1 - z)
            def _():
                others(s_, base + each, late_send, act)

    def late_across(zo, go):
        act = start_all if go else drain_all
        base = (zo - zh) * per * each

        @pl.when((zo > z) & (zo <= zs - 1 - z))
        def _():
            for m in range(1, ys):
                s_ = zo * ys + (y + m) % ys
                if go:
                    arrived(s_, j)
                slot = ys + half_count - 1 + (m - 1) * (half_count - 1)
                others(s_, base + slot * each, late_send, act, z)

    def build(s_):
        for x_ in range(kv_heads):
            for j_ in range(half_count):
                block = block_at(s_, x_, j_)
                place = (x_ * half_count + j_) * rows
                decays = jnp.concatenate(
                    [
                        decay_all[s_ * half_count + n, :, pl.ds(place, rows)]
                        for n in range(half_count)
                    ],
                    axis=0,
                )
                decays = -decays
                high = decays.astype(jnp.bfloat16).astype(jnp.float32)
                rest = decays - high
                middle = rest.astype(jnp.bfloat16).astype(jnp.float32)
                parts = jnp.concatenate(
                    [high, middle, rest - middle, jnp.ones((8, rows), jnp.float32)], axis=0
                ).astype(jnp.bfloat16)
                wide = jnp.concatenate(
                    [kvt_all[block, 0:64], parts, jnp.zeros((32, rows), jnp.bfloat16)], axis=0
                )
                kp_all[s_, pl.ds(place, rows)] = wide.T
                vt_all[s_, 0:64, pl.ds(place, rows)] = kvt_all[block, 64:128]

    def build_if(s_):
        @pl.when(s_ <= jnp.where(is_high, s, s_far))
        def _():
            build(s_)

    def lanes_of(k):
        for way in (1, -1):

            @pl.when(near_from(z - way * k, way))
            def _():
                s_ = (z - way * k) * ys + y
                for n in range(1, half_count):
                    arrived(s_, (j + n) % half_count)
                build_if(s_)

            reach = near_from(z - way * (k - 1), way)
            if way < 0:
                reach = reach & (k != 1)

            @pl.when(reach)
            def _():
                for m in range(1, ys):
                    s_ = (z - way * (k - 1)) * ys + (y + m) % ys
                    for n in range(1, half_count):
                        arrived(s_, (j + n) % half_count)
                    build_if(s_)

    def late_lanes(zo):
        @pl.when((zo > z) & (zo <= zs - 1 - z))
        def _():
            for m in range(ys):
                s_ = zo * ys + (y + m) % ys
                for n in range(1, half_count):
                    arrived(s_, (j + n) % half_count)
                build_if(s_)

    def q_lanes(group, pair):
        return pl.ds(pl.multiple_of(group * width + pair * 128, 128), 128)

    def far_q_copy(group, pair):
        unit = kv_heads * pair + g
        slot = jnp.minimum(pairs + unit, 2 * pairs - 1)
        return remote(
            query_ref.at[:, q_lanes(group, pair)], in_q.at[slot],
            q_send.at[group * pairs + pair], q_recv.at[slot], (s_far, group, j),
        )

    def near_q_copy(pair):
        return remote(
            query_ref.at[:, q_lanes(partner_x, pair)], in_q.at[pair],
            q_send.at[partner_x * pairs + pair], q_recv.at[pair], (s, partner_x, j),
        )

    def q_arrived(slot):
        remote(
            query_ref.at[:, pl.ds(0, 128)], in_q.at[slot], q_send.at[0], q_recv.at[slot], here
        ).wait_recv()

    def is_given(pair, x_):
        return kv_heads * pair + x_ < given

    def far_sends(act):
        for pair in range(pairs):
            for group in range(kv_heads):

                @pl.when(is_given(pair, g))
                def _():
                    act([far_q_copy(group, pair)])

    def near_sends(act):
        for pair in range(pairs):

            @pl.when(jnp.logical_not(is_given(pair, g)))
            def _():
                act([near_q_copy(pair)])

    def far_decay_copies():
        copies = []
        for x_ in range(kv_heads):
            for n in range(half_count):
                source = decay_ref.at[:, pl.ds((x_ * half_count + n) * rows, rows)]
                at = x_ * half_count + n
                copies.append(
                    remote(
                        source, far_decay.at[x_ * half_count + j], far_send.at[at],
                        far_recv.at[x_ * half_count + j], (s_far, g, n),
                    )
                )
        return copies

    own_block = block_at(s, g, j)
    other_block = block_at(s, partner_x, j)
    member = s * half_count + j

    def side_targets():
        targets = [(None, (s, g, (j + n) % half_count)) for n in range(1, half_count)]
        targets.append((inside(z + 1), ((z + 1) * ys + y, g, j)))
        targets += [(None, (z * ys + (y + n) % ys, g, j)) for n in range(1, ys)]
        return targets

    down = (jnp.maximum(z - 1, 0) * ys + y, g, j)
    down_base = (ys + half_count - 1) * each

    def each_side(act):
        for slot, (condition, device) in enumerate(side_targets()):
            if condition is None:
                act(slot * each, device)
            else:

                @pl.when(condition)
                def _():
                    act(slot * each, device)

    def own_copies(base, device):
        return [
            kv_copy(kvt_ref.at[g], own_block, own_send.at[base], device),
            decay_copy(decay_ref, member, own_send.at[base + 1], device),
        ]

    def other_copies(base, device):
        return [kv_copy(kvt_all.at[other_block], other_block, own_send.at[base + 2], device)]

    x_copy = kv_copy(kvt_ref.at[partner_x], own_block, x_send, (s, partner_x, j))
    x_copy.start()
    each_side(lambda base, device: start_all(own_copies(base, device)))

    @pl.when(is_high)
    def _():
        far_sends(start_all)
        start_all(far_decay_copies())

    @pl.when(z > 0)
    def _():
        start_all(own_copies(down_base, down))

    near_sends(start_all)
    kvt_all[own_block] = kvt_ref[g]
    decay_all[member] = decay_ref[...]
    acc_ref[...] = jnp.zeros_like(acc_ref)
    vt_all[:, 64:80] = jnp.ones((sp_count, 16, chunk_rows), jnp.bfloat16)

    def prepare(t, slot, source, pair, decays):
        turned = source.astype(jnp.float32).T.astype(jnp.bfloat16)
        high = decays.astype(jnp.bfloat16).astype(jnp.float32)
        rest = decays - high
        middle = rest.astype(jnp.bfloat16).astype(jnp.float32)
        rest = rest - middle
        row = lax.broadcasted_iota(jnp.int32, (64, rows), 0)
        for n in range(2):
            head = 2 * pair + n
            lanes = pl.ds(slot * span + n * rows, rows)
            picked = (row == head) | (row == 8 + head) | (row == 16 + head)
            extra = jnp.where(picked, 1.0, 0.0)
            for at, part in ((24, high), (25, middle), (26, rest)):
                extra = jnp.where(row == at, part[n : n + 1], extra)
            qt_ref[t, 0:64, lanes] = turned[n * 64 : (n + 1) * 64]
            qt_ref[t, 64:128, lanes] = extra.astype(jnp.bfloat16)

    def own_decays(pair, x_):
        first = (2 * pair) % local
        at = pl.ds(pl.multiple_of((x_ * half_count + j) * rows, rows), rows)
        return decay_all[s * half_count + (2 * pair) // local, first : first + 2, at]

    def far_decays(slot):
        pair, x_ = slot // kv_heads, slot % kv_heads
        first = (2 * pair) % local
        return far_decay[x_ * half_count + (2 * pair) // local, first : first + 2]

    def work(t, at, lanes, chunk, start, size, step, limit=None):
        at = pl.ds(pl.multiple_of(at, span), lanes)
        q = qt_ref[t, :, at]
        total = acc_ref[t, :, at]
        for b in range(size // step):
            where = pl.ds(pl.multiple_of(start + b * step, step), step)
            scores = jnp.dot(kp_all[chunk, where], q, preferred_element_type=jnp.float32)
            if limit is not None:
                key = lax.broadcasted_iota(jnp.int32, (step, lanes), 0)
                row = lax.broadcasted_iota(jnp.int32, (step, lanes), 1) % rows
                scores = jnp.where(key <= row, scores, -1e30)
            weights = jnp.exp2(scores).astype(jnp.bfloat16)
            total = total + jnp.dot(
                vt_all[chunk, :, where], weights, preferred_element_type=jnp.float32
            )
        acc_ref[t, :, at] = total

    def whole(t, at, lanes, chunk):
        work(t, at, lanes, chunk, 0, chunk_rows, chunk_rows if lanes == span else chunk_rows // 2)

    def sweep(t, at, lanes, low, high):
        def body(chunk, carry):
            whole(t, at, lanes, chunk)
            return carry

        lax.fori_loop(low, high, body, 0)

    def diagonal(t, at, lanes, chunk, offset):
        def body(i, carry):
            work(t, at, lanes, chunk, i * rows, rows, rows)
            return carry

        lax.fori_loop(0, offset // rows, body, 0)
        work(t, at, lanes, chunk, offset, rows, rows, True)

    def finished(t, slot):
        out = []
        for n in range(2):
            lanes = pl.ds(slot * span + n * rows, rows)
            out.append(acc_ref[t, 0:64, lanes] / acc_ref[t, 64:65, lanes])
        return jnp.concatenate(out, axis=0).T.astype(jnp.bfloat16)

    def back_copy(slot, pair, device):
        return remote(
            res_ref.at[slot], out_ref.at[:, q_lanes(g, pair)], back_send.at[slot],
            back_recv.at[g * pairs + pair], device,
        )

    def back_arrived(group, pair):
        remote(
            res_ref.at[0], out_ref.at[:, q_lanes(group, pair)], back_send.at[0],
            back_recv.at[group * pairs + pair], here,
        ).wait_recv()

    def kept_groups(first, act):
        def body(i, carry):
            @pl.when(first <= 2 * i)
            def _():
                act(i * 2 * span, 2 * span)

            @pl.when(first == 2 * i + 1)
            def _():
                act((2 * i + 1) * span, span)

            return carry

        lax.fori_loop(0, pairs // 2, body, 0)

    def taken_groups(act):
        def body(i, carry):
            @pl.when(taken >= 2 * i + 2)
            def _():
                act(i * 2 * span, 2 * span)

            @pl.when(taken == 2 * i + 1)
            def _():
                act(i * 2 * span, span)

            return carry

        lax.fori_loop(0, pairs // 2, body, 0)

    my_first = kept_from(g)
    partner_first = kept_from(partner_x)
    offset = (g * half_count + j) * rows
    partner_offset = (partner_x * half_count + j) * rows

    kv_copy(kvt_ref.at[g], other_block, x_send, here).wait_recv()
    each_side(lambda base, device: start_all(other_copies(base, device)))

    @pl.when(z > 0)
    def _():
        start_all(other_copies(down_base, down))

    for n in range(1, half_count):
        arrived(s, (j + n) % half_count)
    build(s)
    for pair in range(pairs):
        prepare(0, pair, query_ref[:, q_lanes(g, pair)], pair, own_decays(pair, g))
    kept_groups(my_first, lambda at, lanes: diagonal(0, at, lanes, s, offset))
    round_of(1, True)

    def item(k, carry):
        lanes_of(k)

        @pl.when(k < zs)
        def _():
            round_of(k + 1, True)

        back = jnp.where(y == 0, jnp.where(k == 1, ys, jnp.where(k == ys, 1, k)), k)

        @pl.when(k <= s)
        def _():
            kept_groups(my_first, lambda at, lanes: whole(0, at, lanes, s - back))

        return carry

    lax.fori_loop(1, zs + 1, item, 0)

    @pl.when(z >= zh)
    def _():
        for extra in range(zs - zh):
            late(jnp.maximum(z + 1, zh) + extra, True)

    first_late = jnp.maximum(z + 1, zh)

    def partner_phase():
        def body(i, carry):
            for n in range(pairs):

                @pl.when((i == n // 2) & (partner_first <= n))
                def _():
                    q_arrived(n)
                    prepare(1, n, in_q[n], n, own_decays(n, partner_x))

            def run(at, lanes):
                diagonal(1, at, lanes, s, partner_offset)
                sweep(1, at, lanes, 0, s)

            @pl.when(partner_first <= 2 * i)
            def _():
                run(i * 2 * span, 2 * span)

            @pl.when(partner_first == 2 * i + 1)
            def _():
                run((2 * i + 1) * span, span)

            for n in range(pairs):

                @pl.when((i == n // 2) & (partner_first <= n))
                def _():
                    res_ref[n] = finished(1, n)
                    back_copy(n, n, (s, partner_x, j)).start()

            @pl.when((i == 0) & (z < zh))
            def _():
                late(first_late, True)
                late_across(first_late, True)

            return carry

        lax.fori_loop(0, pairs // 2, body, 0)

        @pl.when((z > 0) & (z < zh))
        def _():
            for extra in range(1, zs - zh):
                late(first_late + extra, True)
                late_across(first_late + extra, True)

    def far_phase():
        for n in range(kv_heads * half_count):
            remote(
                decay_ref.at[:, pl.ds(0, rows)], far_decay.at[n], far_send.at[n],
                far_recv.at[n], here,
            ).wait_recv()

        for n in range(pairs):

            @pl.when(n < taken)
            def _():
                q_arrived(pairs + n)
                prepare(2, n, in_q[pairs + n], n // kv_heads, far_decays(n))

        taken_groups(lambda at, lanes: sweep(2, at, lanes, 0, upper))

    def turn(i, carry):
        @pl.when((i == 0) == (z > 0))
        def _():
            partner_phase()

        @pl.when(((i == 0) == (z == 0)) & (z < zh))
        def _():
            far_phase()

        return carry

    lax.fori_loop(0, 2, turn, 0)

    @pl.when(z < zh)
    def _():
        def zone(zo, carry):
            @pl.when((z == 0) & (zo > first_late))
            def _():
                late(zo, True)
                late_across(zo, True)

            late_lanes(zo)

            @pl.when(zo < zs - 1 - z)
            def _():
                taken_groups(lambda at, lanes: sweep(2, at, lanes, zo * ys, zo * ys + ys))

            return carry

        lax.fori_loop(zh, zs - z, zone, 0)
        last = (zs - 1 - z) * ys
        taken_groups(lambda at, lanes: sweep(2, at, lanes, last, s_far))

        def close(n, carry):
            unit_x = n % kv_heads
            diagonal(2, n * span, span, s_far, (unit_x * half_count + j) * rows)
            for m in range(pairs):

                @pl.when(n == m)
                def _():
                    res_ref[pairs + m] = finished(2, m)
                    back_copy(
                        pairs + m, m // kv_heads, (s_far, m % kv_heads, j)
                    ).start()

            return carry

        lax.fori_loop(0, taken, close, 0)

    kept_groups(my_first, lambda at, lanes: sweep(0, at, lanes, 0, jnp.maximum(s - zs, 0)))
    for pair in range(pairs):

        @pl.when(pair >= my_first)
        def _():
            out_ref[:, q_lanes(g, pair)] = finished(0, pair)

    x_copy.wait_send()
    each_side(
        lambda base, device: drain_all(own_copies(base, device) + other_copies(base, device))
    )

    @pl.when(z > 0)
    def _():
        drain_all(own_copies(down_base, down) + other_copies(down_base, down))

    def drain(k, carry):
        round_of(k, False)
        return carry

    lax.fori_loop(1, zs + 1, drain, 0)

    def drain_late(zo, carry):
        late(zo, False)
        late_across(zo, False)
        return carry

    lax.fori_loop(zh, zs, drain_late, 0)

    @pl.when(is_high)
    def _():
        far_sends(drain_all)
        drain_all(far_decay_copies())

    near_sends(drain_all)
    for pair in range(pairs):

        @pl.when(partner_first <= pair)
        def _():
            back_copy(pair, pair, (s, partner_x, j)).wait_send()

        @pl.when(pair < taken)
        def _():
            back_copy(
                pairs + pair, pair // kv_heads, (s_far, pair % kv_heads, j)
            ).wait_send()

        back_arrived(partner_x, pair)

        @pl.when(pair < my_first)
        def _():
            back_arrived(g, pair)


def lines_of(sp_count):
    ys = 1 << ((sp_count.bit_length() - 1) // 2)
    return sp_count // ys, ys


def stream(queries, kvt, decays, sizes):
    sp_count, kv_heads, half_count = sizes
    rows = queries.shape[0]
    heads = queries.shape[1] // 64 // kv_heads
    local, chunk_rows = decays.shape
    zs, ys = lines_of(sp_count)
    pairs = heads // 2
    count = sp_count * kv_heads * half_count
    members = sp_count * half_count
    per = 1 + (ys - 1) + (half_count - 1) + (ys - 1) * (half_count - 1)
    each = kv_heads + 1
    vmem = pl.BlockSpec(memory_space=pltpu.VMEM)
    dma = pltpu.SemaphoreType.DMA
    return pl.pallas_call(
        lambda *refs: stream_kernel(
            *refs, sizes=sizes, lines=(zs, ys), rows=rows, heads=heads
        ),
        out_shape=jax.ShapeDtypeStruct(queries.shape, jnp.bfloat16),
        in_specs=[vmem] * 3,
        out_specs=vmem,
        scratch_shapes=[
            pltpu.VMEM((count, 128, rows), jnp.bfloat16),
            pltpu.VMEM((members, local, chunk_rows), jnp.float32),
            pltpu.VMEM((kv_heads * half_count, local, rows), jnp.float32),
            pltpu.VMEM((2 * pairs, rows, 128), jnp.bfloat16),
            pltpu.VMEM((3, 128, heads * rows), jnp.bfloat16),
            pltpu.VMEM((3, 80, heads * rows), jnp.float32),
            pltpu.VMEM((sp_count, chunk_rows, 128), jnp.bfloat16),
            pltpu.VMEM((sp_count, 80, chunk_rows), jnp.bfloat16),
            pltpu.VMEM((2 * pairs, rows, 128), jnp.bfloat16),
            dma((count,)), dma((members,)), dma, dma(((ys + half_count) * each,)),
            dma((zs * 2 * per * each,)), dma(((zs - zs // 2) * per * each,)),
            dma((kv_heads * half_count,)), dma((kv_heads * half_count,)),
            dma((2 * pairs,)), dma((2 * pairs,)), dma((2 * pairs,)), dma((2 * pairs,)),
        ],
        compiler_params=pltpu.CompilerParams(
            has_side_effects=True, vmem_limit_bytes=44 * 1024 * 1024
        ),
        name="stream",
    )(kvt, queries, decays)


def any_scores(queries, kv_blocks, decays, sizes):
    sp_count, kv_heads, half_count = sizes
    group = lax.axis_index("kv")
    me = (lax.axis_index("sp") * kv_heads + group) * half_count + lax.axis_index("half")
    count = sp_count * kv_heads * half_count
    mirror = [(i, count - 1 - i) for i in range(count)]
    rows = queries.shape[0]
    length = rows * count
    heads = queries.shape[1] // 64 // kv_heads
    width = heads * 64
    members = sp_count * half_count
    key_block = math.gcd(length, KEY_BLOCK)

    def choose(a, b):
        return jnp.where(group == 0, a, b)

    decay_rows = decays.reshape(-1, 128)
    own_q = choose(queries[:, :width], queries[:, width:])
    sent_q = choose(queries[:, width:], queries[:, :width])
    vmem = pl.BlockSpec(memory_space=pltpu.VMEM)
    chips = count // 2
    dma = pltpu.SemaphoreType.DMA
    kv, far_q, decay_all = pl.pallas_call(
        lambda *refs: exchange_kernel(*refs, rows=rows, sizes=sizes),
        out_shape=(
            jax.ShapeDtypeStruct((length, 128), jnp.bfloat16),
            jax.ShapeDtypeStruct((rows, width), jnp.bfloat16),
            jax.ShapeDtypeStruct((members, *decay_rows.shape), jnp.float32),
        ),
        in_specs=[vmem] * 3,
        out_specs=(vmem,) * 3,
        scratch_shapes=[
            dma((2,)), dma((chips,)), dma((count,)), dma((chips,)), dma((members // 2,)),
            dma((members,)), dma((members // 2,)), dma, dma,
        ],
        compiler_params=pltpu.CompilerParams(has_side_effects=True),
        name="exchange",
    )(kv_blocks, sent_q, decay_rows)
    decay_all = decay_all.reshape(sp_count, heads, -1, key_block)
    decay_all = decay_all.transpose(0, 2, 1, 3).reshape(length // key_block, heads, key_block)
    firsts = (me * rows, (count - 1 - me) * rows)
    place = jnp.stack(firsts).astype(jnp.int32)
    row_decay = jnp.stack(
        [
            lax.dynamic_slice(
                decay_all, (first // key_block, 0, first % key_block), (1, heads, rows)
            )[0].T
            for first in firsts
        ]
    )
    attended = attend(place, own_q, far_q, row_decay, decay_all, kv, False)
    back = lax.ppermute(attended[1], ALL, mirror)
    return choose(
        jnp.concatenate([attended[0], back], axis=1), jnp.concatenate([back, attended[0]], axis=1)
    )


def per_device(inputs, in_gain, w_query, w_key, w_value, query_gain, key_gain, decay_sums, w_out):
    kv_heads = lax.axis_size("kv")
    sizes = (lax.axis_size("sp"), kv_heads, lax.axis_size("half"))
    head_size = query_gain.shape[0]
    rows = inputs.shape[0]
    all_heads = w_query.shape[1] // head_size

    normed = rms_norm(inputs.astype(jnp.float32), in_gain).astype(jnp.bfloat16)
    keys = rms_norm(
        jnp.dot(normed, w_key, preferred_element_type=jnp.float32).reshape(
            rows, kv_heads, head_size
        ),
        key_gain,
    ).astype(jnp.bfloat16)
    values = (
        jnp.dot(normed, w_value, preferred_element_type=jnp.float32)
        .astype(jnp.bfloat16)
        .reshape(rows, kv_heads, head_size)
    )
    pairs = jnp.concatenate([keys, values], axis=2)
    kvt = pairs.transpose(1, 2, 0)
    decays = decay_sums.T * LOG2E

    queries = rms_norm(
        jnp.dot(normed, w_query, preferred_element_type=jnp.float32).reshape(
            rows, all_heads, head_size
        ),
        query_gain * (LOG2E * head_size ** (-0.5)),
    ).astype(jnp.bfloat16).reshape(rows, all_heads * head_size)
    bound = head_size**0.5 * LOG2E * jnp.max(query_gain) * jnp.max(key_gain)
    whole = lax.cond(
        bound <= SMALL,
        lambda queries, kvt, decays: stream(queries, kvt, decays, sizes),
        lambda queries, kvt, decays: any_scores(
            queries, kvt.transpose(0, 2, 1), decays, sizes
        ),
        queries, kvt, decays,
    )
    return jnp.dot(whole, w_out, preferred_element_type=jnp.float32).astype(jnp.bfloat16)


def solution(mesh):
    sp_count, tp_count = mesh.devices.shape
    split = Mesh(mesh.devices.reshape(sp_count, 2, tp_count // 2), ALL)
    placed = (P(ALL, None), P(), P(), P(), P(), P(), P(), P("sp", ("kv", "half")), P())
    return jax.shard_map(
        per_device, mesh=split, in_specs=placed, out_specs=P(ALL, None), check_vma=False
    )
```

```python
import math

import jax
import jax.numpy as jnp
from jax import lax
from jax.experimental import pallas as pl
from jax.experimental.pallas import tpu as pltpu
from jax.sharding import Mesh, PartitionSpec as P

epsilon = 1e-06
LOG2E = math.log2(math.e)
ALL = ("sp", "kv", "half")
HEADS_PER_DOT = 2
KEY_BLOCK = 512
SMALL = 60.0


def rms_norm(vector, gain_vec):
    return (
        vector * lax.rsqrt(jnp.mean(vector * vector, axis=-1, keepdims=True) + epsilon) * gain_vec
    )


def exchange_kernel(
    kv_ref, q_ref, decay_ref, kv_out, q_out, decay_out, own_sems, kv_send, kv_recv, kv_relay,
    decay_send, decay_recv, decay_relay, q_send, q_recv, *, rows, sizes
):
    sp_count, kv_heads, half_count = sizes
    sp, group, half = lax.axis_index("sp"), lax.axis_index("kv"), lax.axis_index("half")
    core, chips = half % 2, half_count // 2
    partner = (sp, group, half + 1 - 2 * core)

    def device_of(chip):
        return (chip // (kv_heads * chips), (chip // chips) % kv_heads, (chip % chips) * 2 + core)

    def block_of(place):
        return (place[0] * kv_heads + place[1]) * half_count + place[2]

    def kv_copy(source, block, send, device):
        return pltpu.make_async_remote_copy(
            src_ref=source, dst_ref=kv_out.at[pl.ds(pl.multiple_of(block * rows, rows), rows)],
            send_sem=send, recv_sem=kv_recv.at[block], device_id=device,
            device_id_type=pl.DeviceIdType.MESH,
        )

    def decay_copy(source, member, send, device):
        return pltpu.make_async_remote_copy(
            src_ref=source, dst_ref=decay_out.at[member], send_sem=send,
            recv_sem=decay_recv.at[member], device_id=device,
            device_id_type=pl.DeviceIdType.MESH,
        )

    me = block_of((sp, group, half))
    chip = (sp * kv_heads + group) * chips + half // 2
    total = sp_count * kv_heads * chips
    member = sp * half_count + half
    cluster = sp * chips + half // 2
    clusters = sp_count * chips
    started = []
    for k in range(1, total):
        place = device_of((chip + k) % total)
        started.append(kv_copy(kv_ref.at[place[1]], me, kv_send.at[k], place))
        started[-1].start()
    for k in range(1, clusters):
        other = (cluster + k) % clusters
        place = (other // chips, group, (other % chips) * 2 + core)
        started.append(decay_copy(decay_ref, member, decay_send.at[k], place))
        started[-1].start()
    q_copy = pltpu.make_async_remote_copy(
        src_ref=q_ref, dst_ref=q_out, send_sem=q_send, recv_sem=q_recv,
        device_id=(sp_count - 1 - sp, kv_heads - 1 - group, half_count - 1 - half),
        device_id_type=pl.DeviceIdType.MESH,
    )
    q_copy.start()
    started.append(kv_copy(kv_ref.at[group], me, kv_relay.at[0], partner))
    started[-1].start()
    started.append(decay_copy(decay_ref, member, decay_relay.at[0], partner))
    started[-1].start()
    own_kv = pltpu.make_async_copy(
        kv_ref.at[group], kv_out.at[pl.ds(pl.multiple_of(me * rows, rows), rows)], own_sems.at[0]
    )
    own_kv.start()
    own_decay = pltpu.make_async_copy(decay_ref, decay_out.at[member], own_sems.at[1])
    own_decay.start()
    for k in range(1, clusters):
        other = (cluster + clusters - k) % clusters
        which = (other // chips) * half_count + (other % chips) * 2 + core
        landed = decay_out.at[which]
        relay = decay_copy(landed, which, decay_relay.at[k], partner)
        relay.wait_recv()
        relay.start()
        started.append(relay)
    for k in range(1, total):
        block = block_of(device_of((chip + total - k) % total))
        landed = kv_out.at[pl.ds(pl.multiple_of(block * rows, rows), rows)]
        relay = kv_copy(landed, block, kv_relay.at[k], partner)
        relay.wait_recv()
        relay.start()
        started.append(relay)
    for k in range(clusters):
        other = (cluster + clusters - k) % clusters
        which = (other // chips) * half_count + (other % chips) * 2 + 1 - core
        decay_copy(decay_out.at[which], which, decay_relay.at[k], partner).wait_recv()
    for k in range(total):
        place = device_of((chip + total - k) % total)
        block = block_of((place[0], place[1], place[2] + 1 - 2 * core))
        landed = kv_out.at[pl.ds(pl.multiple_of(block * rows, rows), rows)]
        kv_copy(landed, block, kv_relay.at[k], partner).wait_recv()
    for copy in started:
        copy.wait_send()
    own_kv.wait()
    own_decay.wait()
    q_copy.wait()


def attend_kernel(
    place_ref, near_ref, far_ref, row_ref, decay_ref, kv_ref, out_ref, ones_ref, q_ref, peak_ref,
    acc_ref, *, rows, heads, key_block, small
):
    lane = lax.broadcasted_iota(jnp.int32, (rows, 128), 1)
    low = lane < 64
    for r, ref in enumerate((near_ref, far_ref)):
        for pair in range(heads // 2):
            both = ref[:, pair * 128 : (pair + 1) * 128].astype(jnp.float32)
            even = jnp.where(low, both, 0.0)
            odd = jnp.where(low, pltpu.roll(both, 64, 1), 0.0)
            q_ref[r, (2 * pair) * rows : (2 * pair + 1) * rows] = even.astype(jnp.bfloat16)
            q_ref[r, (2 * pair + 1) * rows : (2 * pair + 2) * rows] = odd.astype(jnp.bfloat16)

    def fill(i, carry):
        at = pl.ds(pl.multiple_of(i * key_block, key_block), key_block)
        wide = lax.broadcasted_iota(jnp.int32, (key_block, 128), 1) < 64
        ones_ref[at] = jnp.where(wide, 1.0, kv_ref[at].astype(jnp.float32)).astype(jnp.bfloat16)
        return carry

    lax.fori_loop(0, kv_ref.shape[0] // key_block, fill, 0)
    span = HEADS_PER_DOT * rows

    for r in range(2):
        first = place_ref[r]
        for head in range(heads):
            part = pl.ds(head * rows, rows)
            if small:
                peak_ref[part] = jnp.broadcast_to(row_ref[r, :, head : head + 1], (rows, 128))
            else:
                peak_ref[part] = jnp.full((rows, 128), -1e30, jnp.float32)
        acc_ref[...] = jnp.zeros_like(acc_ref)

        def step(index, masked):
            at = pl.ds(pl.multiple_of(index * key_block, key_block), key_block)
            keys = kv_ref[at]
            values = ones_ref[at]
            for start in range(0, heads, HEADS_PER_DOT):
                part = pl.ds(start * rows, span)
                before = peak_ref[part]
                scores = lax.dot_general(
                    q_ref[r, part], keys, (((1,), (1,)), ((), ())),
                    preferred_element_type=jnp.float32,
                )
                if small:
                    scores = scores + jnp.concatenate([before] * (key_block // 128), axis=1)
                scores = scores.reshape(HEADS_PER_DOT, rows, key_block)
                scores = scores - decay_ref[index, start : start + HEADS_PER_DOT][:, None, :]
                if masked:
                    row = first + lax.broadcasted_iota(jnp.int32, (rows, key_block), 0)
                    col = index * key_block + lax.broadcasted_iota(
                        jnp.int32, (rows, key_block), 1
                    )
                    scores = jnp.where((col <= row)[None], scores, -1e30)
                scores = scores.reshape(span, key_block)
                if small:
                    weights = jnp.exp2(scores).astype(jnp.bfloat16)
                    acc_ref[part] += jnp.dot(weights, values, preferred_element_type=jnp.float32)
                else:
                    after = jnp.maximum(before, jnp.max(scores, axis=1, keepdims=True))
                    weights = jnp.exp2(scores - after[:, :1]).astype(jnp.bfloat16)
                    acc_ref[part] = acc_ref[part] * jnp.exp2(before - after) + jnp.dot(
                        weights, values, preferred_element_type=jnp.float32
                    )
                    peak_ref[part] = after

        full = first // key_block

        def body(index, carry):
            step(index, False)
            return carry

        lax.fori_loop(0, full, body, 0)
        step(full, True)
        for pair in range(heads // 2):
            even = acc_ref[(2 * pair) * rows : (2 * pair + 1) * rows]
            odd = acc_ref[(2 * pair + 1) * rows : (2 * pair + 2) * rows]
            done = jnp.where(low, pltpu.roll(even, 64, 1), odd) / jnp.where(
                low, even, pltpu.roll(odd, 64, 1)
            )
            out_ref[r, :, pair * 128 : (pair + 1) * 128] = done.astype(jnp.bfloat16)


def attend(place, near, far, row_decay, decays, kv, small):
    length = kv.shape[0]
    rows, width = near.shape
    heads, key_block = decays.shape[1:]
    vmem = pl.BlockSpec(memory_space=pltpu.VMEM)
    return pl.pallas_call(
        lambda *refs: attend_kernel(
            *refs, rows=rows, heads=heads, key_block=key_block, small=small
        ),
        out_shape=jax.ShapeDtypeStruct((2, rows, width), jnp.bfloat16),
        in_specs=[pl.BlockSpec(memory_space=pltpu.SMEM)] + [vmem] * 5,
        out_specs=vmem,
        scratch_shapes=[
            pltpu.VMEM((length, 128), jnp.bfloat16),
            pltpu.VMEM((2, heads * rows, 128), jnp.bfloat16),
            pltpu.VMEM((heads * rows, 128), jnp.float32),
            pltpu.VMEM((heads * rows, 128), jnp.float32),
        ],
        compiler_params=pltpu.CompilerParams(vmem_limit_bytes=40 * 1024 * 1024),
        name="attend_small" if small else "attend_any",
    )(place, near, far, row_decay, decays, kv)


def stream_kernel(
    x_hbm, in_gain, wq_hbm, wk_hbm, wv_hbm, query_gain, key_gain, sums_hbm, wo_hbm, out_ref,
    x_ref, wkv_ref, wq_ref, sums_ref, wo_ref, normed_ref, kvt_ref, query_ref, decay_ref, att_ref,
    kvt_all, decay_all, far_decay, in_q, qt_ref, acc_ref, kp_all, vt_all, res_ref, loads, kv_recv,
    decay_recv, x_send, own_send, round_send, late_send, far_send, far_recv, q_send, q_recv,
    back_send, back_recv, *, sizes, lines, rows, heads
):
    sp_count, kv_heads, half_count = sizes
    zs, ys = lines
    zh = zs // 2
    upper = sp_count // 2
    pairs = heads // 2
    units = pairs * kv_heads
    width = heads * 64
    span = 2 * rows
    local, chunk_rows = decay_ref.shape
    s, g, j = lax.axis_index("sp"), lax.axis_index("kv"), lax.axis_index("half")
    z, y = s // ys, s % ys
    partner_x = 1 - g
    s_far = sp_count - 1 - s
    is_high = s >= upper

    def share(s_):
        return (2 * units * (2 * s_ + 1 - sp_count) + 2 * s_ + 1) // (2 * (2 * s_ + 1))

    given = jnp.where(is_high, share(jnp.maximum(s, upper)), 0)
    taken = jnp.where(is_high, 0, share(jnp.maximum(s_far, upper)))

    def kept_from(x_):
        return (jnp.maximum(given - x_, 0) + kv_heads - 1) // kv_heads

    def block_at(s_, x_, j_):
        return (s_ * kv_heads + x_) * half_count + j_

    def remote(source, target, send, recv, device):
        return pltpu.make_async_remote_copy(
            src_ref=source, dst_ref=target, send_sem=send, recv_sem=recv, device_id=device,
            device_id_type=pl.DeviceIdType.MESH,
        )

    def kv_copy(source, block, send, device):
        return remote(source, kvt_all.at[block], send, kv_recv.at[block], device)

    def decay_copy(source, member, send, device):
        return remote(source, decay_all.at[member], send, decay_recv.at[member], device)

    here = (s, g, j)
    each = kv_heads + 1

    def one_piece(s_, j_, piece, base, device, sems):
        if piece == kv_heads:
            member = s_ * half_count + j_
            return decay_copy(decay_all.at[member], member, sems.at[base + piece], device)
        block = block_at(s_, piece, j_)
        return kv_copy(kvt_all.at[block], block, sems.at[base + piece], device)

    def arrived(s_, j_):
        for piece in range(each):
            one_piece(s_, j_, piece, 0, here, own_send).wait_recv()

    def start_all(copies):
        for copy in copies:
            copy.start()

    def drain_all(copies):
        for copy in copies:
            copy.wait_send()

    def inside(z_):
        return (z_ >= 0) & (z_ < zs)

    def to_rows(base):
        return [
            (None, base + (n - 1) * each, (z * ys + (y + n) % ys, g, j)) for n in range(1, ys)
        ]

    def to_lanes(base):
        return [
            (None, base + (n - 1) * each, (s, g, (j + n) % half_count))
            for n in range(1, half_count)
        ]

    def relay(s_, routes, sems, go):
        for piece in range(each):
            if go:
                one_piece(s_, j, piece, 0, here, own_send).wait_recv()
            for condition, base, device in routes:
                copy = one_piece(s_, j, piece, base, device, sems)
                act = copy.start if go else copy.wait_send
                if condition is None:
                    act()
                else:
                    pl.when(condition)(act)

    per = 1 + (ys - 1) + (half_count - 1) + (ys - 1) * (half_count - 1)

    def spread(s_, base, condition, device, sems, go):
        routes = [(condition, base, device)]
        routes += to_rows(base + each) + to_lanes(base + ys * each)
        relay(s_, routes, sems, go)

    def across(zo, base, sems, go):
        for m in range(1, ys):
            slot = ys + half_count - 1 + (m - 1) * (half_count - 1)
            relay(zo * ys + (y + m) % ys, to_lanes(base + slot * each), sems, go)

    def near_from(z_, way):
        return inside(z_) if way > 0 else inside(z_) & (z_ < zh)

    def round_of(k, go):
        for d, way in enumerate((1, -1)):
            base = ((k - 1) * 2 + d) * per * each

            @pl.when(near_from(z - way * k, way))
            def _():
                spread(
                    (z - way * k) * ys + y, base, inside(z + way), ((z + way) * ys + y, g, j),
                    round_send, go,
                )

            reach = near_from(z - way * (k - 1), way)
            if way < 0:
                reach = reach & (k != 1)

            @pl.when(reach)
            def _():
                across(z - way * (k - 1), base, round_send, go)

    def late(zo, go):
        @pl.when(zo <= zs - 1 - z)
        def _():
            base = (zo - zh) * per * each
            spread(zo * ys + y, base, z > 0, ((z - 1) * ys + y, g, j), late_send, go)

    def late_across(zo, go):
        @pl.when(zo <= zs - 1 - z)
        def _():
            across(zo, (zo - zh) * per * each, late_send, go)

    def build(s_):
        for x_ in range(kv_heads):
            for j_ in range(half_count):
                block = block_at(s_, x_, j_)
                place = (x_ * half_count + j_) * rows
                decays = jnp.concatenate(
                    [
                        decay_all[s_ * half_count + n, :, pl.ds(place, rows)]
                        for n in range(half_count)
                    ],
                    axis=0,
                )
                decays = -decays
                high = decays.astype(jnp.bfloat16).astype(jnp.float32)
                rest = decays - high
                middle = rest.astype(jnp.bfloat16).astype(jnp.float32)
                parts = jnp.concatenate(
                    [high, middle, rest - middle, jnp.ones((8, rows), jnp.float32)], axis=0
                ).astype(jnp.bfloat16)
                wide = jnp.concatenate(
                    [kvt_all[block, 0:64], parts, jnp.zeros((32, rows), jnp.bfloat16)], axis=0
                )
                kp_all[s_, pl.ds(place, rows)] = wide.T
                vt_all[s_, 0:64, pl.ds(place, rows)] = kvt_all[block, 64:128]

    def build_if(s_):
        @pl.when(s_ <= jnp.where(is_high, s, s_far))
        def _():
            build(s_)

    def lanes_of(k):
        for way in (1, -1):

            @pl.when(near_from(z - way * k, way))
            def _():
                s_ = (z - way * k) * ys + y
                for n in range(1, half_count):
                    arrived(s_, (j + n) % half_count)
                build_if(s_)

            reach = near_from(z - way * (k - 1), way)
            if way < 0:
                reach = reach & (k != 1)

            @pl.when(reach)
            def _():
                for m in range(1, ys):
                    s_ = (z - way * (k - 1)) * ys + (y + m) % ys
                    for n in range(1, half_count):
                        arrived(s_, (j + n) % half_count)
                    build_if(s_)

    def late_lanes(zo):
        @pl.when(zo <= zs - 1 - z)
        def _():
            for m in range(ys):
                s_ = zo * ys + (y + m) % ys
                for n in range(1, half_count):
                    arrived(s_, (j + n) % half_count)
                build_if(s_)

    def q_lanes(group, pair):
        return pl.ds(pl.multiple_of(group * width + pair * 128, 128), 128)

    fetches = [
        pltpu.make_async_copy(source, target, loads.at[n])
        for n, (source, target) in enumerate(
            (
                (x_hbm, x_ref), (wk_hbm, wkv_ref.at[:, 0:128]), (wv_hbm, wkv_ref.at[:, 128:256]),
                (sums_hbm, sums_ref), (wq_hbm, wq_ref), (wo_hbm, wo_ref),
            )
        )
    ]
    for fetch in fetches:
        fetch.start()

    barrier = pltpu.get_barrier_semaphore()

    def greet(device):
        pl.semaphore_signal(
            barrier, inc=1, device_id=device, device_id_type=pl.DeviceIdType.MESH
        )

    greeted = 0
    for n in range(1, half_count):
        greet((s, g, (j + n) % half_count))
        greeted += 1
    greet((s, partner_x, j))
    greet(((zs - 1 - z) * ys + y, g, j))
    greeted += 2
    for n in range(1, ys):
        greet((z * ys + (y + n) % ys, g, j))
        greeted += 1
    for x_ in range(kv_heads):
        for n in range(half_count):
            greet((s_far, x_, n))
            greeted += 1
    for way in (1, -1):

        @pl.when(inside(z + way))
        def _():
            greet(((z + way) * ys + y, g, j))

        greeted = greeted + jnp.where(inside(z + way), 1, 0)

    def columns(gain):
        wide = jnp.broadcast_to(gain.reshape(1, 64), (64, 64))
        wide = jnp.concatenate([wide, wide], axis=1)
        wide = jnp.concatenate([wide, wide], axis=0).T
        return jnp.concatenate([wide[0:64]] * (rows // 128), axis=1)

    def per_head(turned, gain):
        many = turned.reshape(turned.shape[0] // 64, 64, rows)
        mean = jnp.mean(many * many, axis=1, keepdims=True)
        return (many * lax.rsqrt(mean + epsilon) * gain[None]).reshape(turned.shape)

    fetches[0].wait()
    x = x_ref[...].astype(jnp.float32)
    scale = lax.rsqrt(jnp.mean(x * x, axis=1, keepdims=True) + epsilon)
    normed_ref[...] = (x * scale * in_gain[...].reshape(1, -1)).astype(jnp.bfloat16)
    fetches[1].wait()
    fetches[2].wait()
    both = jnp.dot(normed_ref[...], wkv_ref[...], preferred_element_type=jnp.float32).T
    turned_keys = per_head(both[0:128], columns(key_gain[...])).astype(jnp.bfloat16)
    turned_values = both[128:256].astype(jnp.bfloat16)
    for n in range(kv_heads):
        kvt_ref[n, 0:64] = turned_keys[n * 64 : (n + 1) * 64]
        kvt_ref[n, 64:128] = turned_values[n * 64 : (n + 1) * 64]
    fetches[3].wait()
    decay_ref[...] = sums_ref[...].T * LOG2E

    def far_q_copy(group, pair):
        unit = kv_heads * pair + g
        slot = jnp.minimum(pairs + unit, 2 * pairs - 1)
        return remote(
            query_ref.at[q_lanes(group, pair)], in_q.at[slot],
            q_send.at[group * pairs + pair], q_recv.at[slot], (s_far, group, j),
        )

    def near_q_copy(pair):
        return remote(
            query_ref.at[q_lanes(partner_x, pair)], in_q.at[pair],
            q_send.at[partner_x * pairs + pair], q_recv.at[pair], (s, partner_x, j),
        )

    def q_arrived(slot):
        remote(
            query_ref.at[pl.ds(0, 128)], in_q.at[slot], q_send.at[0], q_recv.at[slot], here
        ).wait_recv()

    def is_given(pair, x_):
        return kv_heads * pair + x_ < given

    def far_sends(act):
        for pair in range(pairs):
            for group in range(kv_heads):

                @pl.when(is_given(pair, g))
                def _():
                    act([far_q_copy(group, pair)])

    def near_sends(act):
        for pair in range(pairs):

            @pl.when(jnp.logical_not(is_given(pair, g)))
            def _():
                act([near_q_copy(pair)])

    def far_decay_copies():
        copies = []
        for x_ in range(kv_heads):
            for n in range(half_count):
                source = decay_ref.at[:, pl.ds((x_ * half_count + n) * rows, rows)]
                at = x_ * half_count + n
                copies.append(
                    remote(
                        source, far_decay.at[x_ * half_count + j], far_send.at[at],
                        far_recv.at[x_ * half_count + j], (s_far, g, n),
                    )
                )
        return copies

    own_block = block_at(s, g, j)
    other_block = block_at(s, partner_x, j)
    member = s * half_count + j

    def side_targets():
        targets = [(None, (s, g, (j + n) % half_count)) for n in range(1, half_count)]
        targets.append((inside(z + 1), ((z + 1) * ys + y, g, j)))
        targets += [(None, (z * ys + (y + n) % ys, g, j)) for n in range(1, ys)]
        return targets

    down = (jnp.where(is_high, zs - 1 - z, jnp.maximum(z - 1, 0)) * ys + y, g, j)
    down_base = (ys + half_count - 1) * each

    def each_side(act):
        for slot, (condition, device) in enumerate(side_targets()):
            if condition is None:
                act(slot * each, device)
            else:

                @pl.when(condition)
                def _():
                    act(slot * each, device)

    def own_copies(base, device):
        return [
            kv_copy(kvt_ref.at[g], own_block, own_send.at[base], device),
            decay_copy(decay_ref, member, own_send.at[base + 1], device),
        ]

    def other_copies(base, device):
        return [kv_copy(kvt_all.at[other_block], other_block, own_send.at[base + 2], device)]

    x_copy = kv_copy(kvt_ref.at[partner_x], own_block, x_send, (s, partner_x, j))
    pl.semaphore_wait(barrier, greeted)
    x_copy.start()
    each_side(lambda base, device: start_all(own_copies(base, device)))

    @pl.when((z > 0) & jnp.logical_not(is_high))
    def _():
        start_all(own_copies(down_base, down))

    fetches[4].wait()
    query_columns = columns(query_gain[...] * (LOG2E * 64 ** (-0.5)))

    def project(n, carry):
        at = pl.ds(pl.multiple_of(n * 256, 256), 256)
        turned = jnp.dot(
            normed_ref[...], wq_ref[:, at], preferred_element_type=jnp.float32
        ).T
        query_ref[at] = per_head(turned, query_columns).astype(jnp.bfloat16)
        return carry

    lax.fori_loop(0, query_ref.shape[0] // 256, project, 0)

    @pl.when(z > zh)
    def _():
        far_sends(start_all)

    @pl.when(is_high)
    def _():
        start_all(own_copies(down_base, down))

    near_sends(start_all)
    kvt_all[own_block] = kvt_ref[g]
    decay_all[member] = decay_ref[...]
    acc_ref[...] = jnp.zeros_like(acc_ref)
    vt_all[:, 64:80] = jnp.ones((sp_count, 16, chunk_rows), jnp.bfloat16)

    def prepare(t, slot, source, pair, decays):
        turned = source
        high = decays.astype(jnp.bfloat16).astype(jnp.float32)
        rest = decays - high
        middle = rest.astype(jnp.bfloat16).astype(jnp.float32)
        rest = rest - middle
        row = lax.broadcasted_iota(jnp.int32, (64, rows), 0)
        for n in range(2):
            head = 2 * pair + n
            lanes = pl.ds(slot * span + n * rows, rows)
            picked = (row == head) | (row == 8 + head) | (row == 16 + head)
            extra = jnp.where(picked, 1.0, 0.0)
            for at, part in ((24, high), (25, middle), (26, rest)):
                extra = jnp.where(row == at, part[n : n + 1], extra)
            qt_ref[t, 0:64, lanes] = turned[n * 64 : (n + 1) * 64]
            qt_ref[t, 64:128, lanes] = extra.astype(jnp.bfloat16)

    def own_decays(pair, x_):
        first = (2 * pair) % local
        at = pl.ds(pl.multiple_of((x_ * half_count + j) * rows, rows), rows)
        return decay_all[s * half_count + (2 * pair) // local, first : first + 2, at]

    def far_decays(slot):
        pair, x_ = slot // kv_heads, slot % kv_heads
        first = (2 * pair) % local
        return far_decay[x_ * half_count + (2 * pair) // local, first : first + 2]

    def work(t, at, lanes, chunk, start, size, step, limit=None):
        at = pl.ds(pl.multiple_of(at, span), lanes)
        q = qt_ref[t, :, at]
        total = acc_ref[t, :, at]
        for b in range(size // step):
            where = pl.ds(pl.multiple_of(start + b * step, step), step)
            scores = jnp.dot(kp_all[chunk, where], q, preferred_element_type=jnp.float32)
            if limit is not None:
                key = lax.broadcasted_iota(jnp.int32, (step, lanes), 0)
                row = lax.broadcasted_iota(jnp.int32, (step, lanes), 1) % rows
                scores = jnp.where(key <= row, scores, -1e30)
            weights = jnp.exp2(scores).astype(jnp.bfloat16)
            total = total + jnp.dot(
                vt_all[chunk, :, where], weights, preferred_element_type=jnp.float32
            )
        acc_ref[t, :, at] = total

    def whole(t, at, lanes, chunk):
        work(t, at, lanes, chunk, 0, chunk_rows, chunk_rows if lanes == span else chunk_rows // 2)

    def sweep(t, at, lanes, low, high):
        def body(chunk, carry):
            whole(t, at, lanes, chunk)
            return carry

        lax.fori_loop(low, high, body, 0)

    def diagonal(t, at, lanes, chunk, offset):
        def body(i, carry):
            work(t, at, lanes, chunk, i * rows, rows, rows)
            return carry

        lax.fori_loop(0, offset // rows, body, 0)
        work(t, at, lanes, chunk, offset, rows, rows, True)

    def finished(t, slot):
        out = []
        for n in range(2):
            lanes = pl.ds(slot * span + n * rows, rows)
            out.append(acc_ref[t, 0:64, lanes] / acc_ref[t, 64:65, lanes])
        return jnp.concatenate(out, axis=0).T.astype(jnp.bfloat16)

    def back_copy(slot, pair, device):
        return remote(
            res_ref.at[slot], att_ref.at[:, q_lanes(g, pair)], back_send.at[slot],
            back_recv.at[g * pairs + pair], device,
        )

    def back_arrived(group, pair):
        remote(
            res_ref.at[0], att_ref.at[:, q_lanes(group, pair)], back_send.at[0],
            back_recv.at[group * pairs + pair], here,
        ).wait_recv()

    def kept_groups(first, act):
        def body(i, carry):
            @pl.when(first <= 2 * i)
            def _():
                act(i * 2 * span, 2 * span)

            @pl.when(first == 2 * i + 1)
            def _():
                act((2 * i + 1) * span, span)

            return carry

        lax.fori_loop(0, pairs // 2, body, 0)

    def taken_groups(act):
        def body(i, carry):
            @pl.when(taken >= 2 * i + 2)
            def _():
                act(i * 2 * span, 2 * span)

            @pl.when(taken == 2 * i + 1)
            def _():
                act(i * 2 * span, span)

            return carry

        lax.fori_loop(0, pairs // 2, body, 0)

    my_first = kept_from(g)
    partner_first = kept_from(partner_x)
    offset = (g * half_count + j) * rows
    partner_offset = (partner_x * half_count + j) * rows

    kv_copy(kvt_ref.at[g], other_block, x_send, here).wait_recv()
    each_side(lambda base, device: start_all(other_copies(base, device)))

    @pl.when(z > 0)
    def _():
        start_all(other_copies(down_base, down))

    @pl.when(z == zh)
    def _():
        far_sends(start_all)

    @pl.when(is_high)
    def _():
        start_all(far_decay_copies())

    for n in range(1, half_count):
        arrived(s, (j + n) % half_count)
    build(s)
    for pair in range(pairs):
        prepare(0, pair, query_ref[q_lanes(g, pair)], pair, own_decays(pair, g))
    kept_groups(my_first, lambda at, lanes: diagonal(0, at, lanes, s, offset))
    round_of(1, True)

    def item(k, carry):
        lanes_of(k)

        @pl.when(k < zs)
        def _():
            round_of(k + 1, True)

        back = jnp.where(y == 0, jnp.where(k == 1, ys, jnp.where(k == ys, 1, k)), k)

        @pl.when(k <= s)
        def _():
            kept_groups(my_first, lambda at, lanes: whole(0, at, lanes, s - back))

        return carry

    lax.fori_loop(1, zs + 1, item, 0)

    @pl.when((z > 0) & (z < zh))
    def _():
        late(zh, True)

    def partner_phase():
        def body(i, carry):
            for n in range(pairs):

                @pl.when((i == n // 2) & (partner_first <= n))
                def _():
                    q_arrived(n)
                    prepare(1, n, in_q[n], n, own_decays(n, partner_x))

            def run(at, lanes):
                diagonal(1, at, lanes, s, partner_offset)
                sweep(1, at, lanes, 0, s)

            @pl.when(partner_first <= 2 * i)
            def _():
                run(i * 2 * span, 2 * span)

            @pl.when(partner_first == 2 * i + 1)
            def _():
                run((2 * i + 1) * span, span)

            for n in range(pairs):

                @pl.when((i == n // 2) & (partner_first <= n))
                def _():
                    res_ref[n] = finished(1, n)
                    back_copy(n, n, (s, partner_x, j)).start()

            @pl.when((i == 0) & (z > 0) & (z < zh))
            def _():
                late_across(zh, True)

            return carry

        lax.fori_loop(0, pairs // 2, body, 0)

    def far_phase():
        for n in range(kv_heads * half_count):
            remote(
                decay_ref.at[:, pl.ds(0, rows)], far_decay.at[n], far_send.at[n],
                far_recv.at[n], here,
            ).wait_recv()

        def body(i, carry):
            for n in range(pairs):

                @pl.when((i == n // 2) & (n < taken))
                def _():
                    q_arrived(pairs + n)
                    prepare(2, n, in_q[pairs + n], n // kv_heads, far_decays(n))

            @pl.when(taken >= 2 * i + 2)
            def _():
                sweep(2, i * 2 * span, 2 * span, 0, upper)

            @pl.when(taken == 2 * i + 1)
            def _():
                sweep(2, i * 2 * span, span, 0, upper)

            @pl.when((z == 0) & (i == 0))
            def _():
                late(zh, True)

            @pl.when((z == 0) & (i == 1))
            def _():
                late_across(zh, True)
                late(zh + 1, True)

            return carry

        lax.fori_loop(0, pairs // 2, body, 0)

    def turn(i, carry):
        @pl.when((i == 0) == (z > 0))
        def _():
            partner_phase()

        @pl.when(((i == 0) == (z == 0)) & (z < zh))
        def _():
            far_phase()

        return carry

    lax.fori_loop(0, 2, turn, 0)

    @pl.when(z < zh)
    def _():
        def zone(zo, carry):
            @pl.when(zo > jnp.where(z == 0, zh + 1, zh))
            def _():
                late(zo, True)
                late_across(zo, True)

            @pl.when((z == 0) & (zo == zh))
            def _():
                late_across(zh + 1, True)

            late_lanes(zo)

            @pl.when(zo < zs - 1 - z)
            def _():
                taken_groups(lambda at, lanes: sweep(2, at, lanes, zo * ys, zo * ys + ys))

            return carry

        lax.fori_loop(zh, zs - z, zone, 0)
        last = (zs - 1 - z) * ys
        taken_groups(lambda at, lanes: sweep(2, at, lanes, last, s_far))

        def close(n, carry):
            unit_x = n % kv_heads
            diagonal(2, n * span, span, s_far, (unit_x * half_count + j) * rows)
            for m in range(pairs):

                @pl.when(n == m)
                def _():
                    res_ref[pairs + m] = finished(2, m)
                    back_copy(
                        pairs + m, m // kv_heads, (s_far, m % kv_heads, j)
                    ).start()

            return carry

        lax.fori_loop(0, taken, close, 0)

    kept_groups(my_first, lambda at, lanes: sweep(0, at, lanes, 0, jnp.maximum(s - zs, 0)))
    for pair in range(pairs):

        @pl.when(pair >= my_first)
        def _():
            att_ref[:, q_lanes(g, pair)] = finished(0, pair)

    x_copy.wait_send()
    each_side(
        lambda base, device: drain_all(own_copies(base, device) + other_copies(base, device))
    )

    @pl.when(z > 0)
    def _():
        drain_all(own_copies(down_base, down) + other_copies(down_base, down))

    def drain(k, carry):
        round_of(k, False)
        return carry

    lax.fori_loop(1, zs + 1, drain, 0)

    def drain_late(zo, carry):
        late(zo, False)
        late_across(zo, False)
        return carry

    @pl.when(z < zh)
    def _():
        lax.fori_loop(zh, zs, drain_late, 0)


    @pl.when(is_high)
    def _():
        far_sends(drain_all)
        drain_all(far_decay_copies())

    near_sends(drain_all)
    for pair in range(pairs):

        @pl.when(partner_first <= pair)
        def _():
            back_copy(pair, pair, (s, partner_x, j)).wait_send()

        @pl.when(pair < taken)
        def _():
            back_copy(
                pairs + pair, pair // kv_heads, (s_far, pair % kv_heads, j)
            ).wait_send()

        back_arrived(partner_x, pair)

        @pl.when(pair < my_first)
        def _():
            back_arrived(g, pair)

    fetches[5].wait()

    def output(n, carry):
        at = pl.ds(pl.multiple_of(n * 512, 512), 512)
        out_ref[:, at] = jnp.dot(
            att_ref[...], wo_ref[:, at], preferred_element_type=jnp.float32
        ).astype(jnp.bfloat16)
        return carry

    lax.fori_loop(0, wo_ref.shape[1] // 512, output, 0)


def lines_of(sp_count):
    ys = 1 << ((sp_count.bit_length() - 1) // 2)
    return sp_count // ys, ys


def stream(
    inputs, in_gain, w_query, w_key, w_value, query_gain, key_gain, decay_sums, w_out, sizes
):
    sp_count, kv_heads, half_count = sizes
    rows, model = inputs.shape
    width = w_query.shape[1]
    heads = width // 64 // kv_heads
    chunk_rows, local = decay_sums.shape
    zs, ys = lines_of(sp_count)
    pairs = heads // 2
    count = sp_count * kv_heads * half_count
    members = sp_count * half_count
    per = 1 + (ys - 1) + (half_count - 1) + (ys - 1) * (half_count - 1)
    each = kv_heads + 1
    vmem = pl.BlockSpec(memory_space=pltpu.VMEM)
    hbm = pl.BlockSpec(memory_space=pltpu.MemorySpace.HBM)
    dma = pltpu.SemaphoreType.DMA
    return pl.pallas_call(
        lambda *refs: stream_kernel(
            *refs, sizes=sizes, lines=(zs, ys), rows=rows, heads=heads
        ),
        out_shape=jax.ShapeDtypeStruct((rows, w_out.shape[1]), jnp.bfloat16),
        in_specs=[hbm, vmem, hbm, hbm, hbm, vmem, vmem, hbm, hbm],
        out_specs=vmem,
        scratch_shapes=[
            pltpu.VMEM((rows, model), jnp.bfloat16),
            pltpu.VMEM((model, 256), jnp.bfloat16),
            pltpu.VMEM(w_query.shape, jnp.bfloat16),
            pltpu.VMEM(decay_sums.shape, jnp.float32),
            pltpu.VMEM(w_out.shape, jnp.bfloat16),
            pltpu.VMEM((rows, model), jnp.bfloat16),
            pltpu.VMEM((kv_heads, 128, rows), jnp.bfloat16),
            pltpu.VMEM((width, rows), jnp.bfloat16),
            pltpu.VMEM((local, chunk_rows), jnp.float32),
            pltpu.VMEM((rows, width), jnp.bfloat16),
            pltpu.VMEM((count, 128, rows), jnp.bfloat16),
            pltpu.VMEM((members, local, chunk_rows), jnp.float32),
            pltpu.VMEM((kv_heads * half_count, local, rows), jnp.float32),
            pltpu.VMEM((2 * pairs, 128, rows), jnp.bfloat16),
            pltpu.VMEM((3, 128, heads * rows), jnp.bfloat16),
            pltpu.VMEM((3, 80, heads * rows), jnp.float32),
            pltpu.VMEM((sp_count, chunk_rows, 128), jnp.bfloat16),
            pltpu.VMEM((sp_count, 80, chunk_rows), jnp.bfloat16),
            pltpu.VMEM((2 * pairs, rows, 128), jnp.bfloat16),
            dma((6,)),
            dma((count,)), dma((members,)), dma, dma(((ys + half_count) * each,)),
            dma((zs * 2 * per * each,)), dma(((zs - zs // 2) * per * each,)),
            dma((kv_heads * half_count,)), dma((kv_heads * half_count,)),
            dma((2 * pairs,)), dma((2 * pairs,)), dma((2 * pairs,)), dma((2 * pairs,)),
        ],
        compiler_params=pltpu.CompilerParams(
            has_side_effects=True, collective_id=0, vmem_limit_bytes=56 * 1024 * 1024
        ),
        name="stream",
    )(inputs, in_gain, w_query, w_key, w_value, query_gain, key_gain, decay_sums, w_out)


def any_scores(queries, kv_blocks, decays, sizes):
    sp_count, kv_heads, half_count = sizes
    group = lax.axis_index("kv")
    me = (lax.axis_index("sp") * kv_heads + group) * half_count + lax.axis_index("half")
    count = sp_count * kv_heads * half_count
    mirror = [(i, count - 1 - i) for i in range(count)]
    rows = queries.shape[0]
    length = rows * count
    heads = queries.shape[1] // 64 // kv_heads
    width = heads * 64
    members = sp_count * half_count
    key_block = math.gcd(length, KEY_BLOCK)

    def choose(a, b):
        return jnp.where(group == 0, a, b)

    decay_rows = decays.reshape(-1, 128)
    own_q = choose(queries[:, :width], queries[:, width:])
    sent_q = choose(queries[:, width:], queries[:, :width])
    vmem = pl.BlockSpec(memory_space=pltpu.VMEM)
    chips = count // 2
    dma = pltpu.SemaphoreType.DMA
    kv, far_q, decay_all = pl.pallas_call(
        lambda *refs: exchange_kernel(*refs, rows=rows, sizes=sizes),
        out_shape=(
            jax.ShapeDtypeStruct((length, 128), jnp.bfloat16),
            jax.ShapeDtypeStruct((rows, width), jnp.bfloat16),
            jax.ShapeDtypeStruct((members, *decay_rows.shape), jnp.float32),
        ),
        in_specs=[vmem] * 3,
        out_specs=(vmem,) * 3,
        scratch_shapes=[
            dma((2,)), dma((chips,)), dma((count,)), dma((chips,)), dma((members // 2,)),
            dma((members,)), dma((members // 2,)), dma, dma,
        ],
        compiler_params=pltpu.CompilerParams(has_side_effects=True),
        name="exchange",
    )(kv_blocks, sent_q, decay_rows)
    decay_all = decay_all.reshape(sp_count, heads, -1, key_block)
    decay_all = decay_all.transpose(0, 2, 1, 3).reshape(length // key_block, heads, key_block)
    firsts = (me * rows, (count - 1 - me) * rows)
    place = jnp.stack(firsts).astype(jnp.int32)
    row_decay = jnp.stack(
        [
            lax.dynamic_slice(
                decay_all, (first // key_block, 0, first % key_block), (1, heads, rows)
            )[0].T
            for first in firsts
        ]
    )
    attended = attend(place, own_q, far_q, row_decay, decay_all, kv, False)
    back = lax.ppermute(attended[1], ALL, mirror)
    return choose(
        jnp.concatenate([attended[0], back], axis=1), jnp.concatenate([back, attended[0]], axis=1)
    )


def any_program(
    inputs, in_gain, w_query, w_key, w_value, query_gain, key_gain, decay_sums, w_out, sizes
):
    kv_heads = sizes[1]
    head_size = query_gain.shape[0]
    rows = inputs.shape[0]
    all_heads = w_query.shape[1] // head_size

    normed = rms_norm(inputs.astype(jnp.float32), in_gain).astype(jnp.bfloat16)
    keys = rms_norm(
        jnp.dot(normed, w_key, preferred_element_type=jnp.float32).reshape(
            rows, kv_heads, head_size
        ),
        key_gain,
    ).astype(jnp.bfloat16)
    values = (
        jnp.dot(normed, w_value, preferred_element_type=jnp.float32)
        .astype(jnp.bfloat16)
        .reshape(rows, kv_heads, head_size)
    )
    kv_blocks = jnp.concatenate([keys, values], axis=2).transpose(1, 0, 2)
    queries = rms_norm(
        jnp.dot(normed, w_query, preferred_element_type=jnp.float32).reshape(
            rows, all_heads, head_size
        ),
        query_gain * (LOG2E * head_size ** (-0.5)),
    ).astype(jnp.bfloat16).reshape(rows, all_heads * head_size)
    whole = any_scores(queries, kv_blocks, decay_sums.T * LOG2E, sizes)
    return jnp.dot(whole, w_out, preferred_element_type=jnp.float32).astype(jnp.bfloat16)


def per_device(*arrays):
    query_gain, key_gain = arrays[5:7]
    sizes = (lax.axis_size("sp"), lax.axis_size("kv"), lax.axis_size("half"))
    bound = query_gain.shape[0] ** 0.5 * LOG2E * jnp.max(query_gain) * jnp.max(key_gain)
    return lax.cond(
        bound <= SMALL,
        lambda *given: stream(*given, sizes),
        lambda *given: any_program(*given, sizes),
        *arrays,
    )


def solution(mesh):
    sp_count, tp_count = mesh.devices.shape
    split = Mesh(mesh.devices.reshape(sp_count, 2, tp_count // 2), ALL)
    placed = (P(ALL, None), P(), P(), P(), P(), P(), P(), P("sp", ("kv", "half")), P())
    return jax.shard_map(
        per_device, mesh=split, in_specs=placed, out_specs=P(ALL, None), check_vma=False
    )
```

```python
import math

import jax
import jax.numpy as jnp
from jax import lax
from jax.experimental import pallas as pl
from jax.experimental.pallas import tpu as pltpu
from jax.sharding import Mesh, PartitionSpec as P

epsilon = 1e-06
LOG2E = math.log2(math.e)
ALL = ("sp", "kv", "half")
HEADS_PER_DOT = 2
KEY_BLOCK = 512
SMALL = 60.0
SPARED = 1


def rms_norm(vector, gain_vec):
    return (
        vector * lax.rsqrt(jnp.mean(vector * vector, axis=-1, keepdims=True) + epsilon) * gain_vec
    )


def exchange_kernel(
    kv_ref, q_ref, decay_ref, kv_out, q_out, decay_out, own_sems, kv_send, kv_recv, kv_relay,
    decay_send, decay_recv, decay_relay, q_send, q_recv, *, rows, sizes
):
    sp_count, kv_heads, half_count = sizes
    sp, group, half = lax.axis_index("sp"), lax.axis_index("kv"), lax.axis_index("half")
    core, chips = half % 2, half_count // 2
    partner = (sp, group, half + 1 - 2 * core)

    def device_of(chip):
        return (chip // (kv_heads * chips), (chip // chips) % kv_heads, (chip % chips) * 2 + core)

    def block_of(place):
        return (place[0] * kv_heads + place[1]) * half_count + place[2]

    def kv_copy(source, block, send, device):
        return pltpu.make_async_remote_copy(
            src_ref=source, dst_ref=kv_out.at[pl.ds(pl.multiple_of(block * rows, rows), rows)],
            send_sem=send, recv_sem=kv_recv.at[block], device_id=device,
            device_id_type=pl.DeviceIdType.MESH,
        )

    def decay_copy(source, member, send, device):
        return pltpu.make_async_remote_copy(
            src_ref=source, dst_ref=decay_out.at[member], send_sem=send,
            recv_sem=decay_recv.at[member], device_id=device,
            device_id_type=pl.DeviceIdType.MESH,
        )

    me = block_of((sp, group, half))
    chip = (sp * kv_heads + group) * chips + half // 2
    total = sp_count * kv_heads * chips
    member = sp * half_count + half
    cluster = sp * chips + half // 2
    clusters = sp_count * chips
    started = []
    for k in range(1, total):
        place = device_of((chip + k) % total)
        started.append(kv_copy(kv_ref.at[place[1]], me, kv_send.at[k], place))
        started[-1].start()
    for k in range(1, clusters):
        other = (cluster + k) % clusters
        place = (other // chips, group, (other % chips) * 2 + core)
        started.append(decay_copy(decay_ref, member, decay_send.at[k], place))
        started[-1].start()
    q_copy = pltpu.make_async_remote_copy(
        src_ref=q_ref, dst_ref=q_out, send_sem=q_send, recv_sem=q_recv,
        device_id=(sp_count - 1 - sp, kv_heads - 1 - group, half_count - 1 - half),
        device_id_type=pl.DeviceIdType.MESH,
    )
    q_copy.start()
    started.append(kv_copy(kv_ref.at[group], me, kv_relay.at[0], partner))
    started[-1].start()
    started.append(decay_copy(decay_ref, member, decay_relay.at[0], partner))
    started[-1].start()
    own_kv = pltpu.make_async_copy(
        kv_ref.at[group], kv_out.at[pl.ds(pl.multiple_of(me * rows, rows), rows)], own_sems.at[0]
    )
    own_kv.start()
    own_decay = pltpu.make_async_copy(decay_ref, decay_out.at[member], own_sems.at[1])
    own_decay.start()
    for k in range(1, clusters):
        other = (cluster + clusters - k) % clusters
        which = (other // chips) * half_count + (other % chips) * 2 + core
        landed = decay_out.at[which]
        relay = decay_copy(landed, which, decay_relay.at[k], partner)
        relay.wait_recv()
        relay.start()
        started.append(relay)
    for k in range(1, total):
        block = block_of(device_of((chip + total - k) % total))
        landed = kv_out.at[pl.ds(pl.multiple_of(block * rows, rows), rows)]
        relay = kv_copy(landed, block, kv_relay.at[k], partner)
        relay.wait_recv()
        relay.start()
        started.append(relay)
    for k in range(clusters):
        other = (cluster + clusters - k) % clusters
        which = (other // chips) * half_count + (other % chips) * 2 + 1 - core
        decay_copy(decay_out.at[which], which, decay_relay.at[k], partner).wait_recv()
    for k in range(total):
        place = device_of((chip + total - k) % total)
        block = block_of((place[0], place[1], place[2] + 1 - 2 * core))
        landed = kv_out.at[pl.ds(pl.multiple_of(block * rows, rows), rows)]
        kv_copy(landed, block, kv_relay.at[k], partner).wait_recv()
    for copy in started:
        copy.wait_send()
    own_kv.wait()
    own_decay.wait()
    q_copy.wait()


def attend_kernel(
    place_ref, near_ref, far_ref, row_ref, decay_ref, kv_ref, out_ref, ones_ref, q_ref, peak_ref,
    acc_ref, *, rows, heads, key_block, small
):
    lane = lax.broadcasted_iota(jnp.int32, (rows, 128), 1)
    low = lane < 64
    for r, ref in enumerate((near_ref, far_ref)):
        for pair in range(heads // 2):
            both = ref[:, pair * 128 : (pair + 1) * 128].astype(jnp.float32)
            even = jnp.where(low, both, 0.0)
            odd = jnp.where(low, pltpu.roll(both, 64, 1), 0.0)
            q_ref[r, (2 * pair) * rows : (2 * pair + 1) * rows] = even.astype(jnp.bfloat16)
            q_ref[r, (2 * pair + 1) * rows : (2 * pair + 2) * rows] = odd.astype(jnp.bfloat16)

    def fill(i, carry):
        at = pl.ds(pl.multiple_of(i * key_block, key_block), key_block)
        wide = lax.broadcasted_iota(jnp.int32, (key_block, 128), 1) < 64
        ones_ref[at] = jnp.where(wide, 1.0, kv_ref[at].astype(jnp.float32)).astype(jnp.bfloat16)
        return carry

    lax.fori_loop(0, kv_ref.shape[0] // key_block, fill, 0)
    span = HEADS_PER_DOT * rows

    for r in range(2):
        first = place_ref[r]
        for head in range(heads):
            part = pl.ds(head * rows, rows)
            if small:
                peak_ref[part] = jnp.broadcast_to(row_ref[r, :, head : head + 1], (rows, 128))
            else:
                peak_ref[part] = jnp.full((rows, 128), -1e30, jnp.float32)
        acc_ref[...] = jnp.zeros_like(acc_ref)

        def step(index, masked):
            at = pl.ds(pl.multiple_of(index * key_block, key_block), key_block)
            keys = kv_ref[at]
            values = ones_ref[at]
            for start in range(0, heads, HEADS_PER_DOT):
                part = pl.ds(start * rows, span)
                before = peak_ref[part]
                scores = lax.dot_general(
                    q_ref[r, part], keys, (((1,), (1,)), ((), ())),
                    preferred_element_type=jnp.float32,
                )
                if small:
                    scores = scores + jnp.concatenate([before] * (key_block // 128), axis=1)
                scores = scores.reshape(HEADS_PER_DOT, rows, key_block)
                scores = scores - decay_ref[index, start : start + HEADS_PER_DOT][:, None, :]
                if masked:
                    row = first + lax.broadcasted_iota(jnp.int32, (rows, key_block), 0)
                    col = index * key_block + lax.broadcasted_iota(
                        jnp.int32, (rows, key_block), 1
                    )
                    scores = jnp.where((col <= row)[None], scores, -1e30)
                scores = scores.reshape(span, key_block)
                if small:
                    weights = jnp.exp2(scores).astype(jnp.bfloat16)
                    acc_ref[part] += jnp.dot(weights, values, preferred_element_type=jnp.float32)
                else:
                    after = jnp.maximum(before, jnp.max(scores, axis=1, keepdims=True))
                    weights = jnp.exp2(scores - after[:, :1]).astype(jnp.bfloat16)
                    acc_ref[part] = acc_ref[part] * jnp.exp2(before - after) + jnp.dot(
                        weights, values, preferred_element_type=jnp.float32
                    )
                    peak_ref[part] = after

        full = first // key_block

        def body(index, carry):
            step(index, False)
            return carry

        lax.fori_loop(0, full, body, 0)
        step(full, True)
        for pair in range(heads // 2):
            even = acc_ref[(2 * pair) * rows : (2 * pair + 1) * rows]
            odd = acc_ref[(2 * pair + 1) * rows : (2 * pair + 2) * rows]
            done = jnp.where(low, pltpu.roll(even, 64, 1), odd) / jnp.where(
                low, even, pltpu.roll(odd, 64, 1)
            )
            out_ref[r, :, pair * 128 : (pair + 1) * 128] = done.astype(jnp.bfloat16)


def attend(place, near, far, row_decay, decays, kv, small):
    length = kv.shape[0]
    rows, width = near.shape
    heads, key_block = decays.shape[1:]
    vmem = pl.BlockSpec(memory_space=pltpu.VMEM)
    return pl.pallas_call(
        lambda *refs: attend_kernel(
            *refs, rows=rows, heads=heads, key_block=key_block, small=small
        ),
        out_shape=jax.ShapeDtypeStruct((2, rows, width), jnp.bfloat16),
        in_specs=[pl.BlockSpec(memory_space=pltpu.SMEM)] + [vmem] * 5,
        out_specs=vmem,
        scratch_shapes=[
            pltpu.VMEM((length, 128), jnp.bfloat16),
            pltpu.VMEM((2, heads * rows, 128), jnp.bfloat16),
            pltpu.VMEM((heads * rows, 128), jnp.float32),
            pltpu.VMEM((heads * rows, 128), jnp.float32),
        ],
        compiler_params=pltpu.CompilerParams(vmem_limit_bytes=40 * 1024 * 1024),
        name="attend_small" if small else "attend_any",
    )(place, near, far, row_decay, decays, kv)


def stream_kernel(
    x_hbm, in_gain, wq_hbm, wk_hbm, wv_hbm, query_gain, key_gain, sums_hbm, wo_hbm, out_ref,
    x_ref, wkv_ref, wq_ref, sums_ref, wo_ref, normed_ref, kvt_ref, query_ref, decay_ref, att_ref,
    kvt_all, decay_all, far_decay, in_q, qt_ref, acc_ref, kp_all, vt_all, res_ref, done_ref, loads, kv_recv,
    decay_recv, x_send, own_send, round_send, late_send, far_send, far_recv, q_send, q_recv,
    back_send, back_recv, *, sizes, lines, rows, heads
):
    sp_count, kv_heads, half_count = sizes
    zs, ys = lines
    zh = zs // 2
    upper = sp_count // 2
    pairs = heads // 2
    units = pairs * kv_heads
    width = heads * 64
    span = 2 * rows
    local, chunk_rows = decay_ref.shape
    s, g, j = lax.axis_index("sp"), lax.axis_index("kv"), lax.axis_index("half")
    z, y = s // ys, s % ys
    partner_x = 1 - g
    s_far = sp_count - 1 - s
    is_high = s >= upper

    def share(s_):
        even = (2 * units * (2 * s_ + 1 - sp_count) + 2 * s_ + 1) // (2 * (2 * s_ + 1))
        return jnp.maximum(even - SPARED, 0)

    given = jnp.where(is_high, share(jnp.maximum(s, upper)), 0)
    taken = jnp.where(is_high, 0, share(jnp.maximum(s_far, upper)))

    def kept_from(x_):
        return (jnp.maximum(given - x_, 0) + kv_heads - 1) // kv_heads

    def block_at(s_, x_, j_):
        return (s_ * kv_heads + x_) * half_count + j_

    def remote(source, target, send, recv, device):
        return pltpu.make_async_remote_copy(
            src_ref=source, dst_ref=target, send_sem=send, recv_sem=recv, device_id=device,
            device_id_type=pl.DeviceIdType.MESH,
        )

    def kv_copy(source, block, send, device):
        return remote(source, kvt_all.at[block], send, kv_recv.at[block], device)

    def decay_copy(source, member, send, device):
        return remote(source, decay_all.at[member], send, decay_recv.at[member], device)

    here = (s, g, j)
    each = kv_heads + 1

    def one_piece(s_, j_, piece, base, device, sems):
        if piece == kv_heads:
            member = s_ * half_count + j_
            return decay_copy(decay_all.at[member], member, sems.at[base + piece], device)
        block = block_at(s_, piece, j_)
        return kv_copy(kvt_all.at[block], block, sems.at[base + piece], device)

    def arrived(s_, j_):
        for piece in range(each):
            one_piece(s_, j_, piece, 0, here, own_send).wait_recv()

    def start_all(copies):
        for copy in copies:
            copy.start()

    def drain_all(copies):
        for copy in copies:
            copy.wait_send()

    def inside(z_):
        return (z_ >= 0) & (z_ < zs)

    def to_rows(base):
        return [
            (None, base + (n - 1) * each, (z * ys + (y + n) % ys, g, j)) for n in range(1, ys)
        ]

    def to_lanes(base):
        return [
            (None, base + (n - 1) * each, (s, g, (j + n) % half_count))
            for n in range(1, half_count)
        ]

    def relay(s_, routes, sems, go):
        for piece in range(each):
            if go:
                one_piece(s_, j, piece, 0, here, own_send).wait_recv()
            for condition, base, device in routes:
                copy = one_piece(s_, j, piece, base, device, sems)
                act = copy.start if go else copy.wait_send
                if condition is None:
                    act()
                else:
                    pl.when(condition)(act)

    per = 1 + (ys - 1) + (half_count - 1) + (ys - 1) * (half_count - 1)

    def spread(s_, base, condition, device, sems, go):
        routes = [(condition, base, device)]
        routes += to_rows(base + each) + to_lanes(base + ys * each)
        relay(s_, routes, sems, go)

    def across(zo, base, sems, go):
        for m in range(1, ys):
            slot = ys + half_count - 1 + (m - 1) * (half_count - 1)
            relay(zo * ys + (y + m) % ys, to_lanes(base + slot * each), sems, go)

    def round_of(k, go):
        base = (k - 1) * per * each

        @pl.when(inside(z - k))
        def _():
            spread(
                (z - k) * ys + y, base, inside(z + 1), ((z + 1) * ys + y, g, j), round_send, go
            )

        @pl.when(inside(z - k + 1))
        def _():
            across(z - k + 1, base, round_send, go)

    def late(zo, go):
        base = (zo - 1) * per * each
        routes = to_rows(base + each) + to_lanes(base + ys * each)
        relay(zo * ys + y, routes, late_send, go)

    def late_across(zo, go):
        across(zo, (zo - 1) * per * each, late_send, go)

    def build(s_):
        for x_ in range(kv_heads):
            for j_ in range(half_count):
                block = block_at(s_, x_, j_)
                place = (x_ * half_count + j_) * rows
                decays = jnp.concatenate(
                    [
                        decay_all[s_ * half_count + n, :, pl.ds(place, rows)]
                        for n in range(half_count)
                    ],
                    axis=0,
                )
                decays = -decays
                high = decays.astype(jnp.bfloat16).astype(jnp.float32)
                rest = decays - high
                middle = rest.astype(jnp.bfloat16).astype(jnp.float32)
                parts = jnp.concatenate(
                    [high, middle, rest - middle, jnp.ones((8, rows), jnp.float32)], axis=0
                ).astype(jnp.bfloat16)
                wide = jnp.concatenate(
                    [kvt_all[block, 0:64], parts, jnp.zeros((32, rows), jnp.bfloat16)], axis=0
                )
                kp_all[s_, pl.ds(place, rows)] = wide.T
                vt_all[s_, 0:64, pl.ds(place, rows)] = kvt_all[block, 64:128]

    def build_if(s_):
        @pl.when(s_ <= jnp.where(is_high, s, s_far))
        def _():
            build(s_)

    def lanes_of(k):
        @pl.when(inside(z - k))
        def _():
            s_ = (z - k) * ys + y
            for n in range(1, half_count):
                arrived(s_, (j + n) % half_count)
            build_if(s_)

        @pl.when(inside(z - k + 1))
        def _():
            for m in range(1, ys):
                s_ = (z - k + 1) * ys + (y + m) % ys
                for n in range(1, half_count):
                    arrived(s_, (j + n) % half_count)
                build_if(s_)

    def late_lanes(zo):
        for m in range(ys):
            s_ = zo * ys + (y + m) % ys
            for n in range(1, half_count):
                arrived(s_, (j + n) % half_count)
            build_if(s_)

    def q_lanes(group, pair):
        return pl.ds(pl.multiple_of(group * width + pair * 128, 128), 128)

    fetches = [
        pltpu.make_async_copy(source, target, loads.at[n])
        for n, (source, target) in enumerate(
            (
                (x_hbm, x_ref), (wk_hbm, wkv_ref.at[:, 0:128]), (wv_hbm, wkv_ref.at[:, 128:256]),
                (sums_hbm, sums_ref), (wq_hbm, wq_ref), (wo_hbm, wo_ref),
            )
        )
    ]
    for fetch in fetches:
        fetch.start()

    barrier = pltpu.get_barrier_semaphore()

    def greet(device):
        pl.semaphore_signal(
            barrier, inc=1, device_id=device, device_id_type=pl.DeviceIdType.MESH
        )

    greeted = 0
    for n in range(1, half_count):
        greet((s, g, (j + n) % half_count))
        greeted += 1
    greet((s, partner_x, j))
    greeted += 1
    for z_ in range(zs):
        met = ((z_ < z) & (z_ <= zs - 1 - z)) | ((z < z_) & (z <= zs - 1 - z_))

        @pl.when(met)
        def _():
            greet((z_ * ys + y, g, j))

        greeted = greeted + jnp.where(met, 1, 0)
    for n in range(1, ys):
        greet((z * ys + (y + n) % ys, g, j))
        greeted += 1
    for x_ in range(kv_heads):
        for n in range(half_count):
            greet((s_far, x_, n))
            greeted += 1
    for way in (1, -1):

        @pl.when(inside(z + way))
        def _():
            greet(((z + way) * ys + y, g, j))

        greeted = greeted + jnp.where(inside(z + way), 1, 0)

    def columns(gain):
        wide = jnp.broadcast_to(gain.reshape(1, 64), (64, 64))
        wide = jnp.concatenate([wide, wide], axis=1)
        wide = jnp.concatenate([wide, wide], axis=0).T
        return jnp.concatenate([wide[0:64]] * (rows // 128), axis=1)

    def per_head(turned, gain):
        many = turned.reshape(turned.shape[0] // 64, 64, rows)
        mean = jnp.mean(many * many, axis=1, keepdims=True)
        return (many * lax.rsqrt(mean + epsilon) * gain[None]).reshape(turned.shape)

    fetches[0].wait()
    x = x_ref[...].astype(jnp.float32)
    scale = lax.rsqrt(jnp.mean(x * x, axis=1, keepdims=True) + epsilon)
    normed_ref[...] = (x * scale * in_gain[...].reshape(1, -1)).astype(jnp.bfloat16)
    fetches[1].wait()
    fetches[2].wait()
    both = jnp.dot(normed_ref[...], wkv_ref[...], preferred_element_type=jnp.float32).T
    turned_keys = per_head(both[0:128], columns(key_gain[...])).astype(jnp.bfloat16)
    turned_values = both[128:256].astype(jnp.bfloat16)
    for n in range(kv_heads):
        kvt_ref[n, 0:64] = turned_keys[n * 64 : (n + 1) * 64]
        kvt_ref[n, 64:128] = turned_values[n * 64 : (n + 1) * 64]
    fetches[3].wait()
    decay_ref[...] = sums_ref[...] * LOG2E

    def far_q_copy(group, pair):
        unit = kv_heads * pair + g
        slot = jnp.minimum(pairs + unit, 2 * pairs - 1)
        return remote(
            query_ref.at[q_lanes(group, pair)], in_q.at[slot],
            q_send.at[group * pairs + pair], q_recv.at[slot], (s_far, group, j),
        )

    def near_q_copy(pair):
        return remote(
            query_ref.at[q_lanes(partner_x, pair)], in_q.at[pair],
            q_send.at[partner_x * pairs + pair], q_recv.at[pair], (s, partner_x, j),
        )

    def q_arrived(slot):
        remote(
            query_ref.at[pl.ds(0, 128)], in_q.at[slot], q_send.at[0], q_recv.at[slot], here
        ).wait_recv()

    def is_given(pair, x_):
        return kv_heads * pair + x_ < given

    def far_sends(act):
        for pair in range(pairs):
            for group in range(kv_heads):

                @pl.when(is_given(pair, g))
                def _():
                    act([far_q_copy(group, pair)])

    def near_sends(act):
        for pair in range(pairs):

            @pl.when(jnp.logical_not(is_given(pair, g)))
            def _():
                act([near_q_copy(pair)])

    def far_decay_copies():
        copies = []
        for x_ in range(kv_heads):
            for n in range(half_count):
                source = decay_ref.at[:, pl.ds((x_ * half_count + n) * rows, rows)]
                at = x_ * half_count + n
                copies.append(
                    remote(
                        source, far_decay.at[x_ * half_count + j], far_send.at[at],
                        far_recv.at[x_ * half_count + j], (s_far, g, n),
                    )
                )
        return copies

    own_block = block_at(s, g, j)
    other_block = block_at(s, partner_x, j)
    member = s * half_count + j

    def side_targets():
        targets = [(None, (s, g, (j + n) % half_count)) for n in range(1, half_count)]
        targets.append((inside(z + 1), ((z + 1) * ys + y, g, j)))
        targets += [(None, (z * ys + (y + n) % ys, g, j)) for n in range(1, ys)]
        return targets

    def each_down(act):
        for z_ in range(zh - 1, -1, -1):

            @pl.when((z_ < z) & (z_ <= zs - 1 - z))
            def _():
                act((ys + half_count - 1 + z_) * each, (z_ * ys + y, g, j))

    def each_side(act):
        for slot, (condition, device) in enumerate(side_targets()):
            if condition is None:
                act(slot * each, device)
            else:

                @pl.when(condition)
                def _():
                    act(slot * each, device)

    def own_copies(base, device):
        return [
            kv_copy(kvt_ref.at[g], own_block, own_send.at[base], device),
            decay_copy(decay_ref, member, own_send.at[base + 1], device),
        ]

    def other_copies(base, device):
        return [kv_copy(kvt_all.at[other_block], other_block, own_send.at[base + 2], device)]

    x_copy = kv_copy(kvt_ref.at[partner_x], own_block, x_send, (s, partner_x, j))
    pl.semaphore_wait(barrier, greeted)
    x_copy.start()
    each_side(lambda base, device: start_all(own_copies(base, device)))

    @pl.when(z <= zh)
    def _():
        each_down(lambda base, device: start_all(own_copies(base, device)))

    fetches[4].wait()
    query_columns = columns(query_gain[...] * (LOG2E * 64 ** (-0.5)))

    def project(n, carry):
        at = pl.ds(pl.multiple_of(n * 512, 512), 512)
        turned = jnp.dot(
            normed_ref[...], wq_ref[:, at], preferred_element_type=jnp.float32
        ).T
        query_ref[at] = per_head(turned, query_columns).astype(jnp.bfloat16)
        return carry

    lax.fori_loop(0, query_ref.shape[0] // 512, project, 0)

    @pl.when(z > zh)
    def _():
        far_sends(start_all)

    near_sends(start_all)
    kvt_all[own_block] = kvt_ref[g]
    decay_all[member] = decay_ref[...]
    acc_ref[...] = jnp.zeros_like(acc_ref)
    vt_all[:, 64:80] = jnp.ones((sp_count, 16, chunk_rows), jnp.bfloat16)

    def prepare(t, slot, source, pair, decays):
        turned = source
        high = decays.astype(jnp.bfloat16).astype(jnp.float32)
        rest = decays - high
        middle = rest.astype(jnp.bfloat16).astype(jnp.float32)
        rest = rest - middle
        row = lax.broadcasted_iota(jnp.int32, (64, rows), 0)
        for n in range(2):
            head = 2 * pair + n
            lanes = pl.ds(slot * span + n * rows, rows)
            picked = (row == head) | (row == 8 + head) | (row == 16 + head)
            extra = jnp.where(picked, 1.0, 0.0)
            for at, part in ((24, high), (25, middle), (26, rest)):
                extra = jnp.where(row == at, part[n : n + 1], extra)
            qt_ref[t, 0:64, lanes] = turned[n * 64 : (n + 1) * 64]
            qt_ref[t, 64:128, lanes] = extra.astype(jnp.bfloat16)

    def own_decays(pair, x_):
        first = (2 * pair) % local
        at = pl.ds(pl.multiple_of((x_ * half_count + j) * rows, rows), rows)
        return decay_all[s * half_count + (2 * pair) // local, first : first + 2, at]

    def far_decays(slot):
        pair, x_ = slot // kv_heads, slot % kv_heads
        first = (2 * pair) % local
        return far_decay[x_ * half_count + (2 * pair) // local, first : first + 2]

    def work(t, at, lanes, chunk, start, size, step, limit=None):
        at = pl.ds(pl.multiple_of(at, span), lanes)
        q = qt_ref[t, :, at]
        total = acc_ref[t, :, at]
        for b in range(size // step):
            where = pl.ds(pl.multiple_of(start + b * step, step), step)
            scores = jnp.dot(kp_all[chunk, where], q, preferred_element_type=jnp.float32)
            if limit is not None:
                key = lax.broadcasted_iota(jnp.int32, (step, lanes), 0)
                row = lax.broadcasted_iota(jnp.int32, (step, lanes), 1) % rows
                scores = jnp.where(key <= row, scores, -1e30)
            weights = jnp.exp2(scores).astype(jnp.bfloat16)
            total = total + jnp.dot(
                vt_all[chunk, :, where], weights, preferred_element_type=jnp.float32
            )
        acc_ref[t, :, at] = total

    def whole(t, at, lanes, chunk):
        work(t, at, lanes, chunk, 0, chunk_rows, chunk_rows if lanes == span else chunk_rows // 2)

    def sweep(t, at, lanes, low, high):
        def body(chunk, carry):
            whole(t, at, lanes, chunk)
            return carry

        lax.fori_loop(low, high, body, 0)

    def diagonal(t, at, lanes, chunk, offset):
        def body(i, carry):
            work(t, at, lanes, chunk, i * rows, rows, rows)
            return carry

        lax.fori_loop(0, offset // rows, body, 0)
        work(t, at, lanes, chunk, offset, rows, rows, True)

    def finished(t, slot):
        out = []
        for n in range(2):
            lanes = pl.ds(slot * span + n * rows, rows)
            out.append(acc_ref[t, 0:64, lanes] / acc_ref[t, 64:65, lanes])
        return jnp.concatenate(out, axis=0).T.astype(jnp.bfloat16)

    def back_copy(slot, pair, device):
        return remote(
            res_ref.at[slot], att_ref.at[:, q_lanes(g, pair)], back_send.at[slot],
            back_recv.at[g * pairs + pair], device,
        )

    def back_arrived(group, pair):
        remote(
            res_ref.at[0], att_ref.at[:, q_lanes(group, pair)], back_send.at[0],
            back_recv.at[group * pairs + pair], here,
        ).wait_recv()

    def kept_groups(first, act):
        def body(i, carry):
            @pl.when(first <= 2 * i)
            def _():
                act(i * 2 * span, 2 * span)

            @pl.when(first == 2 * i + 1)
            def _():
                act((2 * i + 1) * span, span)

            return carry

        lax.fori_loop(0, pairs // 2, body, 0)

    def taken_groups(act):
        def body(i, carry):
            @pl.when(taken >= 2 * i + 2)
            def _():
                act(i * 2 * span, 2 * span)

            @pl.when(taken == 2 * i + 1)
            def _():
                act(i * 2 * span, span)

            return carry

        lax.fori_loop(0, pairs // 2, body, 0)

    my_first = kept_from(g)
    partner_first = kept_from(partner_x)
    offset = (g * half_count + j) * rows
    partner_offset = (partner_x * half_count + j) * rows

    kv_copy(kvt_ref.at[g], other_block, x_send, here).wait_recv()
    each_side(lambda base, device: start_all(other_copies(base, device)))

    @pl.when(z <= zh)
    def _():
        each_down(lambda base, device: start_all(other_copies(base, device)))

    @pl.when(z == zh)
    def _():
        far_sends(start_all)

    @pl.when(is_high)
    def _():
        start_all(far_decay_copies())

    for n in range(1, half_count):
        arrived(s, (j + n) % half_count)
    build(s)
    for pair in range(pairs):
        prepare(0, pair, query_ref[q_lanes(g, pair)], pair, own_decays(pair, g))
    kept_groups(my_first, lambda at, lanes: diagonal(0, at, lanes, s, offset))
    round_of(1, True)

    def at_step(k):
        return s - jnp.where(y == 0, jnp.where(k == 1, ys, jnp.where(k == ys, 1, k)), k)

    def comes(zo):
        return (z < zh) & (zo > z) & (zo <= zs - 1 - z)

    def item(k, carry):
        @pl.when((k == 2) & (z > zh))
        def _():
            each_down(
                lambda base, device: start_all(
                    own_copies(base, device) + other_copies(base, device)
                )
            )

        lanes_of(k)

        @pl.when(k <= s)
        def _():
            kept_groups(my_first, lambda at, lanes: whole(0, at, lanes, at_step(k)))

        @pl.when(k < zs)
        def _():
            round_of(k + 1, True)

        for step, duty, zo in ((2, late, z + 1), (3, late_across, z + 1), (4, late, z + 2)):

            @pl.when((k == step) & comes(zo))
            def _():
                duty(zo, True)

        @pl.when(k == 2)
        def _():
            for n in range(pairs):

                @pl.when(partner_first <= n)
                def _():
                    q_arrived(n)
                    prepare(1, n, in_q[n], n, own_decays(n, partner_x))

            kept_groups(
                partner_first, lambda at, lanes: diagonal(1, at, lanes, s, partner_offset)
            )

        @pl.when((k > 2) & (k - 2 <= s))
        def _():
            kept_groups(partner_first, lambda at, lanes: whole(1, at, lanes, at_step(k - 2)))

        return carry

    lax.fori_loop(1, zs + 1, item, 0)

    def partner_phase():
        def body(i, carry):
            def run(at, lanes):
                def body(k, carry):
                    whole(1, at, lanes, at_step(k))
                    return carry

                lax.fori_loop(zs - 1, jnp.minimum(s, zs) + 1, body, 0)
                sweep(1, at, lanes, 0, jnp.maximum(s - zs, 0))

            @pl.when(partner_first <= 2 * i)
            def _():
                run(i * 2 * span, 2 * span)

            @pl.when(partner_first == 2 * i + 1)
            def _():
                run((2 * i + 1) * span, span)

            for n in range(pairs):

                @pl.when((i == n // 2) & (partner_first <= n))
                def _():
                    res_ref[n] = finished(1, n)
                    back_copy(n, n, (s, partner_x, j)).start()

            return carry

        lax.fori_loop(0, pairs // 2, body, 0)

    def far_phase():
        for n in range(kv_heads * half_count):
            remote(
                decay_ref.at[:, pl.ds(0, rows)], far_decay.at[n], far_send.at[n],
                far_recv.at[n], here,
            ).wait_recv()

        for n in range(pairs):

            @pl.when(n < taken)
            def _():
                q_arrived(pairs + n)
                prepare(2, n, in_q[pairs + n], n // kv_heads, far_decays(n))

        def zone(zo, carry):
            high = jnp.minimum(zo * ys + ys, s_far)

            def body(i, carry):
                @pl.when(taken >= 2 * i + 2)
                def _():
                    sweep(2, i * 2 * span, 2 * span, zo * ys, high)

                @pl.when(taken == 2 * i + 1)
                def _():
                    sweep(2, i * 2 * span, span, zo * ys, high)

                for turn, ahead, duty, zl in (
                    (0, 0, late_across, z + 2), (1, 0, late, z + 3), (0, 1, late_across, z + 3),
                ):

                    @pl.when((i == turn) & (zo == z + ahead) & comes(zl))
                    def _():
                        duty(zl, True)

                return carry

            lax.fori_loop(0, pairs // 2, body, 0)

            @pl.when(comes(zo + 1) & (zo > z + 2))
            def _():
                late(zo + 1, True)
                late_across(zo + 1, True)

            @pl.when(comes(zo + 1))
            def _():
                late_lanes(zo + 1)

            return carry

        lax.fori_loop(0, zs - z, zone, 0)

        def close(n, carry):
            unit_x = n % kv_heads
            diagonal(2, n * span, span, s_far, (unit_x * half_count + j) * rows)
            for m in range(pairs):

                @pl.when(n == m)
                def _():
                    res_ref[pairs + m] = finished(2, m)
                    back_copy(
                        pairs + m, m // kv_heads, (s_far, m % kv_heads, j)
                    ).start()

            return carry

        lax.fori_loop(0, taken, close, 0)

    partner_phase()

    @pl.when(z < zh)
    def _():
        far_phase()

    kept_groups(my_first, lambda at, lanes: sweep(0, at, lanes, 0, jnp.maximum(s - zs, 0)))
    for pair in range(pairs):

        @pl.when(pair >= my_first)
        def _():
            att_ref[:, q_lanes(g, pair)] = finished(0, pair)

    x_copy.wait_send()
    each_side(
        lambda base, device: drain_all(own_copies(base, device) + other_copies(base, device))
    )

    each_down(
        lambda base, device: drain_all(own_copies(base, device) + other_copies(base, device))
    )

    def drain(k, carry):
        round_of(k, False)
        return carry

    lax.fori_loop(1, zs + 1, drain, 0)

    def drain_late(zo, carry):
        late(zo, False)
        late_across(zo, False)
        return carry

    @pl.when(z < zh)
    def _():
        lax.fori_loop(z + 1, zs - z, drain_late, 0)


    @pl.when(is_high)
    def _():
        far_sends(drain_all)
        drain_all(far_decay_copies())

    near_sends(drain_all)
    for pair in range(pairs):

        @pl.when(partner_first <= pair)
        def _():
            back_copy(pair, pair, (s, partner_x, j)).wait_send()

        @pl.when(pair < taken)
        def _():
            back_copy(
                pairs + pair, pair // kv_heads, (s_far, pair % kv_heads, j)
            ).wait_send()

        back_arrived(partner_x, pair)

        @pl.when(pair < my_first)
        def _():
            back_arrived(g, pair)

    fetches[5].wait()

    model = wo_ref.shape[1]
    half = model // 2
    puts = []
    for n in range(2):
        at = pl.ds(n * half, half)
        done_ref[:, at] = jnp.dot(
            att_ref[...], wo_ref[:, at], preferred_element_type=jnp.float32
        ).astype(jnp.bfloat16)
        puts.append(pltpu.make_async_copy(done_ref.at[:, at], out_ref.at[:, at], loads.at[n]))
        puts[n].start()
    for put in puts:
        put.wait()


def lines_of(sp_count):
    ys = 1 << ((sp_count.bit_length() - 1) // 2)
    return sp_count // ys, ys


def stream(
    inputs, in_gain, w_query, w_key, w_value, query_gain, key_gain, decay_sums, w_out, sizes
):
    sp_count, kv_heads, half_count = sizes
    rows, model = inputs.shape
    width = w_query.shape[1]
    heads = width // 64 // kv_heads
    local, chunk_rows = decay_sums.shape
    zs, ys = lines_of(sp_count)
    pairs = heads // 2
    count = sp_count * kv_heads * half_count
    members = sp_count * half_count
    per = 1 + (ys - 1) + (half_count - 1) + (ys - 1) * (half_count - 1)
    each = kv_heads + 1
    vmem = pl.BlockSpec(memory_space=pltpu.VMEM)
    hbm = pl.BlockSpec(memory_space=pltpu.MemorySpace.HBM)
    dma = pltpu.SemaphoreType.DMA
    return pl.pallas_call(
        lambda *refs: stream_kernel(
            *refs, sizes=sizes, lines=(zs, ys), rows=rows, heads=heads
        ),
        out_shape=jax.ShapeDtypeStruct((rows, w_out.shape[1]), jnp.bfloat16),
        in_specs=[hbm, vmem, hbm, hbm, hbm, vmem, vmem, hbm, hbm],
        out_specs=hbm,
        scratch_shapes=[
            pltpu.VMEM((rows, model), jnp.bfloat16),
            pltpu.VMEM((model, 256), jnp.bfloat16),
            pltpu.VMEM(w_query.shape, jnp.bfloat16),
            pltpu.VMEM(decay_sums.shape, jnp.float32),
            pltpu.VMEM(w_out.shape, jnp.bfloat16),
            pltpu.VMEM((rows, model), jnp.bfloat16),
            pltpu.VMEM((kv_heads, 128, rows), jnp.bfloat16),
            pltpu.VMEM((width, rows), jnp.bfloat16),
            pltpu.VMEM((local, chunk_rows), jnp.float32),
            pltpu.VMEM((rows, width), jnp.bfloat16),
            pltpu.VMEM((count, 128, rows), jnp.bfloat16),
            pltpu.VMEM((members, local, chunk_rows), jnp.float32),
            pltpu.VMEM((kv_heads * half_count, local, rows), jnp.float32),
            pltpu.VMEM((2 * pairs, 128, rows), jnp.bfloat16),
            pltpu.VMEM((3, 128, heads * rows), jnp.bfloat16),
            pltpu.VMEM((3, 80, heads * rows), jnp.float32),
            pltpu.VMEM((sp_count, chunk_rows, 128), jnp.bfloat16),
            pltpu.VMEM((sp_count, 80, chunk_rows), jnp.bfloat16),
            pltpu.VMEM((2 * pairs, rows, 128), jnp.bfloat16),
            pltpu.VMEM((rows, w_out.shape[1]), jnp.bfloat16),
            dma((6,)),
            dma((count,)), dma((members,)), dma, dma(((ys + half_count + zs // 2) * each,)),
            dma((zs * per * each,)), dma((zs * per * each,)),
            dma((kv_heads * half_count,)), dma((kv_heads * half_count,)),
            dma((2 * pairs,)), dma((2 * pairs,)), dma((2 * pairs,)), dma((2 * pairs,)),
        ],
        compiler_params=pltpu.CompilerParams(
            has_side_effects=True, collective_id=0, vmem_limit_bytes=56 * 1024 * 1024
        ),
        name="stream",
    )(inputs, in_gain, w_query, w_key, w_value, query_gain, key_gain, decay_sums, w_out)


def any_scores(queries, kv_blocks, decays, sizes):
    sp_count, kv_heads, half_count = sizes
    group = lax.axis_index("kv")
    me = (lax.axis_index("sp") * kv_heads + group) * half_count + lax.axis_index("half")
    count = sp_count * kv_heads * half_count
    mirror = [(i, count - 1 - i) for i in range(count)]
    rows = queries.shape[0]
    length = rows * count
    heads = queries.shape[1] // 64 // kv_heads
    width = heads * 64
    members = sp_count * half_count
    key_block = math.gcd(length, KEY_BLOCK)

    def choose(a, b):
        return jnp.where(group == 0, a, b)

    decay_rows = decays.reshape(-1, 128)
    own_q = choose(queries[:, :width], queries[:, width:])
    sent_q = choose(queries[:, width:], queries[:, :width])
    vmem = pl.BlockSpec(memory_space=pltpu.VMEM)
    chips = count // 2
    dma = pltpu.SemaphoreType.DMA
    kv, far_q, decay_all = pl.pallas_call(
        lambda *refs: exchange_kernel(*refs, rows=rows, sizes=sizes),
        out_shape=(
            jax.ShapeDtypeStruct((length, 128), jnp.bfloat16),
            jax.ShapeDtypeStruct((rows, width), jnp.bfloat16),
            jax.ShapeDtypeStruct((members, *decay_rows.shape), jnp.float32),
        ),
        in_specs=[vmem] * 3,
        out_specs=(vmem,) * 3,
        scratch_shapes=[
            dma((2,)), dma((chips,)), dma((count,)), dma((chips,)), dma((members // 2,)),
            dma((members,)), dma((members // 2,)), dma, dma,
        ],
        compiler_params=pltpu.CompilerParams(has_side_effects=True),
        name="exchange",
    )(kv_blocks, sent_q, decay_rows)
    decay_all = decay_all.reshape(sp_count, heads, -1, key_block)
    decay_all = decay_all.transpose(0, 2, 1, 3).reshape(length // key_block, heads, key_block)
    firsts = (me * rows, (count - 1 - me) * rows)
    place = jnp.stack(firsts).astype(jnp.int32)
    row_decay = jnp.stack(
        [
            lax.dynamic_slice(
                decay_all, (first // key_block, 0, first % key_block), (1, heads, rows)
            )[0].T
            for first in firsts
        ]
    )
    attended = attend(place, own_q, far_q, row_decay, decay_all, kv, False)
    back = lax.ppermute(attended[1], ALL, mirror)
    return choose(
        jnp.concatenate([attended[0], back], axis=1), jnp.concatenate([back, attended[0]], axis=1)
    )


def any_program(
    inputs, in_gain, w_query, w_key, w_value, query_gain, key_gain, decay_sums, w_out, sizes
):
    kv_heads = sizes[1]
    head_size = query_gain.shape[0]
    rows = inputs.shape[0]
    all_heads = w_query.shape[1] // head_size

    normed = rms_norm(inputs.astype(jnp.float32), in_gain).astype(jnp.bfloat16)
    keys = rms_norm(
        jnp.dot(normed, w_key, preferred_element_type=jnp.float32).reshape(
            rows, kv_heads, head_size
        ),
        key_gain,
    ).astype(jnp.bfloat16)
    values = (
        jnp.dot(normed, w_value, preferred_element_type=jnp.float32)
        .astype(jnp.bfloat16)
        .reshape(rows, kv_heads, head_size)
    )
    kv_blocks = jnp.concatenate([keys, values], axis=2).transpose(1, 0, 2)
    queries = rms_norm(
        jnp.dot(normed, w_query, preferred_element_type=jnp.float32).reshape(
            rows, all_heads, head_size
        ),
        query_gain * (LOG2E * head_size ** (-0.5)),
    ).astype(jnp.bfloat16).reshape(rows, all_heads * head_size)
    whole = any_scores(queries, kv_blocks, decay_sums.T * LOG2E, sizes)
    return jnp.dot(whole, w_out, preferred_element_type=jnp.float32).astype(jnp.bfloat16)


def per_device(*arrays):
    query_gain, key_gain = arrays[5:7]
    sizes = (lax.axis_size("sp"), lax.axis_size("kv"), lax.axis_size("half"))
    most = jnp.max(query_gain[:, None] * key_gain[None, :])
    bound = query_gain.shape[0] ** 0.5 * LOG2E * most
    return lax.cond(
        bound <= SMALL,
        lambda *given: stream(*given[:7], given[7].T, given[8], sizes),
        lambda *given: any_program(*given, sizes),
        *arrays,
    )


def solution(mesh):
    sp_count, tp_count = mesh.devices.shape
    split = Mesh(mesh.devices.reshape(sp_count, 2, tp_count // 2), ALL)
    placed = (P(ALL, None), P(), P(), P(), P(), P(), P(), P("sp", ("kv", "half")), P())
    return jax.shard_map(
        per_device, mesh=split, in_specs=placed, out_specs=P(ALL, None), check_vma=False
    )
```

```python
import math

import jax
import jax.numpy as jnp
from jax import lax
from jax.experimental import pallas as pl
from jax.experimental.pallas import tpu as pltpu
from jax.sharding import Mesh, PartitionSpec as P

epsilon = 1e-06
LOG2E = math.log2(math.e)
ALL = ("sp", "kv", "half")
HEADS_PER_DOT = 2
KEY_BLOCK = 512
SMALL = 60.0
MOVED = (7, 10)


def rms_norm(vector, gain_vec):
    return (
        vector * lax.rsqrt(jnp.mean(vector * vector, axis=-1, keepdims=True) + epsilon) * gain_vec
    )


def exchange_kernel(
    kv_ref, q_ref, decay_ref, kv_out, q_out, decay_out, own_sems, kv_send, kv_recv, kv_relay,
    decay_send, decay_recv, decay_relay, q_send, q_recv, *, rows, sizes
):
    sp_count, kv_heads, half_count = sizes
    sp, group, half = lax.axis_index("sp"), lax.axis_index("kv"), lax.axis_index("half")
    core, chips = half % 2, half_count // 2
    partner = (sp, group, half + 1 - 2 * core)

    def device_of(chip):
        return (chip // (kv_heads * chips), (chip // chips) % kv_heads, (chip % chips) * 2 + core)

    def block_of(place):
        return (place[0] * kv_heads + place[1]) * half_count + place[2]

    def kv_copy(source, block, send, device):
        return pltpu.make_async_remote_copy(
            src_ref=source, dst_ref=kv_out.at[pl.ds(pl.multiple_of(block * rows, rows), rows)],
            send_sem=send, recv_sem=kv_recv.at[block], device_id=device,
            device_id_type=pl.DeviceIdType.MESH,
        )

    def decay_copy(source, member, send, device):
        return pltpu.make_async_remote_copy(
            src_ref=source, dst_ref=decay_out.at[member], send_sem=send,
            recv_sem=decay_recv.at[member], device_id=device,
            device_id_type=pl.DeviceIdType.MESH,
        )

    me = block_of((sp, group, half))
    chip = (sp * kv_heads + group) * chips + half // 2
    total = sp_count * kv_heads * chips
    member = sp * half_count + half
    cluster = sp * chips + half // 2
    clusters = sp_count * chips
    started = []
    for k in range(1, total):
        place = device_of((chip + k) % total)
        started.append(kv_copy(kv_ref.at[place[1]], me, kv_send.at[k], place))
        started[-1].start()
    for k in range(1, clusters):
        other = (cluster + k) % clusters
        place = (other // chips, group, (other % chips) * 2 + core)
        started.append(decay_copy(decay_ref, member, decay_send.at[k], place))
        started[-1].start()
    q_copy = pltpu.make_async_remote_copy(
        src_ref=q_ref, dst_ref=q_out, send_sem=q_send, recv_sem=q_recv,
        device_id=(sp_count - 1 - sp, kv_heads - 1 - group, half_count - 1 - half),
        device_id_type=pl.DeviceIdType.MESH,
    )
    q_copy.start()
    started.append(kv_copy(kv_ref.at[group], me, kv_relay.at[0], partner))
    started[-1].start()
    started.append(decay_copy(decay_ref, member, decay_relay.at[0], partner))
    started[-1].start()
    own_kv = pltpu.make_async_copy(
        kv_ref.at[group], kv_out.at[pl.ds(pl.multiple_of(me * rows, rows), rows)], own_sems.at[0]
    )
    own_kv.start()
    own_decay = pltpu.make_async_copy(decay_ref, decay_out.at[member], own_sems.at[1])
    own_decay.start()
    for k in range(1, clusters):
        other = (cluster + clusters - k) % clusters
        which = (other // chips) * half_count + (other % chips) * 2 + core
        landed = decay_out.at[which]
        relay = decay_copy(landed, which, decay_relay.at[k], partner)
        relay.wait_recv()
        relay.start()
        started.append(relay)
    for k in range(1, total):
        block = block_of(device_of((chip + total - k) % total))
        landed = kv_out.at[pl.ds(pl.multiple_of(block * rows, rows), rows)]
        relay = kv_copy(landed, block, kv_relay.at[k], partner)
        relay.wait_recv()
        relay.start()
        started.append(relay)
    for k in range(clusters):
        other = (cluster + clusters - k) % clusters
        which = (other // chips) * half_count + (other % chips) * 2 + 1 - core
        decay_copy(decay_out.at[which], which, decay_relay.at[k], partner).wait_recv()
    for k in range(total):
        place = device_of((chip + total - k) % total)
        block = block_of((place[0], place[1], place[2] + 1 - 2 * core))
        landed = kv_out.at[pl.ds(pl.multiple_of(block * rows, rows), rows)]
        kv_copy(landed, block, kv_relay.at[k], partner).wait_recv()
    for copy in started:
        copy.wait_send()
    own_kv.wait()
    own_decay.wait()
    q_copy.wait()


def attend_kernel(
    place_ref, near_ref, far_ref, row_ref, decay_ref, kv_ref, out_ref, ones_ref, q_ref, peak_ref,
    acc_ref, *, rows, heads, key_block, small
):
    lane = lax.broadcasted_iota(jnp.int32, (rows, 128), 1)
    low = lane < 64
    for r, ref in enumerate((near_ref, far_ref)):
        for pair in range(heads // 2):
            both = ref[:, pair * 128 : (pair + 1) * 128].astype(jnp.float32)
            even = jnp.where(low, both, 0.0)
            odd = jnp.where(low, pltpu.roll(both, 64, 1), 0.0)
            q_ref[r, (2 * pair) * rows : (2 * pair + 1) * rows] = even.astype(jnp.bfloat16)
            q_ref[r, (2 * pair + 1) * rows : (2 * pair + 2) * rows] = odd.astype(jnp.bfloat16)

    def fill(i, carry):
        at = pl.ds(pl.multiple_of(i * key_block, key_block), key_block)
        wide = lax.broadcasted_iota(jnp.int32, (key_block, 128), 1) < 64
        ones_ref[at] = jnp.where(wide, 1.0, kv_ref[at].astype(jnp.float32)).astype(jnp.bfloat16)
        return carry

    lax.fori_loop(0, kv_ref.shape[0] // key_block, fill, 0)
    span = HEADS_PER_DOT * rows

    for r in range(2):
        first = place_ref[r]
        for head in range(heads):
            part = pl.ds(head * rows, rows)
            if small:
                peak_ref[part] = jnp.broadcast_to(row_ref[r, :, head : head + 1], (rows, 128))
            else:
                peak_ref[part] = jnp.full((rows, 128), -1e30, jnp.float32)
        acc_ref[...] = jnp.zeros_like(acc_ref)

        def step(index, masked):
            at = pl.ds(pl.multiple_of(index * key_block, key_block), key_block)
            keys = kv_ref[at]
            values = ones_ref[at]
            for start in range(0, heads, HEADS_PER_DOT):
                part = pl.ds(start * rows, span)
                before = peak_ref[part]
                scores = lax.dot_general(
                    q_ref[r, part], keys, (((1,), (1,)), ((), ())),
                    preferred_element_type=jnp.float32,
                )
                if small:
                    scores = scores + jnp.concatenate([before] * (key_block // 128), axis=1)
                scores = scores.reshape(HEADS_PER_DOT, rows, key_block)
                scores = scores - decay_ref[index, start : start + HEADS_PER_DOT][:, None, :]
                if masked:
                    row = first + lax.broadcasted_iota(jnp.int32, (rows, key_block), 0)
                    col = index * key_block + lax.broadcasted_iota(
                        jnp.int32, (rows, key_block), 1
                    )
                    scores = jnp.where((col <= row)[None], scores, -1e30)
                scores = scores.reshape(span, key_block)
                if small:
                    weights = jnp.exp2(scores).astype(jnp.bfloat16)
                    acc_ref[part] += jnp.dot(weights, values, preferred_element_type=jnp.float32)
                else:
                    after = jnp.maximum(before, jnp.max(scores, axis=1, keepdims=True))
                    weights = jnp.exp2(scores - after[:, :1]).astype(jnp.bfloat16)
                    acc_ref[part] = acc_ref[part] * jnp.exp2(before - after) + jnp.dot(
                        weights, values, preferred_element_type=jnp.float32
                    )
                    peak_ref[part] = after

        full = first // key_block

        def body(index, carry):
            step(index, False)
            return carry

        lax.fori_loop(0, full, body, 0)
        step(full, True)
        for pair in range(heads // 2):
            even = acc_ref[(2 * pair) * rows : (2 * pair + 1) * rows]
            odd = acc_ref[(2 * pair + 1) * rows : (2 * pair + 2) * rows]
            done = jnp.where(low, pltpu.roll(even, 64, 1), odd) / jnp.where(
                low, even, pltpu.roll(odd, 64, 1)
            )
            out_ref[r, :, pair * 128 : (pair + 1) * 128] = done.astype(jnp.bfloat16)


def attend(place, near, far, row_decay, decays, kv, small):
    length = kv.shape[0]
    rows, width = near.shape
    heads, key_block = decays.shape[1:]
    vmem = pl.BlockSpec(memory_space=pltpu.VMEM)
    return pl.pallas_call(
        lambda *refs: attend_kernel(
            *refs, rows=rows, heads=heads, key_block=key_block, small=small
        ),
        out_shape=jax.ShapeDtypeStruct((2, rows, width), jnp.bfloat16),
        in_specs=[pl.BlockSpec(memory_space=pltpu.SMEM)] + [vmem] * 5,
        out_specs=vmem,
        scratch_shapes=[
            pltpu.VMEM((length, 128), jnp.bfloat16),
            pltpu.VMEM((2, heads * rows, 128), jnp.bfloat16),
            pltpu.VMEM((heads * rows, 128), jnp.float32),
            pltpu.VMEM((heads * rows, 128), jnp.float32),
        ],
        compiler_params=pltpu.CompilerParams(vmem_limit_bytes=40 * 1024 * 1024),
        name="attend_small" if small else "attend_any",
    )(place, near, far, row_decay, decays, kv)


def stream_kernel(
    x_hbm, in_gain, wq_hbm, wk_hbm, wv_hbm, query_gain, key_gain, sums_hbm, wo_hbm, out_ref,
    x_ref, wkv_ref, wq_ref, sums_ref, wo_ref, normed_ref, kvt_ref, query_ref, decay_ref, att_ref,
    kvt_all, decay_all, far_decay, in_q, qt_ref, acc_ref, kp_all, vt_all, res_ref, done_ref, sum_ref, loads, kv_recv,
    decay_recv, x_send, own_send, round_send, late_send, far_send, far_recv, q_send, q_recv,
    back_send, back_recv, *, sizes, lines, rows, heads
):
    sp_count, kv_heads, half_count = sizes
    zs, ys = lines
    zh = zs // 2
    upper = sp_count // 2
    pairs = heads // 2
    units = pairs * kv_heads
    width = heads * 64
    span = 2 * rows
    local, chunk_rows = decay_ref.shape
    s, g, j = lax.axis_index("sp"), lax.axis_index("kv"), lax.axis_index("half")
    z, y = s // ys, s % ys
    partner_x = 1 - g
    s_far = sp_count - 1 - s
    is_high = s >= upper

    def share(s_):
        even = (2 * units * (2 * s_ + 1 - sp_count) + 2 * s_ + 1) // (2 * (2 * s_ + 1))
        return even * MOVED[0] // MOVED[1]

    given = jnp.where(is_high, share(jnp.maximum(s, upper)), 0)
    taken = jnp.where(is_high, 0, share(jnp.maximum(s_far, upper)))

    def kept_from(x_):
        return (jnp.maximum(given - x_, 0) + kv_heads - 1) // kv_heads

    def block_at(s_, x_, j_):
        return (s_ * kv_heads + x_) * half_count + j_

    def remote(source, target, send, recv, device):
        return pltpu.make_async_remote_copy(
            src_ref=source, dst_ref=target, send_sem=send, recv_sem=recv, device_id=device,
            device_id_type=pl.DeviceIdType.MESH,
        )

    def kv_copy(source, block, send, device):
        return remote(source, kvt_all.at[block], send, kv_recv.at[block], device)

    def decay_copy(source, member, send, device):
        return remote(source, decay_all.at[member], send, decay_recv.at[member], device)

    here = (s, g, j)
    each = kv_heads + 1

    def one_piece(s_, j_, piece, base, device, sems):
        if piece == kv_heads:
            member = s_ * half_count + j_
            return decay_copy(decay_all.at[member], member, sems.at[base + piece], device)
        block = block_at(s_, piece, j_)
        return kv_copy(kvt_all.at[block], block, sems.at[base + piece], device)

    def arrived(s_, j_):
        for piece in range(each):
            one_piece(s_, j_, piece, 0, here, own_send).wait_recv()

    def start_all(copies):
        for copy in copies:
            copy.start()

    def drain_all(copies):
        for copy in copies:
            copy.wait_send()

    def inside(z_):
        return (z_ >= 0) & (z_ < zs)

    def to_rows(base):
        return [
            (None, base + (n - 1) * each, (z * ys + (y + n) % ys, g, j)) for n in range(1, ys)
        ]

    def to_lanes(base):
        return [
            (None, base + (n - 1) * each, (s, g, (j + n) % half_count))
            for n in range(1, half_count)
        ]

    def relay(s_, routes, sems, go):
        for piece in range(each):
            if go:
                one_piece(s_, j, piece, 0, here, own_send).wait_recv()
            for condition, base, device in routes:
                copy = one_piece(s_, j, piece, base, device, sems)
                act = copy.start if go else copy.wait_send
                if condition is None:
                    act()
                else:
                    pl.when(condition)(act)

    per = 1 + (ys - 1) + (half_count - 1) + (ys - 1) * (half_count - 1)

    def spread(s_, base, condition, device, sems, go):
        routes = [(condition, base, device)]
        routes += to_rows(base + each) + to_lanes(base + ys * each)
        relay(s_, routes, sems, go)

    def across(zo, base, sems, go):
        for m in range(1, ys):
            slot = ys + half_count - 1 + (m - 1) * (half_count - 1)
            relay(zo * ys + (y + m) % ys, to_lanes(base + slot * each), sems, go)

    def round_of(k, go):
        base = (k - 1) * per * each

        @pl.when(inside(z - k))
        def _():
            spread(
                (z - k) * ys + y, base, inside(z + 1), ((z + 1) * ys + y, g, j), round_send, go
            )

        @pl.when(inside(z - k + 1))
        def _():
            across(z - k + 1, base, round_send, go)

    def late(zo, go):
        base = (zo - 1) * per * each
        routes = to_rows(base + each) + to_lanes(base + ys * each)
        relay(zo * ys + y, routes, late_send, go)

    def late_across(zo, go):
        across(zo, (zo - 1) * per * each, late_send, go)

    def build(s_):
        for x_ in range(kv_heads):
            for j_ in range(half_count):
                block = block_at(s_, x_, j_)
                place = (x_ * half_count + j_) * rows
                decays = jnp.concatenate(
                    [
                        decay_all[s_ * half_count + n, :, pl.ds(place, rows)]
                        for n in range(half_count)
                    ],
                    axis=0,
                )
                decays = -decays
                high = decays.astype(jnp.bfloat16).astype(jnp.float32)
                rest = decays - high
                middle = rest.astype(jnp.bfloat16).astype(jnp.float32)
                parts = jnp.concatenate(
                    [high, middle, rest - middle, jnp.ones((8, rows), jnp.float32)], axis=0
                ).astype(jnp.bfloat16)
                wide = jnp.concatenate(
                    [kvt_all[block, 0:64], parts, jnp.zeros((32, rows), jnp.bfloat16)], axis=0
                )
                kp_all[s_, pl.ds(place, rows)] = wide.T
                vt_all[s_, 0:64, pl.ds(place, rows)] = kvt_all[block, 64:128]

    def build_if(s_):
        @pl.when(s_ <= jnp.where(is_high, s, s_far))
        def _():
            build(s_)

    def lanes_of(k):
        @pl.when(inside(z - k))
        def _():
            s_ = (z - k) * ys + y
            for n in range(1, half_count):
                arrived(s_, (j + n) % half_count)
            build_if(s_)

        @pl.when(inside(z - k + 1))
        def _():
            for m in range(1, ys):
                s_ = (z - k + 1) * ys + (y + m) % ys
                for n in range(1, half_count):
                    arrived(s_, (j + n) % half_count)
                build_if(s_)

    def late_lanes(zo):
        for m in range(ys):
            s_ = zo * ys + (y + m) % ys
            for n in range(1, half_count):
                arrived(s_, (j + n) % half_count)
            build_if(s_)

    def q_lanes(group, pair):
        return pl.ds(pl.multiple_of(group * width + pair * 128, 128), 128)

    fetches = [
        pltpu.make_async_copy(source, target, loads.at[n])
        for n, (source, target) in enumerate(
            (
                (x_hbm, x_ref), (wk_hbm, wkv_ref.at[:, 0:128]), (wv_hbm, wkv_ref.at[:, 128:256]),
                (sums_hbm, sums_ref), (wq_hbm, wq_ref), (wo_hbm, wo_ref),
            )
        )
    ]
    for fetch in fetches:
        fetch.start()

    barrier = pltpu.get_barrier_semaphore()

    def greet(device):
        pl.semaphore_signal(
            barrier, inc=1, device_id=device, device_id_type=pl.DeviceIdType.MESH
        )

    greeted = 0
    for n in range(1, half_count):
        greet((s, g, (j + n) % half_count))
        greeted += 1
    greet((s, partner_x, j))
    greeted += 1
    for z_ in range(zs):
        met = ((z_ < z) & (z_ <= zs - 1 - z)) | ((z < z_) & (z <= zs - 1 - z_))

        @pl.when(met)
        def _():
            greet((z_ * ys + y, g, j))

        greeted = greeted + jnp.where(met, 1, 0)
    for n in range(1, ys):
        greet((z * ys + (y + n) % ys, g, j))
        greeted += 1
    for x_ in range(kv_heads):
        for n in range(half_count):
            greet((s_far, x_, n))
            greeted += 1
    for way in (1, -1):

        @pl.when(inside(z + way))
        def _():
            greet(((z + way) * ys + y, g, j))

        greeted = greeted + jnp.where(inside(z + way), 1, 0)

    def columns(gain):
        wide = jnp.broadcast_to(gain.reshape(1, 64), (64, 64))
        wide = jnp.concatenate([wide, wide], axis=1)
        wide = jnp.concatenate([wide, wide], axis=0).T
        return jnp.concatenate([wide[0:64]] * (rows // 128), axis=1)

    def per_head(turned, gain):
        many = turned.reshape(turned.shape[0] // 64, 64, rows)
        mean = jnp.mean(many * many, axis=1, keepdims=True)
        return (many * lax.rsqrt(mean + epsilon) * gain[None]).reshape(turned.shape)

    fetches[0].wait()
    x = x_ref[...].astype(jnp.float32)
    scale = lax.rsqrt(jnp.mean(x * x, axis=1, keepdims=True) + epsilon)
    normed_ref[...] = (x * scale * in_gain[...].reshape(1, -1)).astype(jnp.bfloat16)
    fetches[1].wait()
    fetches[2].wait()
    both = jnp.dot(normed_ref[...], wkv_ref[...], preferred_element_type=jnp.float32).T
    turned_keys = per_head(both[0:128], columns(key_gain[...])).astype(jnp.bfloat16)
    turned_values = both[128:256].astype(jnp.bfloat16)
    for n in range(kv_heads):
        kvt_ref[n, 0:64] = turned_keys[n * 64 : (n + 1) * 64]
        kvt_ref[n, 64:128] = turned_values[n * 64 : (n + 1) * 64]
    fetches[3].wait()
    decay_ref[...] = sums_ref[...] * LOG2E

    def far_q_copy(group, pair):
        unit = kv_heads * pair + g
        slot = jnp.minimum(pairs + unit, 2 * pairs - 1)
        return remote(
            query_ref.at[q_lanes(group, pair)], in_q.at[slot],
            q_send.at[group * pairs + pair], q_recv.at[slot], (s_far, group, j),
        )

    def near_q_copy(pair):
        return remote(
            query_ref.at[q_lanes(partner_x, pair)], in_q.at[pair],
            q_send.at[partner_x * pairs + pair], q_recv.at[pair], (s, partner_x, j),
        )

    def q_arrived(slot):
        remote(
            query_ref.at[pl.ds(0, 128)], in_q.at[slot], q_send.at[0], q_recv.at[slot], here
        ).wait_recv()

    def is_given(pair, x_):
        return kv_heads * pair + x_ < given

    def far_sends(act):
        for pair in range(pairs):
            for group in range(kv_heads):

                @pl.when(is_given(pair, g))
                def _():
                    act([far_q_copy(group, pair)])

    def near_sends(act):
        for pair in range(pairs):

            @pl.when(jnp.logical_not(is_given(pair, g)))
            def _():
                act([near_q_copy(pair)])

    def far_decay_copies():
        copies = []
        for x_ in range(kv_heads):
            for n in range(half_count):
                source = decay_ref.at[:, pl.ds((x_ * half_count + n) * rows, rows)]
                at = x_ * half_count + n
                copies.append(
                    remote(
                        source, far_decay.at[x_ * half_count + j], far_send.at[at],
                        far_recv.at[x_ * half_count + j], (s_far, g, n),
                    )
                )
        return copies

    own_block = block_at(s, g, j)
    other_block = block_at(s, partner_x, j)
    member = s * half_count + j

    def side_targets():
        targets = [(None, (s, g, (j + n) % half_count)) for n in range(1, half_count)]
        targets.append((inside(z + 1), ((z + 1) * ys + y, g, j)))
        targets += [(None, (z * ys + (y + n) % ys, g, j)) for n in range(1, ys)]
        return targets

    def each_down(act):
        for z_ in range(zh - 1, -1, -1):

            @pl.when((z_ < z) & (z_ <= zs - 1 - z))
            def _():
                act((ys + half_count - 1 + z_) * each, (z_ * ys + y, g, j))

    def each_side(act):
        for slot, (condition, device) in enumerate(side_targets()):
            if condition is None:
                act(slot * each, device)
            else:

                @pl.when(condition)
                def _():
                    act(slot * each, device)

    def own_copies(base, device):
        return [
            kv_copy(kvt_ref.at[g], own_block, own_send.at[base], device),
            decay_copy(decay_ref, member, own_send.at[base + 1], device),
        ]

    def other_copies(base, device):
        return [kv_copy(kvt_all.at[other_block], other_block, own_send.at[base + 2], device)]

    x_copy = kv_copy(kvt_ref.at[partner_x], own_block, x_send, (s, partner_x, j))
    pl.semaphore_wait(barrier, greeted)
    x_copy.start()
    each_side(lambda base, device: start_all(own_copies(base, device)))

    @pl.when(z <= zh)
    def _():
        each_down(lambda base, device: start_all(own_copies(base, device)))

    fetches[4].wait()
    query_columns = columns(query_gain[...] * (LOG2E * 64 ** (-0.5)))

    def project(n, carry):
        at = pl.ds(pl.multiple_of(n * 512, 512), 512)
        turned = jnp.dot(
            normed_ref[...], wq_ref[:, at], preferred_element_type=jnp.float32
        ).T
        query_ref[at] = per_head(turned, query_columns).astype(jnp.bfloat16)
        return carry

    lax.fori_loop(0, query_ref.shape[0] // 512, project, 0)

    @pl.when(z > zh)
    def _():
        far_sends(start_all)

    near_sends(start_all)
    kvt_all[own_block] = kvt_ref[g]
    decay_all[member] = decay_ref[...]
    acc_ref[...] = jnp.zeros_like(acc_ref)
    vt_all[:, 64:80] = jnp.ones((sp_count, 16, chunk_rows), jnp.bfloat16)

    def prepare(t, slot, source, pair, decays):
        turned = source
        high = decays.astype(jnp.bfloat16).astype(jnp.float32)
        rest = decays - high
        middle = rest.astype(jnp.bfloat16).astype(jnp.float32)
        rest = rest - middle
        row = lax.broadcasted_iota(jnp.int32, (64, rows), 0)
        for n in range(2):
            head = 2 * pair + n
            lanes = pl.ds(slot * span + n * rows, rows)
            picked = (row == head) | (row == 8 + head) | (row == 16 + head)
            extra = jnp.where(picked, 1.0, 0.0)
            for at, part in ((24, high), (25, middle), (26, rest)):
                extra = jnp.where(row == at, part[n : n + 1], extra)
            qt_ref[t, 0:64, lanes] = turned[n * 64 : (n + 1) * 64]
            qt_ref[t, 64:128, lanes] = extra.astype(jnp.bfloat16)

    def own_decays(pair, x_):
        first = (2 * pair) % local
        at = pl.ds(pl.multiple_of((x_ * half_count + j) * rows, rows), rows)
        return decay_all[s * half_count + (2 * pair) // local, first : first + 2, at]

    def far_decays(slot):
        pair, x_ = slot // kv_heads, slot % kv_heads
        first = (2 * pair) % local
        return far_decay[x_ * half_count + (2 * pair) // local, first : first + 2]

    def work(t, at, lanes, chunk, start, size, step, limit=None):
        at = pl.ds(pl.multiple_of(at, span), lanes)
        q = qt_ref[t, :, at]
        total = acc_ref[t, :, at]
        for b in range(size // step):
            where = pl.ds(pl.multiple_of(start + b * step, step), step)
            scores = jnp.dot(kp_all[chunk, where], q, preferred_element_type=jnp.float32)
            if limit is not None:
                key = lax.broadcasted_iota(jnp.int32, (step, lanes), 0)
                row = lax.broadcasted_iota(jnp.int32, (step, lanes), 1) % rows
                scores = jnp.where(key <= row + limit, scores, -1e30)
            weights = jnp.exp2(scores).astype(jnp.bfloat16)
            total = total + jnp.dot(
                vt_all[chunk, :, where], weights, preferred_element_type=jnp.float32
            )
        acc_ref[t, :, at] = total

    def whole(t, at, lanes, chunk):
        work(t, at, lanes, chunk, 0, chunk_rows, chunk_rows if lanes == span else chunk_rows // 2)

    def sweep(t, at, lanes, low, high):
        def body(chunk, carry):
            whole(t, at, lanes, chunk)
            return carry

        lax.fori_loop(low, high, body, 0)

    def diagonal(t, at, lanes, chunk, offset):
        full = offset // span

        def body(i, carry):
            work(t, at, lanes, chunk, i * span, span, span)
            return carry

        lax.fori_loop(0, full, body, 0)
        work(t, at, lanes, chunk, full * span, span, span, offset - full * span)

    def finished(t, slot):
        out = []
        for n in range(2):
            lanes = pl.ds(slot * span + n * rows, rows)
            out.append(acc_ref[t, 0:64, lanes] / acc_ref[t, 64:65, lanes])
        return jnp.concatenate(out, axis=0).T.astype(jnp.bfloat16)

    def back_copy(slot, pair, device):
        return remote(
            res_ref.at[slot], att_ref.at[:, q_lanes(g, pair)], back_send.at[slot],
            back_recv.at[g * pairs + pair], device,
        )

    def back_arrived(group, pair):
        remote(
            res_ref.at[0], att_ref.at[:, q_lanes(group, pair)], back_send.at[0],
            back_recv.at[group * pairs + pair], here,
        ).wait_recv()

    def kept_groups(first, act):
        def body(i, carry):
            @pl.when(first <= 2 * i)
            def _():
                act(i * 2 * span, 2 * span)

            @pl.when(first == 2 * i + 1)
            def _():
                act((2 * i + 1) * span, span)

            return carry

        lax.fori_loop(0, pairs // 2, body, 0)

    def taken_groups(act):
        def body(i, carry):
            @pl.when(taken >= 2 * i + 2)
            def _():
                act(i * 2 * span, 2 * span)

            @pl.when(taken == 2 * i + 1)
            def _():
                act(i * 2 * span, span)

            return carry

        lax.fori_loop(0, pairs // 2, body, 0)

    my_first = kept_from(g)
    partner_first = kept_from(partner_x)
    offset = (g * half_count + j) * rows
    partner_offset = (partner_x * half_count + j) * rows

    kv_copy(kvt_ref.at[g], other_block, x_send, here).wait_recv()
    each_side(lambda base, device: start_all(other_copies(base, device)))

    @pl.when(z <= zh)
    def _():
        each_down(lambda base, device: start_all(other_copies(base, device)))

    @pl.when(z == zh)
    def _():
        far_sends(start_all)

    @pl.when(is_high)
    def _():
        start_all(far_decay_copies())

    for n in range(1, half_count):
        arrived(s, (j + n) % half_count)
    build(s)
    for pair in range(pairs):
        prepare(0, pair, query_ref[q_lanes(g, pair)], pair, own_decays(pair, g))
    kept_groups(my_first, lambda at, lanes: diagonal(0, at, lanes, s, offset))
    round_of(1, True)

    def at_step(k):
        return s - jnp.where(y == 0, jnp.where(k == 1, ys, jnp.where(k == ys, 1, k)), k)

    def comes(zo):
        return (z < zh) & (zo > z) & (zo <= zs - 1 - z)

    def item(k, carry):
        @pl.when((k == 2) & (z > zh))
        def _():
            each_down(
                lambda base, device: start_all(
                    own_copies(base, device) + other_copies(base, device)
                )
            )

        lanes_of(k)
        for here_too, step, duty, zo in (
            (z == 0, 1, late, z + 1), (z == 0, 3, late, z + 2),
            (z > 0, 2, late, z + 1), (z > 0, 4, late_across, z + 1),
        ):

            @pl.when(here_too & (k == step) & comes(zo))
            def _():
                duty(zo, True)

        @pl.when(k <= s)
        def _():
            kept_groups(my_first, lambda at, lanes: whole(0, at, lanes, at_step(k)))

        @pl.when(k < zs)
        def _():
            round_of(k + 1, True)

        @pl.when(k == 1)
        def _():
            for n in range(pairs):

                @pl.when(partner_first <= n)
                def _():
                    q_arrived(n)
                    prepare(1, n, in_q[n], n, own_decays(n, partner_x))

            kept_groups(
                partner_first, lambda at, lanes: diagonal(1, at, lanes, s, partner_offset)
            )

        @pl.when((k > 1) & (k - 1 <= s))
        def _():
            kept_groups(partner_first, lambda at, lanes: whole(1, at, lanes, at_step(k - 1)))

        return carry

    lax.fori_loop(1, zs + 1, item, 0)

    def partner_phase():
        def body(i, carry):
            def run(at, lanes):
                def body(k, carry):
                    whole(1, at, lanes, at_step(k))
                    return carry

                lax.fori_loop(zs, jnp.minimum(s, zs) + 1, body, 0)
                sweep(1, at, lanes, 0, jnp.maximum(s - zs, 0))

            @pl.when(partner_first <= 2 * i)
            def _():
                run(i * 2 * span, 2 * span)

            @pl.when(partner_first == 2 * i + 1)
            def _():
                run((2 * i + 1) * span, span)

            for n in range(pairs):

                @pl.when((i == n // 2) & (partner_first <= n))
                def _():
                    res_ref[n] = finished(1, n)
                    back_copy(n, n, (s, partner_x, j)).start()

            return carry

        lax.fori_loop(0, pairs // 2, body, 0)

    def far_phase():
        for n in range(kv_heads * half_count):
            remote(
                decay_ref.at[:, pl.ds(0, rows)], far_decay.at[n], far_send.at[n],
                far_recv.at[n], here,
            ).wait_recv()

        for n in range(pairs):

            @pl.when(n < taken)
            def _():
                q_arrived(pairs + n)
                prepare(2, n, in_q[pairs + n], n // kv_heads, far_decays(n))

        def zone(zo, carry):
            high = jnp.minimum(zo * ys + ys, s_far)

            def body(i, carry):
                @pl.when(taken >= 2 * i + 2)
                def _():
                    sweep(2, i * 2 * span, 2 * span, zo * ys, high)

                @pl.when(taken == 2 * i + 1)
                def _():
                    sweep(2, i * 2 * span, span, zo * ys, high)

                for turn, ahead, duty, zl in (
                    (0, 0, late_across, z + 1), (0, 1, late, z + 3), (1, 1, late_across, z + 2),
                    (0, 2, late_across, z + 3),
                ):

                    @pl.when((z == 0) & (i == turn) & (zo == ahead) & comes(zl))
                    def _():
                        duty(zl, True)

                return carry

            lax.fori_loop(0, pairs // 2, body, 0)

            @pl.when(comes(zo + 1) & (zo > jnp.where(z == 0, 2, z)))
            def _():
                late(zo + 1, True)
                late_across(zo + 1, True)

            @pl.when(comes(zo + 1))
            def _():
                late_lanes(zo + 1)

            return carry

        lax.fori_loop(0, zs - z, zone, 0)

        def close(n, carry):
            unit_x = n % kv_heads
            diagonal(2, n * span, span, s_far, (unit_x * half_count + j) * rows)
            for m in range(pairs):

                @pl.when(n == m)
                def _():
                    res_ref[pairs + m] = finished(2, m)
                    back_copy(
                        pairs + m, m // kv_heads, (s_far, m % kv_heads, j)
                    ).start()

            return carry

        lax.fori_loop(0, taken, close, 0)

    partner_phase()

    @pl.when(z < zh)
    def _():
        far_phase()

    kept_groups(my_first, lambda at, lanes: sweep(0, at, lanes, 0, jnp.maximum(s - zs, 0)))
    for pair in range(pairs):

        @pl.when(pair >= my_first)
        def _():
            att_ref[:, q_lanes(g, pair)] = finished(0, pair)

    fetches[5].wait()
    for pair in range(pairs):

        @pl.when(pair < my_first)
        def _():
            back_arrived(g, pair)

    mine = pl.ds(pl.multiple_of(g * width, width), width)
    theirs = pl.ds(pl.multiple_of(partner_x * width, width), width)
    model = wo_ref.shape[1]
    half = model // 2
    for n in range(2):
        at = pl.ds(n * half, half)
        sum_ref[:, at] = jnp.dot(
            att_ref[:, mine], wo_ref[mine, at], preferred_element_type=jnp.float32
        )
    for pair in range(pairs):
        back_arrived(partner_x, pair)
    puts = []
    for n in range(2):
        at = pl.ds(n * half, half)
        done_ref[:, at] = (
            sum_ref[:, at]
            + jnp.dot(att_ref[:, theirs], wo_ref[theirs, at], preferred_element_type=jnp.float32)
        ).astype(jnp.bfloat16)
        puts.append(pltpu.make_async_copy(done_ref.at[:, at], out_ref.at[:, at], loads.at[n]))
        puts[n].start()
    x_copy.wait_send()
    each_side(
        lambda base, device: drain_all(own_copies(base, device) + other_copies(base, device))
    )

    each_down(
        lambda base, device: drain_all(own_copies(base, device) + other_copies(base, device))
    )

    def drain(k, carry):
        round_of(k, False)
        return carry

    lax.fori_loop(1, zs + 1, drain, 0)

    def drain_late(zo, carry):
        late(zo, False)
        late_across(zo, False)
        return carry

    @pl.when(z < zh)
    def _():
        lax.fori_loop(z + 1, zs - z, drain_late, 0)


    @pl.when(is_high)
    def _():
        far_sends(drain_all)
        drain_all(far_decay_copies())

    near_sends(drain_all)
    for pair in range(pairs):

        @pl.when(partner_first <= pair)
        def _():
            back_copy(pair, pair, (s, partner_x, j)).wait_send()

        @pl.when(pair < taken)
        def _():
            back_copy(
                pairs + pair, pair // kv_heads, (s_far, pair % kv_heads, j)
            ).wait_send()
    for put in puts:
        put.wait()


def lines_of(sp_count):
    ys = 1 << ((sp_count.bit_length() - 1) // 2)
    return sp_count // ys, ys


def stream(
    inputs, in_gain, w_query, w_key, w_value, query_gain, key_gain, decay_sums, w_out, sizes
):
    sp_count, kv_heads, half_count = sizes
    rows, model = inputs.shape
    width = w_query.shape[1]
    heads = width // 64 // kv_heads
    local, chunk_rows = decay_sums.shape
    zs, ys = lines_of(sp_count)
    pairs = heads // 2
    count = sp_count * kv_heads * half_count
    members = sp_count * half_count
    per = 1 + (ys - 1) + (half_count - 1) + (ys - 1) * (half_count - 1)
    each = kv_heads + 1
    vmem = pl.BlockSpec(memory_space=pltpu.VMEM)
    hbm = pl.BlockSpec(memory_space=pltpu.MemorySpace.HBM)
    dma = pltpu.SemaphoreType.DMA
    return pl.pallas_call(
        lambda *refs: stream_kernel(
            *refs, sizes=sizes, lines=(zs, ys), rows=rows, heads=heads
        ),
        out_shape=jax.ShapeDtypeStruct((rows, w_out.shape[1]), jnp.bfloat16),
        in_specs=[hbm, vmem, hbm, hbm, hbm, vmem, vmem, hbm, hbm],
        out_specs=hbm,
        scratch_shapes=[
            pltpu.VMEM((rows, model), jnp.bfloat16),
            pltpu.VMEM((model, 256), jnp.bfloat16),
            pltpu.VMEM(w_query.shape, jnp.bfloat16),
            pltpu.VMEM(decay_sums.shape, jnp.float32),
            pltpu.VMEM(w_out.shape, jnp.bfloat16),
            pltpu.VMEM((rows, model), jnp.bfloat16),
            pltpu.VMEM((kv_heads, 128, rows), jnp.bfloat16),
            pltpu.VMEM((width, rows), jnp.bfloat16),
            pltpu.VMEM((local, chunk_rows), jnp.float32),
            pltpu.VMEM((rows, width), jnp.bfloat16),
            pltpu.VMEM((count, 128, rows), jnp.bfloat16),
            pltpu.VMEM((members, local, chunk_rows), jnp.float32),
            pltpu.VMEM((kv_heads * half_count, local, rows), jnp.float32),
            pltpu.VMEM((2 * pairs, 128, rows), jnp.bfloat16),
            pltpu.VMEM((3, 128, heads * rows), jnp.bfloat16),
            pltpu.VMEM((3, 80, heads * rows), jnp.float32),
            pltpu.VMEM((sp_count, chunk_rows, 128), jnp.bfloat16),
            pltpu.VMEM((sp_count, 80, chunk_rows), jnp.bfloat16),
            pltpu.VMEM((2 * pairs, rows, 128), jnp.bfloat16),
            pltpu.VMEM((rows, w_out.shape[1]), jnp.bfloat16),
            pltpu.VMEM((rows, w_out.shape[1]), jnp.float32),
            dma((6,)),
            dma((count,)), dma((members,)), dma, dma(((ys + half_count + zs // 2) * each,)),
            dma((zs * per * each,)), dma((zs * per * each,)),
            dma((kv_heads * half_count,)), dma((kv_heads * half_count,)),
            dma((2 * pairs,)), dma((2 * pairs,)), dma((2 * pairs,)), dma((2 * pairs,)),
        ],
        compiler_params=pltpu.CompilerParams(
            has_side_effects=True, collective_id=0, vmem_limit_bytes=56 * 1024 * 1024
        ),
        name="stream",
    )(inputs, in_gain, w_query, w_key, w_value, query_gain, key_gain, decay_sums, w_out)


def any_scores(queries, kv_blocks, decays, sizes):
    sp_count, kv_heads, half_count = sizes
    group = lax.axis_index("kv")
    me = (lax.axis_index("sp") * kv_heads + group) * half_count + lax.axis_index("half")
    count = sp_count * kv_heads * half_count
    mirror = [(i, count - 1 - i) for i in range(count)]
    rows = queries.shape[0]
    length = rows * count
    heads = queries.shape[1] // 64 // kv_heads
    width = heads * 64
    members = sp_count * half_count
    key_block = math.gcd(length, KEY_BLOCK)

    def choose(a, b):
        return jnp.where(group == 0, a, b)

    decay_rows = decays.reshape(-1, 128)
    own_q = choose(queries[:, :width], queries[:, width:])
    sent_q = choose(queries[:, width:], queries[:, :width])
    vmem = pl.BlockSpec(memory_space=pltpu.VMEM)
    chips = count // 2
    dma = pltpu.SemaphoreType.DMA
    kv, far_q, decay_all = pl.pallas_call(
        lambda *refs: exchange_kernel(*refs, rows=rows, sizes=sizes),
        out_shape=(
            jax.ShapeDtypeStruct((length, 128), jnp.bfloat16),
            jax.ShapeDtypeStruct((rows, width), jnp.bfloat16),
            jax.ShapeDtypeStruct((members, *decay_rows.shape), jnp.float32),
        ),
        in_specs=[vmem] * 3,
        out_specs=(vmem,) * 3,
        scratch_shapes=[
            dma((2,)), dma((chips,)), dma((count,)), dma((chips,)), dma((members // 2,)),
            dma((members,)), dma((members // 2,)), dma, dma,
        ],
        compiler_params=pltpu.CompilerParams(has_side_effects=True),
        name="exchange",
    )(kv_blocks, sent_q, decay_rows)
    decay_all = decay_all.reshape(sp_count, heads, -1, key_block)
    decay_all = decay_all.transpose(0, 2, 1, 3).reshape(length // key_block, heads, key_block)
    firsts = (me * rows, (count - 1 - me) * rows)
    place = jnp.stack(firsts).astype(jnp.int32)
    row_decay = jnp.stack(
        [
            lax.dynamic_slice(
                decay_all, (first // key_block, 0, first % key_block), (1, heads, rows)
            )[0].T
            for first in firsts
        ]
    )
    attended = attend(place, own_q, far_q, row_decay, decay_all, kv, False)
    back = lax.ppermute(attended[1], ALL, mirror)
    return choose(
        jnp.concatenate([attended[0], back], axis=1), jnp.concatenate([back, attended[0]], axis=1)
    )


def any_program(
    inputs, in_gain, w_query, w_key, w_value, query_gain, key_gain, decay_sums, w_out, sizes
):
    kv_heads = sizes[1]
    head_size = query_gain.shape[0]
    rows = inputs.shape[0]
    all_heads = w_query.shape[1] // head_size

    normed = rms_norm(inputs.astype(jnp.float32), in_gain).astype(jnp.bfloat16)
    keys = rms_norm(
        jnp.dot(normed, w_key, preferred_element_type=jnp.float32).reshape(
            rows, kv_heads, head_size
        ),
        key_gain,
    ).astype(jnp.bfloat16)
    values = (
        jnp.dot(normed, w_value, preferred_element_type=jnp.float32)
        .astype(jnp.bfloat16)
        .reshape(rows, kv_heads, head_size)
    )
    kv_blocks = jnp.concatenate([keys, values], axis=2).transpose(1, 0, 2)
    queries = rms_norm(
        jnp.dot(normed, w_query, preferred_element_type=jnp.float32).reshape(
            rows, all_heads, head_size
        ),
        query_gain * (LOG2E * head_size ** (-0.5)),
    ).astype(jnp.bfloat16).reshape(rows, all_heads * head_size)
    whole = any_scores(queries, kv_blocks, decay_sums.T * LOG2E, sizes)
    return jnp.dot(whole, w_out, preferred_element_type=jnp.float32).astype(jnp.bfloat16)


def per_device(*arrays):
    query_gain, key_gain = arrays[5:7]
    sizes = (lax.axis_size("sp"), lax.axis_size("kv"), lax.axis_size("half"))
    most = jnp.max(query_gain[:, None] * key_gain[None, :])
    bound = query_gain.shape[0] ** 0.5 * LOG2E * most
    return lax.cond(
        bound <= SMALL,
        lambda *given: stream(*given[:7], given[7].T, given[8], sizes),
        lambda *given: any_program(*given, sizes),
        *arrays,
    )


def solution(mesh):
    sp_count, tp_count = mesh.devices.shape
    split = Mesh(mesh.devices.reshape(sp_count, 2, tp_count // 2), ALL)
    placed = (P(ALL, None), P(), P(), P(), P(), P(), P(), P("sp", ("kv", "half")), P())
    return jax.shard_map(
        per_device, mesh=split, in_specs=placed, out_specs=P(ALL, None), check_vma=False
    )
```

```python
import math

import jax
import jax.numpy as jnp
from jax import lax
from jax.experimental import pallas as pl
from jax.experimental.pallas import tpu as pltpu
from jax.sharding import Mesh, PartitionSpec as P

epsilon = 1e-06
LOG2E = math.log2(math.e)
ALL = ("sp", "kv", "half")
HEADS_PER_DOT = 2
KEY_BLOCK = 512
SMALL = 60.0
MOVED = (7, 10)


def rms_norm(vector, gain_vec):
    return (
        vector * lax.rsqrt(jnp.mean(vector * vector, axis=-1, keepdims=True) + epsilon) * gain_vec
    )


def exchange_kernel(
    kv_ref, q_ref, decay_ref, kv_out, q_out, decay_out, own_sems, kv_send, kv_recv, kv_relay,
    decay_send, decay_recv, decay_relay, q_send, q_recv, *, rows, sizes
):
    sp_count, kv_heads, half_count = sizes
    sp, group, half = lax.axis_index("sp"), lax.axis_index("kv"), lax.axis_index("half")
    core, chips = half % 2, half_count // 2
    partner = (sp, group, half + 1 - 2 * core)

    def device_of(chip):
        return (chip // (kv_heads * chips), (chip // chips) % kv_heads, (chip % chips) * 2 + core)

    def block_of(place):
        return (place[0] * kv_heads + place[1]) * half_count + place[2]

    def kv_copy(source, block, send, device):
        return pltpu.make_async_remote_copy(
            src_ref=source, dst_ref=kv_out.at[pl.ds(pl.multiple_of(block * rows, rows), rows)],
            send_sem=send, recv_sem=kv_recv.at[block], device_id=device,
            device_id_type=pl.DeviceIdType.MESH,
        )

    def decay_copy(source, member, send, device):
        return pltpu.make_async_remote_copy(
            src_ref=source, dst_ref=decay_out.at[member], send_sem=send,
            recv_sem=decay_recv.at[member], device_id=device,
            device_id_type=pl.DeviceIdType.MESH,
        )

    me = block_of((sp, group, half))
    chip = (sp * kv_heads + group) * chips + half // 2
    total = sp_count * kv_heads * chips
    member = sp * half_count + half
    cluster = sp * chips + half // 2
    clusters = sp_count * chips
    started = []
    for k in range(1, total):
        place = device_of((chip + k) % total)
        started.append(kv_copy(kv_ref.at[place[1]], me, kv_send.at[k], place))
        started[-1].start()
    for k in range(1, clusters):
        other = (cluster + k) % clusters
        place = (other // chips, group, (other % chips) * 2 + core)
        started.append(decay_copy(decay_ref, member, decay_send.at[k], place))
        started[-1].start()
    q_copy = pltpu.make_async_remote_copy(
        src_ref=q_ref, dst_ref=q_out, send_sem=q_send, recv_sem=q_recv,
        device_id=(sp_count - 1 - sp, kv_heads - 1 - group, half_count - 1 - half),
        device_id_type=pl.DeviceIdType.MESH,
    )
    q_copy.start()
    started.append(kv_copy(kv_ref.at[group], me, kv_relay.at[0], partner))
    started[-1].start()
    started.append(decay_copy(decay_ref, member, decay_relay.at[0], partner))
    started[-1].start()
    own_kv = pltpu.make_async_copy(
        kv_ref.at[group], kv_out.at[pl.ds(pl.multiple_of(me * rows, rows), rows)], own_sems.at[0]
    )
    own_kv.start()
    own_decay = pltpu.make_async_copy(decay_ref, decay_out.at[member], own_sems.at[1])
    own_decay.start()
    for k in range(1, clusters):
        other = (cluster + clusters - k) % clusters
        which = (other // chips) * half_count + (other % chips) * 2 + core
        landed = decay_out.at[which]
        relay = decay_copy(landed, which, decay_relay.at[k], partner)
        relay.wait_recv()
        relay.start()
        started.append(relay)
    for k in range(1, total):
        block = block_of(device_of((chip + total - k) % total))
        landed = kv_out.at[pl.ds(pl.multiple_of(block * rows, rows), rows)]
        relay = kv_copy(landed, block, kv_relay.at[k], partner)
        relay.wait_recv()
        relay.start()
        started.append(relay)
    for k in range(clusters):
        other = (cluster + clusters - k) % clusters
        which = (other // chips) * half_count + (other % chips) * 2 + 1 - core
        decay_copy(decay_out.at[which], which, decay_relay.at[k], partner).wait_recv()
    for k in range(total):
        place = device_of((chip + total - k) % total)
        block = block_of((place[0], place[1], place[2] + 1 - 2 * core))
        landed = kv_out.at[pl.ds(pl.multiple_of(block * rows, rows), rows)]
        kv_copy(landed, block, kv_relay.at[k], partner).wait_recv()
    for copy in started:
        copy.wait_send()
    own_kv.wait()
    own_decay.wait()
    q_copy.wait()


def attend_kernel(
    place_ref, near_ref, far_ref, row_ref, decay_ref, kv_ref, out_ref, ones_ref, q_ref, peak_ref,
    acc_ref, *, rows, heads, key_block, small
):
    lane = lax.broadcasted_iota(jnp.int32, (rows, 128), 1)
    low = lane < 64
    for r, ref in enumerate((near_ref, far_ref)):
        for pair in range(heads // 2):
            both = ref[:, pair * 128 : (pair + 1) * 128].astype(jnp.float32)
            even = jnp.where(low, both, 0.0)
            odd = jnp.where(low, pltpu.roll(both, 64, 1), 0.0)
            q_ref[r, (2 * pair) * rows : (2 * pair + 1) * rows] = even.astype(jnp.bfloat16)
            q_ref[r, (2 * pair + 1) * rows : (2 * pair + 2) * rows] = odd.astype(jnp.bfloat16)

    def fill(i, carry):
        at = pl.ds(pl.multiple_of(i * key_block, key_block), key_block)
        wide = lax.broadcasted_iota(jnp.int32, (key_block, 128), 1) < 64
        ones_ref[at] = jnp.where(wide, 1.0, kv_ref[at].astype(jnp.float32)).astype(jnp.bfloat16)
        return carry

    lax.fori_loop(0, kv_ref.shape[0] // key_block, fill, 0)
    span = HEADS_PER_DOT * rows

    for r in range(2):
        first = place_ref[r]
        for head in range(heads):
            part = pl.ds(head * rows, rows)
            if small:
                peak_ref[part] = jnp.broadcast_to(row_ref[r, :, head : head + 1], (rows, 128))
            else:
                peak_ref[part] = jnp.full((rows, 128), -1e30, jnp.float32)
        acc_ref[...] = jnp.zeros_like(acc_ref)

        def step(index, masked):
            at = pl.ds(pl.multiple_of(index * key_block, key_block), key_block)
            keys = kv_ref[at]
            values = ones_ref[at]
            for start in range(0, heads, HEADS_PER_DOT):
                part = pl.ds(start * rows, span)
                before = peak_ref[part]
                scores = lax.dot_general(
                    q_ref[r, part], keys, (((1,), (1,)), ((), ())),
                    preferred_element_type=jnp.float32,
                )
                if small:
                    scores = scores + jnp.concatenate([before] * (key_block // 128), axis=1)
                scores = scores.reshape(HEADS_PER_DOT, rows, key_block)
                scores = scores - decay_ref[index, start : start + HEADS_PER_DOT][:, None, :]
                if masked:
                    row = first + lax.broadcasted_iota(jnp.int32, (rows, key_block), 0)
                    col = index * key_block + lax.broadcasted_iota(
                        jnp.int32, (rows, key_block), 1
                    )
                    scores = jnp.where((col <= row)[None], scores, -1e30)
                scores = scores.reshape(span, key_block)
                if small:
                    weights = jnp.exp2(scores).astype(jnp.bfloat16)
                    acc_ref[part] += jnp.dot(weights, values, preferred_element_type=jnp.float32)
                else:
                    after = jnp.maximum(before, jnp.max(scores, axis=1, keepdims=True))
                    weights = jnp.exp2(scores - after[:, :1]).astype(jnp.bfloat16)
                    acc_ref[part] = acc_ref[part] * jnp.exp2(before - after) + jnp.dot(
                        weights, values, preferred_element_type=jnp.float32
                    )
                    peak_ref[part] = after

        full = first // key_block

        def body(index, carry):
            step(index, False)
            return carry

        lax.fori_loop(0, full, body, 0)
        step(full, True)
        for pair in range(heads // 2):
            even = acc_ref[(2 * pair) * rows : (2 * pair + 1) * rows]
            odd = acc_ref[(2 * pair + 1) * rows : (2 * pair + 2) * rows]
            done = jnp.where(low, pltpu.roll(even, 64, 1), odd) / jnp.where(
                low, even, pltpu.roll(odd, 64, 1)
            )
            out_ref[r, :, pair * 128 : (pair + 1) * 128] = done.astype(jnp.bfloat16)


def attend(place, near, far, row_decay, decays, kv, small):
    length = kv.shape[0]
    rows, width = near.shape
    heads, key_block = decays.shape[1:]
    vmem = pl.BlockSpec(memory_space=pltpu.VMEM)
    return pl.pallas_call(
        lambda *refs: attend_kernel(
            *refs, rows=rows, heads=heads, key_block=key_block, small=small
        ),
        out_shape=jax.ShapeDtypeStruct((2, rows, width), jnp.bfloat16),
        in_specs=[pl.BlockSpec(memory_space=pltpu.SMEM)] + [vmem] * 5,
        out_specs=vmem,
        scratch_shapes=[
            pltpu.VMEM((length, 128), jnp.bfloat16),
            pltpu.VMEM((2, heads * rows, 128), jnp.bfloat16),
            pltpu.VMEM((heads * rows, 128), jnp.float32),
            pltpu.VMEM((heads * rows, 128), jnp.float32),
        ],
        compiler_params=pltpu.CompilerParams(vmem_limit_bytes=40 * 1024 * 1024),
        name="attend_small" if small else "attend_any",
    )(place, near, far, row_decay, decays, kv)


def stream_kernel(
    x_hbm, in_gain, wq_hbm, wk_hbm, wv_hbm, query_gain, key_gain, sums_hbm, wo_hbm, out_ref,
    x_ref, wkv_ref, wq_ref, sums_ref, wo_ref, normed_ref, kvt_ref, query_ref, decay_ref, att_ref,
    kvt_all, decay_all, far_decay, in_q, qt_ref, acc_ref, kp_all, vt_all, res_ref, done_ref, sum_ref, loads, kv_recv,
    decay_recv, x_send, own_send, round_send, late_send, far_send, far_recv, q_send, q_recv,
    back_send, back_recv, *, sizes, lines, rows, heads
):
    sp_count, kv_heads, half_count = sizes
    zs, ys = lines
    zh = zs // 2
    upper = sp_count // 2
    pairs = heads // 2
    units = pairs * kv_heads
    width = heads * 64
    span = 2 * rows
    local, chunk_rows = decay_ref.shape
    s, g, j = lax.axis_index("sp"), lax.axis_index("kv"), lax.axis_index("half")
    z, y = s // ys, s % ys
    partner_x = 1 - g
    s_far = sp_count - 1 - s
    is_high = s >= upper

    def share(s_):
        even = (2 * units * (2 * s_ + 1 - sp_count) + 2 * s_ + 1) // (2 * (2 * s_ + 1))
        return even * MOVED[0] // MOVED[1]

    given = jnp.where(is_high, share(jnp.maximum(s, upper)), 0)
    taken = jnp.where(is_high, 0, share(jnp.maximum(s_far, upper)))

    def kept_from(x_):
        return (jnp.maximum(given - x_, 0) + kv_heads - 1) // kv_heads

    def block_at(s_, x_, j_):
        return (s_ * kv_heads + x_) * half_count + j_

    def remote(source, target, send, recv, device):
        return pltpu.make_async_remote_copy(
            src_ref=source, dst_ref=target, send_sem=send, recv_sem=recv, device_id=device,
            device_id_type=pl.DeviceIdType.MESH,
        )

    def kv_copy(source, block, send, device):
        return remote(source, kvt_all.at[block], send, kv_recv.at[block], device)

    def decay_copy(source, member, send, device):
        return remote(source, decay_all.at[member], send, decay_recv.at[member], device)

    here = (s, g, j)
    each = kv_heads + 1

    def one_piece(s_, j_, piece, base, device, sems):
        if piece == kv_heads:
            member = s_ * half_count + j_
            return decay_copy(decay_all.at[member], member, sems.at[base + piece], device)
        block = block_at(s_, piece, j_)
        return kv_copy(kvt_all.at[block], block, sems.at[base + piece], device)

    def arrived(s_, j_):
        for piece in range(each):
            one_piece(s_, j_, piece, 0, here, own_send).wait_recv()

    def start_all(copies):
        for copy in copies:
            copy.start()

    def drain_all(copies):
        for copy in copies:
            copy.wait_send()

    def inside(z_):
        return (z_ >= 0) & (z_ < zs)

    def to_rows(base):
        return [
            (None, base + (n - 1) * each, (z * ys + (y + n) % ys, g, j)) for n in range(1, ys)
        ]

    def to_lanes(base):
        return [
            (None, base + (n - 1) * each, (s, g, (j + n) % half_count))
            for n in range(1, half_count)
        ]

    def relay(s_, routes, sems, go):
        for piece in range(each):
            if go:
                one_piece(s_, j, piece, 0, here, own_send).wait_recv()
            for condition, base, device in routes:
                copy = one_piece(s_, j, piece, base, device, sems)
                act = copy.start if go else copy.wait_send
                if condition is None:
                    act()
                else:
                    pl.when(condition)(act)

    per = 1 + (ys - 1) + (half_count - 1) + (ys - 1) * (half_count - 1)

    def spread(s_, base, condition, device, sems, go):
        routes = [(condition, base, device)]
        routes += to_rows(base + each) + to_lanes(base + ys * each)
        relay(s_, routes, sems, go)

    def across(zo, base, sems, go):
        for m in range(1, ys):
            slot = ys + half_count - 1 + (m - 1) * (half_count - 1)
            relay(zo * ys + (y + m) % ys, to_lanes(base + slot * each), sems, go)

    def round_of(k, go):
        base = (k - 1) * per * each

        @pl.when(inside(z - k))
        def _():
            spread(
                (z - k) * ys + y, base, inside(z + 1), ((z + 1) * ys + y, g, j), round_send, go
            )

        @pl.when(inside(z - k + 1))
        def _():
            across(z - k + 1, base, round_send, go)

    def late(zo, go):
        base = (zo - 1) * per * each
        routes = to_rows(base + each) + to_lanes(base + ys * each)
        relay(zo * ys + y, routes, late_send, go)

    def late_across(zo, go):
        across(zo, (zo - 1) * per * each, late_send, go)

    def build(s_):
        for x_ in range(kv_heads):
            for j_ in range(half_count):
                block = block_at(s_, x_, j_)
                place = (x_ * half_count + j_) * rows
                decays = jnp.concatenate(
                    [
                        decay_all[s_ * half_count + n, :, pl.ds(place, rows)]
                        for n in range(half_count)
                    ],
                    axis=0,
                )
                decays = -decays
                high = decays.astype(jnp.bfloat16).astype(jnp.float32)
                rest = decays - high
                middle = rest.astype(jnp.bfloat16).astype(jnp.float32)
                parts = jnp.concatenate(
                    [high, middle, rest - middle, jnp.ones((8, rows), jnp.float32)], axis=0
                ).astype(jnp.bfloat16)
                wide = jnp.concatenate(
                    [kvt_all[block, 0:64], parts, jnp.zeros((32, rows), jnp.bfloat16)], axis=0
                )
                kp_all[s_, pl.ds(place, rows)] = wide.T
                vt_all[s_, 0:64, pl.ds(place, rows)] = kvt_all[block, 64:128]

    def build_if(s_):
        @pl.when(s_ <= jnp.where(is_high, s, s_far))
        def _():
            build(s_)

    def lanes_of(k):
        @pl.when(inside(z - k))
        def _():
            s_ = (z - k) * ys + y
            for n in range(1, half_count):
                arrived(s_, (j + n) % half_count)
            build_if(s_)

        @pl.when(inside(z - k + 1))
        def _():
            for m in range(1, ys):
                s_ = (z - k + 1) * ys + (y + m) % ys
                for n in range(1, half_count):
                    arrived(s_, (j + n) % half_count)
                build_if(s_)

    def late_lanes(zo):
        for m in range(ys):
            s_ = zo * ys + (y + m) % ys
            for n in range(1, half_count):
                arrived(s_, (j + n) % half_count)
            build_if(s_)

    def q_lanes(group, pair):
        return pl.ds(pl.multiple_of(group * width + pair * 128, 128), 128)

    fetches = [
        pltpu.make_async_copy(source, target, loads.at[n])
        for n, (source, target) in enumerate(
            (
                (x_hbm, x_ref), (wk_hbm, wkv_ref.at[:, 0:128]), (wv_hbm, wkv_ref.at[:, 128:256]),
                (sums_hbm, sums_ref), (wq_hbm, wq_ref), (wo_hbm, wo_ref),
            )
        )
    ]
    for fetch in fetches:
        fetch.start()

    barrier = pltpu.get_barrier_semaphore()

    def greet(device):
        pl.semaphore_signal(
            barrier, inc=1, device_id=device, device_id_type=pl.DeviceIdType.MESH
        )

    greeted = 0
    for n in range(1, half_count):
        greet((s, g, (j + n) % half_count))
        greeted += 1
    greet((s, partner_x, j))
    greeted += 1
    for z_ in range(zs):
        met = ((z_ < z) & (z_ <= zs - 1 - z)) | ((z < z_) & (z <= zs - 1 - z_))

        @pl.when(met)
        def _():
            greet((z_ * ys + y, g, j))

        greeted = greeted + jnp.where(met, 1, 0)
    for n in range(1, ys):
        greet((z * ys + (y + n) % ys, g, j))
        greeted += 1
    for x_ in range(kv_heads):
        for n in range(half_count):
            greet((s_far, x_, n))
            greeted += 1
    for way in (1, -1):

        @pl.when(inside(z + way))
        def _():
            greet(((z + way) * ys + y, g, j))

        greeted = greeted + jnp.where(inside(z + way), 1, 0)

    def columns(gain):
        wide = jnp.broadcast_to(gain.reshape(1, 64), (64, 64))
        wide = jnp.concatenate([wide, wide], axis=1)
        wide = jnp.concatenate([wide, wide], axis=0).T
        return jnp.concatenate([wide[0:64]] * (rows // 128), axis=1)

    def per_head(turned, gain):
        many = turned.reshape(turned.shape[0] // 64, 64, rows)
        mean = jnp.mean(many * many, axis=1, keepdims=True)
        return (many * lax.rsqrt(mean + epsilon) * gain[None]).reshape(turned.shape)

    fetches[0].wait()
    x = x_ref[...].astype(jnp.float32)
    scale = lax.rsqrt(jnp.mean(x * x, axis=1, keepdims=True) + epsilon)
    normed_ref[...] = (x * scale * in_gain[...].reshape(1, -1)).astype(jnp.bfloat16)
    fetches[1].wait()
    fetches[2].wait()
    both = jnp.dot(normed_ref[...], wkv_ref[...], preferred_element_type=jnp.float32).T
    turned_keys = per_head(both[0:128], columns(key_gain[...])).astype(jnp.bfloat16)
    turned_values = both[128:256].astype(jnp.bfloat16)
    for n in range(kv_heads):
        kvt_ref[n, 0:64] = turned_keys[n * 64 : (n + 1) * 64]
        kvt_ref[n, 64:128] = turned_values[n * 64 : (n + 1) * 64]
    fetches[3].wait()
    decay_ref[...] = sums_ref[...] * LOG2E

    def far_q_copy(group, pair):
        unit = kv_heads * pair + g
        slot = jnp.minimum(pairs + unit, 2 * pairs - 1)
        return remote(
            query_ref.at[q_lanes(group, pair)], in_q.at[slot],
            q_send.at[group * pairs + pair], q_recv.at[slot], (s_far, group, j),
        )

    def near_q_copy(pair):
        return remote(
            query_ref.at[q_lanes(partner_x, pair)], in_q.at[pair],
            q_send.at[partner_x * pairs + pair], q_recv.at[pair], (s, partner_x, j),
        )

    def q_arrived(slot):
        remote(
            query_ref.at[pl.ds(0, 128)], in_q.at[slot], q_send.at[0], q_recv.at[slot], here
        ).wait_recv()

    def is_given(pair, x_):
        return kv_heads * pair + x_ < given

    def far_sends(act):
        for pair in range(pairs):
            for group in range(kv_heads):

                @pl.when(is_given(pair, g))
                def _():
                    act([far_q_copy(group, pair)])

    def near_sends(act):
        for pair in range(pairs):

            @pl.when(jnp.logical_not(is_given(pair, g)))
            def _():
                act([near_q_copy(pair)])

    def far_decay_copies():
        copies = []
        for x_ in range(kv_heads):
            for n in range(half_count):
                source = decay_ref.at[:, pl.ds((x_ * half_count + n) * rows, rows)]
                at = x_ * half_count + n
                copies.append(
                    remote(
                        source, far_decay.at[x_ * half_count + j], far_send.at[at],
                        far_recv.at[x_ * half_count + j], (s_far, g, n),
                    )
                )
        return copies

    own_block = block_at(s, g, j)
    other_block = block_at(s, partner_x, j)
    member = s * half_count + j

    def side_targets():
        targets = [(None, (s, g, (j + n) % half_count)) for n in range(1, half_count)]
        targets.append((inside(z + 1), ((z + 1) * ys + y, g, j)))
        targets += [(None, (z * ys + (y + n) % ys, g, j)) for n in range(1, ys)]
        return targets

    def each_down(act):
        for z_ in range(zh - 1, -1, -1):

            @pl.when((z_ < z) & (z_ <= zs - 1 - z))
            def _():
                act((ys + half_count - 1 + z_) * each, (z_ * ys + y, g, j))

    def each_side(act):
        for slot, (condition, device) in enumerate(side_targets()):
            if condition is None:
                act(slot * each, device)
            else:

                @pl.when(condition)
                def _():
                    act(slot * each, device)

    def own_copies(base, device):
        return [
            kv_copy(kvt_ref.at[g], own_block, own_send.at[base], device),
            decay_copy(decay_ref, member, own_send.at[base + 1], device),
        ]

    def other_copies(base, device):
        return [kv_copy(kvt_all.at[other_block], other_block, own_send.at[base + 2], device)]

    x_copy = kv_copy(kvt_ref.at[partner_x], own_block, x_send, (s, partner_x, j))
    pl.semaphore_wait(barrier, greeted)
    x_copy.start()
    each_side(lambda base, device: start_all(own_copies(base, device)))

    @pl.when(z <= zh)
    def _():
        each_down(lambda base, device: start_all(own_copies(base, device)))

    fetches[4].wait()
    query_columns = columns(query_gain[...] * (LOG2E * 64 ** (-0.5)))

    for n in range(query_ref.shape[0] // 256):
        at = pl.ds(n * 256, 256)
        turned = jnp.dot(
            normed_ref[...], wq_ref[:, at], preferred_element_type=jnp.float32
        ).T
        query_ref[at] = per_head(turned, query_columns).astype(jnp.bfloat16)

    @pl.when(z > zh)
    def _():
        far_sends(start_all)

    near_sends(start_all)
    kvt_all[own_block] = kvt_ref[g]
    decay_all[member] = decay_ref[...]
    acc_ref[...] = jnp.zeros_like(acc_ref)
    vt_all[:, 64:80] = jnp.ones((sp_count, 16, chunk_rows), jnp.bfloat16)

    def prepare(t, slot, source, pair, decays):
        turned = source
        high = decays.astype(jnp.bfloat16).astype(jnp.float32)
        rest = decays - high
        middle = rest.astype(jnp.bfloat16).astype(jnp.float32)
        rest = rest - middle
        row = lax.broadcasted_iota(jnp.int32, (64, rows), 0)
        for n in range(2):
            head = 2 * pair + n
            lanes = pl.ds(slot * span + n * rows, rows)
            picked = (row == head) | (row == 8 + head) | (row == 16 + head)
            extra = jnp.where(picked, 1.0, 0.0)
            for at, part in ((24, high), (25, middle), (26, rest)):
                extra = jnp.where(row == at, part[n : n + 1], extra)
            qt_ref[t, 0:64, lanes] = turned[n * 64 : (n + 1) * 64]
            qt_ref[t, 64:128, lanes] = extra.astype(jnp.bfloat16)

    def own_decays(pair, x_):
        first = (2 * pair) % local
        at = pl.ds(pl.multiple_of((x_ * half_count + j) * rows, rows), rows)
        return decay_all[s * half_count + (2 * pair) // local, first : first + 2, at]

    def far_decays(slot):
        pair, x_ = slot // kv_heads, slot % kv_heads
        first = (2 * pair) % local
        return far_decay[x_ * half_count + (2 * pair) // local, first : first + 2]

    def work(t, at, lanes, chunk, start, size, step, limit=None):
        at = pl.ds(pl.multiple_of(at, span), lanes)
        q = qt_ref[t, :, at]
        total = acc_ref[t, :, at]
        for b in range(size // step):
            where = pl.ds(pl.multiple_of(start + b * step, step), step)
            scores = jnp.dot(kp_all[chunk, where], q, preferred_element_type=jnp.float32)
            if limit is not None:
                key = lax.broadcasted_iota(jnp.int32, (step, lanes), 0)
                row = lax.broadcasted_iota(jnp.int32, (step, lanes), 1) % rows
                scores = jnp.where(key <= row + limit, scores, -1e30)
            weights = jnp.exp2(scores).astype(jnp.bfloat16)
            total = total + jnp.dot(
                vt_all[chunk, :, where], weights, preferred_element_type=jnp.float32
            )
        acc_ref[t, :, at] = total

    def whole(t, at, lanes, chunk):
        work(t, at, lanes, chunk, 0, chunk_rows, chunk_rows if lanes == span else chunk_rows // 2)

    def diagonal(t, at, lanes, chunk, offset):
        def body(i, carry):
            work(t, at, lanes, chunk, i * span, span, span, offset - i * span)
            return carry

        lax.fori_loop(0, offset // span + 1, body, 0)

    def finished(t, slot):
        out = []
        for n in range(2):
            lanes = pl.ds(slot * span + n * rows, rows)
            out.append(acc_ref[t, 0:64, lanes] / acc_ref[t, 64:65, lanes])
        return jnp.concatenate(out, axis=0).T.astype(jnp.bfloat16)

    def back_copy(slot, pair, device):
        return remote(
            res_ref.at[slot], att_ref.at[:, q_lanes(g, pair)], back_send.at[slot],
            back_recv.at[g * pairs + pair], device,
        )

    def back_arrived(group, pair):
        remote(
            res_ref.at[0], att_ref.at[:, q_lanes(group, pair)], back_send.at[0],
            back_recv.at[group * pairs + pair], here,
        ).wait_recv()

    assert MOVED[0] * pairs // MOVED[1] <= kv_heads

    def kept_groups(first, act):
        @pl.when(first == 0)
        def _():
            act(0, pairs * span)

        @pl.when(first > 0)
        def _():
            act(span, (pairs - 1) * span)

    def taken_groups(act):
        @pl.when(taken == 2)
        def _():
            act(0, 2 * span)

        @pl.when(taken == 1)
        def _():
            act(0, span)

    my_first = kept_from(g)
    partner_first = kept_from(partner_x)
    offset = (g * half_count + j) * rows
    partner_offset = (partner_x * half_count + j) * rows

    kv_copy(kvt_ref.at[g], other_block, x_send, here).wait_recv()
    each_side(lambda base, device: start_all(other_copies(base, device)))

    @pl.when(z <= zh)
    def _():
        each_down(lambda base, device: start_all(other_copies(base, device)))

    @pl.when(z == zh)
    def _():
        far_sends(start_all)

    @pl.when(is_high)
    def _():
        start_all(far_decay_copies())

    for n in range(1, half_count):
        arrived(s, (j + n) % half_count)
    build(s)
    for pair in range(pairs):
        prepare(0, pair, query_ref[q_lanes(g, pair)], pair, own_decays(pair, g))
    def at_step(k):
        return s - jnp.where(y == 0, jnp.where(k == 1, ys, jnp.where(k == ys, 1, k)), k)

    def comes(zo):
        return (z < zh) & (zo > z) & (zo <= zs - 1 - z)

    first_steps = 2 * (zs + 1)
    left = jnp.maximum(s - zs + 1, 0)

    def item(f, carry):
        early = f < first_steps
        late_f = f - first_steps
        k = f // 2
        turn = jnp.where(early, f % 2, jnp.where(late_f < left, 1, 0))
        step = jnp.where(
            early, k - turn, jnp.where(late_f < left, zs + late_f, zs + late_f - left)
        )
        idle = early & (turn == 0) & (k == zs) & (s >= zs)

        @pl.when(early & (turn == 0) & (k > 0))
        def _():
            @pl.when((k == 2) & (z > zh))
            def _():
                each_down(
                    lambda base, device: start_all(
                        own_copies(base, device) + other_copies(base, device)
                    )
                )

            lanes_of(k)
            for here_too, when, duty, zo in (
                (z == 0, 1, late, z + 1), (z == 0, 3, late, z + 2),
                (z > 0, 2, late, z + 1), (z > 0, 4, late_across, z + 1),
            ):

                @pl.when(here_too & (k == when) & comes(zo))
                def _():
                    duty(zo, True)

        @pl.when(early & (turn == 1))
        def _():
            @pl.when(k < zs)
            def _():
                round_of(k + 1, True)

            @pl.when(k == 1)
            def _():
                for n in range(pairs):

                    @pl.when(partner_first <= n)
                    def _():
                        q_arrived(n)
                        prepare(1, n, in_q[n], n, own_decays(n, partner_x))

        kept = jnp.where(turn == 0, my_first, partner_first)
        start = jnp.where(turn == 0, offset, partner_offset)

        @pl.when(step == 0)
        def _():
            kept_groups(kept, lambda at, lanes: diagonal(turn, at, lanes, s, start))

        @pl.when((step > 0) & (step <= s) & jnp.logical_not(idle))
        def _():
            kept_groups(kept, lambda at, lanes: whole(turn, at, lanes, at_step(step)))

        @pl.when((step == s) & (turn == 0) & jnp.logical_not(idle))
        def _():
            for pair in range(pairs):

                @pl.when(pair >= my_first)
                def _():
                    att_ref[:, q_lanes(g, pair)] = finished(0, pair)

        @pl.when((step == s) & (turn == 1))
        def _():
            for n in range(pairs):

                @pl.when(partner_first <= n)
                def _():
                    res_ref[n] = finished(1, n)
                    back_copy(n, n, (s, partner_x, j)).start()

        return carry

    lax.fori_loop(0, first_steps + 2 * left, item, 0)

    def far_phase():
        for n in range(kv_heads * half_count):
            remote(
                decay_ref.at[:, pl.ds(0, rows)], far_decay.at[n], far_send.at[n],
                far_recv.at[n], here,
            ).wait_recv()

        for n in range(pairs):

            @pl.when(n < taken)
            def _():
                q_arrived(pairs + n)
                prepare(2, n, in_q[pairs + n], n // kv_heads, far_decays(n))

        def zone(zo, carry):
            def body(i, carry):
                chunk = zo * ys + i

                @pl.when(chunk < s_far)
                def _():
                    taken_groups(lambda at, lanes: whole(2, at, lanes, chunk))

                for place, ahead, duty, zl in (
                    (0, 0, late_across, z + 1), (0, 1, late, z + 3), (ys - 1, 1, late_across, z + 2),
                    (0, 2, late_across, z + 3),
                ):

                    @pl.when((z == 0) & (i == place) & (zo == ahead) & comes(zl))
                    def _():
                        duty(zl, True)

                return carry

            lax.fori_loop(0, ys, body, 0)

            @pl.when(comes(zo + 1) & (zo > jnp.where(z == 0, 2, z)))
            def _():
                late(zo + 1, True)
                late_across(zo + 1, True)

            @pl.when(comes(zo + 1))
            def _():
                late_lanes(zo + 1)

            return carry

        lax.fori_loop(0, zs - z, zone, 0)

        def close(n, carry):
            unit_x = n % kv_heads
            diagonal(2, n * span, span, s_far, (unit_x * half_count + j) * rows)
            for m in range(pairs):

                @pl.when(n == m)
                def _():
                    res_ref[pairs + m] = finished(2, m)
                    back_copy(
                        pairs + m, m // kv_heads, (s_far, m % kv_heads, j)
                    ).start()

            return carry

        lax.fori_loop(0, taken, close, 0)

    @pl.when(z < zh)
    def _():
        far_phase()

    fetches[5].wait()
    for pair in range(1, pairs):
        back_arrived(partner_x, pair)

    firsts = [pl.ds(n * width, 128) for n in range(kv_heads)]
    others = [pl.ds(n * width + 128, width - 128) for n in range(kv_heads)]
    quarter = wo_ref.shape[1] // 4

    def output(parts, at):
        rows_in = jnp.concatenate([att_ref[:, part] for part in parts], axis=1)
        weights_in = jnp.concatenate([wo_ref[part, at] for part in parts], axis=0)
        return jnp.dot(rows_in, weights_in, preferred_element_type=jnp.float32)

    for n in range(4):
        at = pl.ds(n * quarter, quarter)
        sum_ref[:, at] = output(others, at)

    @pl.when(my_first > 0)
    def _():
        back_arrived(g, 0)

    back_arrived(partner_x, 0)
    puts = []
    for n in range(4):
        at = pl.ds(n * quarter, quarter)
        done_ref[:, at] = (sum_ref[:, at] + output(firsts, at)).astype(jnp.bfloat16)
        puts.append(pltpu.make_async_copy(done_ref.at[:, at], out_ref.at[:, at], loads.at[n]))
        puts[n].start()
    x_copy.wait_send()
    each_side(
        lambda base, device: drain_all(own_copies(base, device) + other_copies(base, device))
    )

    each_down(
        lambda base, device: drain_all(own_copies(base, device) + other_copies(base, device))
    )

    def drain(k, carry):
        round_of(k, False)
        return carry

    lax.fori_loop(1, zs + 1, drain, 0)

    def drain_late(zo, carry):
        late(zo, False)
        late_across(zo, False)
        return carry

    @pl.when(z < zh)
    def _():
        lax.fori_loop(z + 1, zs - z, drain_late, 0)


    @pl.when(is_high)
    def _():
        far_sends(drain_all)
        drain_all(far_decay_copies())

    near_sends(drain_all)
    for pair in range(pairs):

        @pl.when(partner_first <= pair)
        def _():
            back_copy(pair, pair, (s, partner_x, j)).wait_send()

        @pl.when(pair < taken)
        def _():
            back_copy(
                pairs + pair, pair // kv_heads, (s_far, pair % kv_heads, j)
            ).wait_send()
    for put in puts:
        put.wait()


def lines_of(sp_count):
    ys = 1 << ((sp_count.bit_length() - 1) // 2)
    return sp_count // ys, ys


def stream(
    inputs, in_gain, w_query, w_key, w_value, query_gain, key_gain, decay_sums, w_out, sizes
):
    sp_count, kv_heads, half_count = sizes
    rows, model = inputs.shape
    width = w_query.shape[1]
    heads = width // 64 // kv_heads
    local, chunk_rows = decay_sums.shape
    zs, ys = lines_of(sp_count)
    pairs = heads // 2
    count = sp_count * kv_heads * half_count
    members = sp_count * half_count
    per = 1 + (ys - 1) + (half_count - 1) + (ys - 1) * (half_count - 1)
    each = kv_heads + 1
    vmem = pl.BlockSpec(memory_space=pltpu.VMEM)
    hbm = pl.BlockSpec(memory_space=pltpu.MemorySpace.HBM)
    dma = pltpu.SemaphoreType.DMA
    return pl.pallas_call(
        lambda *refs: stream_kernel(
            *refs, sizes=sizes, lines=(zs, ys), rows=rows, heads=heads
        ),
        out_shape=jax.ShapeDtypeStruct((rows, w_out.shape[1]), jnp.bfloat16),
        in_specs=[hbm, vmem, hbm, hbm, hbm, vmem, vmem, hbm, hbm],
        out_specs=hbm,
        scratch_shapes=[
            pltpu.VMEM((rows, model), jnp.bfloat16),
            pltpu.VMEM((model, 256), jnp.bfloat16),
            pltpu.VMEM(w_query.shape, jnp.bfloat16),
            pltpu.VMEM(decay_sums.shape, jnp.float32),
            pltpu.VMEM(w_out.shape, jnp.bfloat16),
            pltpu.VMEM((rows, model), jnp.bfloat16),
            pltpu.VMEM((kv_heads, 128, rows), jnp.bfloat16),
            pltpu.VMEM((width, rows), jnp.bfloat16),
            pltpu.VMEM((local, chunk_rows), jnp.float32),
            pltpu.VMEM((rows, width), jnp.bfloat16),
            pltpu.VMEM((count, 128, rows), jnp.bfloat16),
            pltpu.VMEM((members, local, chunk_rows), jnp.float32),
            pltpu.VMEM((kv_heads * half_count, local, rows), jnp.float32),
            pltpu.VMEM((2 * pairs, 128, rows), jnp.bfloat16),
            pltpu.VMEM((3, 128, heads * rows), jnp.bfloat16),
            pltpu.VMEM((3, 80, heads * rows), jnp.float32),
            pltpu.VMEM((sp_count, chunk_rows, 128), jnp.bfloat16),
            pltpu.VMEM((sp_count, 80, chunk_rows), jnp.bfloat16),
            pltpu.VMEM((2 * pairs, rows, 128), jnp.bfloat16),
            pltpu.VMEM((rows, w_out.shape[1]), jnp.bfloat16),
            pltpu.VMEM((rows, w_out.shape[1]), jnp.float32),
            dma((6,)),
            dma((count,)), dma((members,)), dma, dma(((ys + half_count + zs // 2) * each,)),
            dma((zs * per * each,)), dma((zs * per * each,)),
            dma((kv_heads * half_count,)), dma((kv_heads * half_count,)),
            dma((2 * pairs,)), dma((2 * pairs,)), dma((2 * pairs,)), dma((2 * pairs,)),
        ],
        compiler_params=pltpu.CompilerParams(
            has_side_effects=True, collective_id=0, vmem_limit_bytes=56 * 1024 * 1024
        ),
        name="stream",
    )(inputs, in_gain, w_query, w_key, w_value, query_gain, key_gain, decay_sums, w_out)


def any_scores(queries, kv_blocks, decays, sizes):
    sp_count, kv_heads, half_count = sizes
    group = lax.axis_index("kv")
    me = (lax.axis_index("sp") * kv_heads + group) * half_count + lax.axis_index("half")
    count = sp_count * kv_heads * half_count
    mirror = [(i, count - 1 - i) for i in range(count)]
    rows = queries.shape[0]
    length = rows * count
    heads = queries.shape[1] // 64 // kv_heads
    width = heads * 64
    members = sp_count * half_count
    key_block = math.gcd(length, KEY_BLOCK)

    def choose(a, b):
        return jnp.where(group == 0, a, b)

    decay_rows = decays.reshape(-1, 128)
    own_q = choose(queries[:, :width], queries[:, width:])
    sent_q = choose(queries[:, width:], queries[:, :width])
    vmem = pl.BlockSpec(memory_space=pltpu.VMEM)
    chips = count // 2
    dma = pltpu.SemaphoreType.DMA
    kv, far_q, decay_all = pl.pallas_call(
        lambda *refs: exchange_kernel(*refs, rows=rows, sizes=sizes),
        out_shape=(
            jax.ShapeDtypeStruct((length, 128), jnp.bfloat16),
            jax.ShapeDtypeStruct((rows, width), jnp.bfloat16),
            jax.ShapeDtypeStruct((members, *decay_rows.shape), jnp.float32),
        ),
        in_specs=[vmem] * 3,
        out_specs=(vmem,) * 3,
        scratch_shapes=[
            dma((2,)), dma((chips,)), dma((count,)), dma((chips,)), dma((members // 2,)),
            dma((members,)), dma((members // 2,)), dma, dma,
        ],
        compiler_params=pltpu.CompilerParams(has_side_effects=True),
        name="exchange",
    )(kv_blocks, sent_q, decay_rows)
    decay_all = decay_all.reshape(sp_count, heads, -1, key_block)
    decay_all = decay_all.transpose(0, 2, 1, 3).reshape(length // key_block, heads, key_block)
    firsts = (me * rows, (count - 1 - me) * rows)
    place = jnp.stack(firsts).astype(jnp.int32)
    row_decay = jnp.stack(
        [
            lax.dynamic_slice(
                decay_all, (first // key_block, 0, first % key_block), (1, heads, rows)
            )[0].T
            for first in firsts
        ]
    )
    attended = attend(place, own_q, far_q, row_decay, decay_all, kv, False)
    back = lax.ppermute(attended[1], ALL, mirror)
    return choose(
        jnp.concatenate([attended[0], back], axis=1), jnp.concatenate([back, attended[0]], axis=1)
    )


def any_program(
    inputs, in_gain, w_query, w_key, w_value, query_gain, key_gain, decay_sums, w_out, sizes
):
    kv_heads = sizes[1]
    head_size = query_gain.shape[0]
    rows = inputs.shape[0]
    all_heads = w_query.shape[1] // head_size

    normed = rms_norm(inputs.astype(jnp.float32), in_gain).astype(jnp.bfloat16)
    keys = rms_norm(
        jnp.dot(normed, w_key, preferred_element_type=jnp.float32).reshape(
            rows, kv_heads, head_size
        ),
        key_gain,
    ).astype(jnp.bfloat16)
    values = (
        jnp.dot(normed, w_value, preferred_element_type=jnp.float32)
        .astype(jnp.bfloat16)
        .reshape(rows, kv_heads, head_size)
    )
    kv_blocks = jnp.concatenate([keys, values], axis=2).transpose(1, 0, 2)
    queries = rms_norm(
        jnp.dot(normed, w_query, preferred_element_type=jnp.float32).reshape(
            rows, all_heads, head_size
        ),
        query_gain * (LOG2E * head_size ** (-0.5)),
    ).astype(jnp.bfloat16).reshape(rows, all_heads * head_size)
    whole = any_scores(queries, kv_blocks, decay_sums.T * LOG2E, sizes)
    return jnp.dot(whole, w_out, preferred_element_type=jnp.float32).astype(jnp.bfloat16)


def per_device(*arrays):
    query_gain, key_gain = arrays[5:7]
    sizes = (lax.axis_size("sp"), lax.axis_size("kv"), lax.axis_size("half"))
    most = jnp.max(query_gain[:, None] * key_gain[None, :])
    bound = query_gain.shape[0] ** 0.5 * LOG2E * most
    return lax.cond(
        bound <= SMALL,
        lambda *given: stream(*given[:7], given[7].T, given[8], sizes),
        lambda *given: any_program(*given, sizes),
        *arrays,
    )


def solution(mesh):
    sp_count, tp_count = mesh.devices.shape
    split = Mesh(mesh.devices.reshape(sp_count, 2, tp_count // 2), ALL)
    placed = (P(ALL, None), P(), P(), P(), P(), P(), P(), P("sp", ("kv", "half")), P())
    return jax.shard_map(
        per_device, mesh=split, in_specs=placed, out_specs=P(ALL, None), check_vma=False
    )
```

```python
import math

import jax
import jax.numpy as jnp
from jax import lax
from jax.experimental import pallas as pl
from jax.experimental.pallas import tpu as pltpu
from jax.sharding import Mesh, PartitionSpec as P

epsilon = 1e-06
LOG2E = math.log2(math.e)
ALL = ("sp", "kv", "half")
HEADS_PER_DOT = 2
KEY_BLOCK = 512
SMALL = 60.0
MOVED = (7, 10)


def rms_norm(vector, gain_vec):
    return (
        vector * lax.rsqrt(jnp.mean(vector * vector, axis=-1, keepdims=True) + epsilon) * gain_vec
    )


def exchange_kernel(
    kv_ref, q_ref, decay_ref, kv_out, q_out, decay_out, own_sems, kv_send, kv_recv, kv_relay,
    decay_send, decay_recv, decay_relay, q_send, q_recv, *, rows, sizes
):
    sp_count, kv_heads, half_count = sizes
    sp, group, half = lax.axis_index("sp"), lax.axis_index("kv"), lax.axis_index("half")
    core, chips = half % 2, half_count // 2
    partner = (sp, group, half + 1 - 2 * core)

    def device_of(chip):
        return (chip // (kv_heads * chips), (chip // chips) % kv_heads, (chip % chips) * 2 + core)

    def block_of(place):
        return (place[0] * kv_heads + place[1]) * half_count + place[2]

    def kv_copy(source, block, send, device):
        return pltpu.make_async_remote_copy(
            src_ref=source, dst_ref=kv_out.at[pl.ds(pl.multiple_of(block * rows, rows), rows)],
            send_sem=send, recv_sem=kv_recv.at[block], device_id=device,
            device_id_type=pl.DeviceIdType.MESH,
        )

    def decay_copy(source, member, send, device):
        return pltpu.make_async_remote_copy(
            src_ref=source, dst_ref=decay_out.at[member], send_sem=send,
            recv_sem=decay_recv.at[member], device_id=device,
            device_id_type=pl.DeviceIdType.MESH,
        )

    me = block_of((sp, group, half))
    chip = (sp * kv_heads + group) * chips + half // 2
    total = sp_count * kv_heads * chips
    member = sp * half_count + half
    cluster = sp * chips + half // 2
    clusters = sp_count * chips
    started = []
    for k in range(1, total):
        place = device_of((chip + k) % total)
        started.append(kv_copy(kv_ref.at[place[1]], me, kv_send.at[k], place))
        started[-1].start()
    for k in range(1, clusters):
        other = (cluster + k) % clusters
        place = (other // chips, group, (other % chips) * 2 + core)
        started.append(decay_copy(decay_ref, member, decay_send.at[k], place))
        started[-1].start()
    q_copy = pltpu.make_async_remote_copy(
        src_ref=q_ref, dst_ref=q_out, send_sem=q_send, recv_sem=q_recv,
        device_id=(sp_count - 1 - sp, kv_heads - 1 - group, half_count - 1 - half),
        device_id_type=pl.DeviceIdType.MESH,
    )
    q_copy.start()
    started.append(kv_copy(kv_ref.at[group], me, kv_relay.at[0], partner))
    started[-1].start()
    started.append(decay_copy(decay_ref, member, decay_relay.at[0], partner))
    started[-1].start()
    own_kv = pltpu.make_async_copy(
        kv_ref.at[group], kv_out.at[pl.ds(pl.multiple_of(me * rows, rows), rows)], own_sems.at[0]
    )
    own_kv.start()
    own_decay = pltpu.make_async_copy(decay_ref, decay_out.at[member], own_sems.at[1])
    own_decay.start()
    for k in range(1, clusters):
        other = (cluster + clusters - k) % clusters
        which = (other // chips) * half_count + (other % chips) * 2 + core
        landed = decay_out.at[which]
        relay = decay_copy(landed, which, decay_relay.at[k], partner)
        relay.wait_recv()
        relay.start()
        started.append(relay)
    for k in range(1, total):
        block = block_of(device_of((chip + total - k) % total))
        landed = kv_out.at[pl.ds(pl.multiple_of(block * rows, rows), rows)]
        relay = kv_copy(landed, block, kv_relay.at[k], partner)
        relay.wait_recv()
        relay.start()
        started.append(relay)
    for k in range(clusters):
        other = (cluster + clusters - k) % clusters
        which = (other // chips) * half_count + (other % chips) * 2 + 1 - core
        decay_copy(decay_out.at[which], which, decay_relay.at[k], partner).wait_recv()
    for k in range(total):
        place = device_of((chip + total - k) % total)
        block = block_of((place[0], place[1], place[2] + 1 - 2 * core))
        landed = kv_out.at[pl.ds(pl.multiple_of(block * rows, rows), rows)]
        kv_copy(landed, block, kv_relay.at[k], partner).wait_recv()
    for copy in started:
        copy.wait_send()
    own_kv.wait()
    own_decay.wait()
    q_copy.wait()


def attend_kernel(
    place_ref, near_ref, far_ref, row_ref, decay_ref, kv_ref, out_ref, ones_ref, q_ref, peak_ref,
    acc_ref, *, rows, heads, key_block, small
):
    lane = lax.broadcasted_iota(jnp.int32, (rows, 128), 1)
    low = lane < 64
    for r, ref in enumerate((near_ref, far_ref)):
        for pair in range(heads // 2):
            both = ref[:, pair * 128 : (pair + 1) * 128].astype(jnp.float32)
            even = jnp.where(low, both, 0.0)
            odd = jnp.where(low, pltpu.roll(both, 64, 1), 0.0)
            q_ref[r, (2 * pair) * rows : (2 * pair + 1) * rows] = even.astype(jnp.bfloat16)
            q_ref[r, (2 * pair + 1) * rows : (2 * pair + 2) * rows] = odd.astype(jnp.bfloat16)

    def fill(i, carry):
        at = pl.ds(pl.multiple_of(i * key_block, key_block), key_block)
        wide = lax.broadcasted_iota(jnp.int32, (key_block, 128), 1) < 64
        ones_ref[at] = jnp.where(wide, 1.0, kv_ref[at].astype(jnp.float32)).astype(jnp.bfloat16)
        return carry

    lax.fori_loop(0, kv_ref.shape[0] // key_block, fill, 0)
    span = HEADS_PER_DOT * rows

    for r in range(2):
        first = place_ref[r]
        for head in range(heads):
            part = pl.ds(head * rows, rows)
            if small:
                peak_ref[part] = jnp.broadcast_to(row_ref[r, :, head : head + 1], (rows, 128))
            else:
                peak_ref[part] = jnp.full((rows, 128), -1e30, jnp.float32)
        acc_ref[...] = jnp.zeros_like(acc_ref)

        def step(index, masked):
            at = pl.ds(pl.multiple_of(index * key_block, key_block), key_block)
            keys = kv_ref[at]
            values = ones_ref[at]
            for start in range(0, heads, HEADS_PER_DOT):
                part = pl.ds(start * rows, span)
                before = peak_ref[part]
                scores = lax.dot_general(
                    q_ref[r, part], keys, (((1,), (1,)), ((), ())),
                    preferred_element_type=jnp.float32,
                )
                if small:
                    scores = scores + jnp.concatenate([before] * (key_block // 128), axis=1)
                scores = scores.reshape(HEADS_PER_DOT, rows, key_block)
                scores = scores - decay_ref[index, start : start + HEADS_PER_DOT][:, None, :]
                if masked:
                    row = first + lax.broadcasted_iota(jnp.int32, (rows, key_block), 0)
                    col = index * key_block + lax.broadcasted_iota(
                        jnp.int32, (rows, key_block), 1
                    )
                    scores = jnp.where((col <= row)[None], scores, -1e30)
                scores = scores.reshape(span, key_block)
                if small:
                    weights = jnp.exp2(scores).astype(jnp.bfloat16)
                    acc_ref[part] += jnp.dot(weights, values, preferred_element_type=jnp.float32)
                else:
                    after = jnp.maximum(before, jnp.max(scores, axis=1, keepdims=True))
                    weights = jnp.exp2(scores - after[:, :1]).astype(jnp.bfloat16)
                    acc_ref[part] = acc_ref[part] * jnp.exp2(before - after) + jnp.dot(
                        weights, values, preferred_element_type=jnp.float32
                    )
                    peak_ref[part] = after

        full = first // key_block

        def body(index, carry):
            step(index, False)
            return carry

        lax.fori_loop(0, full, body, 0)
        step(full, True)
        for pair in range(heads // 2):
            even = acc_ref[(2 * pair) * rows : (2 * pair + 1) * rows]
            odd = acc_ref[(2 * pair + 1) * rows : (2 * pair + 2) * rows]
            done = jnp.where(low, pltpu.roll(even, 64, 1), odd) / jnp.where(
                low, even, pltpu.roll(odd, 64, 1)
            )
            out_ref[r, :, pair * 128 : (pair + 1) * 128] = done.astype(jnp.bfloat16)


def attend(place, near, far, row_decay, decays, kv, small):
    length = kv.shape[0]
    rows, width = near.shape
    heads, key_block = decays.shape[1:]
    vmem = pl.BlockSpec(memory_space=pltpu.VMEM)
    return pl.pallas_call(
        lambda *refs: attend_kernel(
            *refs, rows=rows, heads=heads, key_block=key_block, small=small
        ),
        out_shape=jax.ShapeDtypeStruct((2, rows, width), jnp.bfloat16),
        in_specs=[pl.BlockSpec(memory_space=pltpu.SMEM)] + [vmem] * 5,
        out_specs=vmem,
        scratch_shapes=[
            pltpu.VMEM((length, 128), jnp.bfloat16),
            pltpu.VMEM((2, heads * rows, 128), jnp.bfloat16),
            pltpu.VMEM((heads * rows, 128), jnp.float32),
            pltpu.VMEM((heads * rows, 128), jnp.float32),
        ],
        compiler_params=pltpu.CompilerParams(vmem_limit_bytes=40 * 1024 * 1024),
        name="attend_small" if small else "attend_any",
    )(place, near, far, row_decay, decays, kv)


def stream_kernel(
    x_hbm, in_gain, wq_hbm, wk_hbm, wv_hbm, query_gain, key_gain, sums_hbm, wo_hbm, out_ref,
    x_ref, wkv_ref, wq_ref, sums_ref, wo_ref, normed_ref, kvt_ref, query_ref, decay_ref, att_ref,
    kvt_all, decay_all, far_decay, in_q, qt_ref, acc_ref, kp_all, vt_all, res_ref, done_ref, sum_ref, loads, kv_recv,
    decay_recv, x_send, own_send, round_send, late_send, far_send, far_recv, q_send, q_recv,
    back_send, back_recv, *, sizes, lines, rows, heads
):
    sp_count, kv_heads, half_count = sizes
    zs, ys = lines
    zh = zs // 2
    upper = sp_count // 2
    pairs = heads // 2
    units = pairs * kv_heads
    width = heads * 64
    span = 2 * rows
    local, chunk_rows = decay_ref.shape
    s, g, j = lax.axis_index("sp"), lax.axis_index("kv"), lax.axis_index("half")
    z, y = s // ys, s % ys
    partner_x = 1 - g
    s_far = sp_count - 1 - s
    is_high = s >= upper

    def share(s_):
        even = (2 * units * (2 * s_ + 1 - sp_count) + 2 * s_ + 1) // (2 * (2 * s_ + 1))
        return even * MOVED[0] // MOVED[1]

    given = jnp.where(is_high, share(jnp.maximum(s, upper)), 0)
    taken = jnp.where(is_high, 0, share(jnp.maximum(s_far, upper)))

    def kept_from(x_):
        return (jnp.maximum(given - x_, 0) + kv_heads - 1) // kv_heads

    def block_at(s_, x_, j_):
        return (s_ * kv_heads + x_) * half_count + j_

    def remote(source, target, send, recv, device):
        return pltpu.make_async_remote_copy(
            src_ref=source, dst_ref=target, send_sem=send, recv_sem=recv, device_id=device,
            device_id_type=pl.DeviceIdType.MESH,
        )

    def kv_copy(source, block, send, device):
        return remote(source, kvt_all.at[block], send, kv_recv.at[block], device)

    def decay_copy(source, member, send, device):
        return remote(source, decay_all.at[member], send, decay_recv.at[member], device)

    here = (s, g, j)
    each = kv_heads + 1

    def one_piece(s_, j_, piece, base, device, sems):
        if piece == kv_heads:
            member = s_ * half_count + j_
            return decay_copy(decay_all.at[member], member, sems.at[base + piece], device)
        block = block_at(s_, piece, j_)
        return kv_copy(kvt_all.at[block], block, sems.at[base + piece], device)

    def arrived(s_, j_):
        for piece in range(each):
            one_piece(s_, j_, piece, 0, here, own_send).wait_recv()

    def start_all(copies):
        for copy in copies:
            copy.start()

    def drain_all(copies):
        for copy in copies:
            copy.wait_send()

    def inside(z_):
        return (z_ >= 0) & (z_ < zs)

    def to_rows(base):
        return [
            (None, base + (n - 1) * each, (z * ys + (y + n) % ys, g, j)) for n in range(1, ys)
        ]

    def to_lanes(base):
        return [
            (None, base + (n - 1) * each, (s, g, (j + n) % half_count))
            for n in range(1, half_count)
        ]

    def relay(s_, routes, sems, go):
        for piece in range(each):
            if go:
                one_piece(s_, j, piece, 0, here, own_send).wait_recv()
            for condition, base, device in routes:
                copy = one_piece(s_, j, piece, base, device, sems)
                act = copy.start if go else copy.wait_send
                if condition is None:
                    act()
                else:
                    pl.when(condition)(act)

    per = 1 + (ys - 1) + (half_count - 1) + (ys - 1) * (half_count - 1)

    def spread(s_, base, condition, device, sems, go):
        routes = [(condition, base, device)]
        routes += to_rows(base + each) + to_lanes(base + ys * each)
        relay(s_, routes, sems, go)

    def across(zo, base, sems, go):
        for m in range(1, ys):
            slot = ys + half_count - 1 + (m - 1) * (half_count - 1)
            relay(zo * ys + (y + m) % ys, to_lanes(base + slot * each), sems, go)

    def round_of(k, go):
        base = (k - 1) * per * each

        @pl.when(inside(z - k))
        def _():
            spread(
                (z - k) * ys + y, base, inside(z + 1), ((z + 1) * ys + y, g, j), round_send, go
            )

        @pl.when(inside(z - k + 1))
        def _():
            across(z - k + 1, base, round_send, go)

    def late(zo, go):
        base = (zo - 1) * per * each
        routes = to_rows(base + each) + to_lanes(base + ys * each)
        relay(zo * ys + y, routes, late_send, go)

    def late_across(zo, go):
        across(zo, (zo - 1) * per * each, late_send, go)

    def build(s_):
        for x_ in range(kv_heads):
            for j_ in range(half_count):
                block = block_at(s_, x_, j_)
                place = (x_ * half_count + j_) * rows
                decays = jnp.concatenate(
                    [
                        decay_all[s_ * half_count + n, :, pl.ds(place, rows)]
                        for n in range(half_count)
                    ],
                    axis=0,
                )
                decays = -decays
                high = decays.astype(jnp.bfloat16).astype(jnp.float32)
                rest = decays - high
                middle = rest.astype(jnp.bfloat16).astype(jnp.float32)
                parts = jnp.concatenate(
                    [high, middle, rest - middle, jnp.ones((8, rows), jnp.float32)], axis=0
                ).astype(jnp.bfloat16)
                wide = jnp.concatenate(
                    [kvt_all[block, 0:64], parts, jnp.zeros((32, rows), jnp.bfloat16)], axis=0
                )
                kp_all[s_, pl.ds(place, rows)] = wide.T
                vt_all[s_, 0:64, pl.ds(place, rows)] = kvt_all[block, 64:128]

    def build_if(s_):
        @pl.when(s_ <= jnp.where(is_high, s, s_far))
        def _():
            build(s_)

    def lanes_of(k):
        @pl.when(inside(z - k))
        def _():
            s_ = (z - k) * ys + y
            for n in range(1, half_count):
                arrived(s_, (j + n) % half_count)
            build_if(s_)

        @pl.when(inside(z - k + 1))
        def _():
            for m in range(1, ys):
                s_ = (z - k + 1) * ys + (y + m) % ys
                for n in range(1, half_count):
                    arrived(s_, (j + n) % half_count)
                build_if(s_)

    def late_lanes(zo):
        for m in range(ys):
            s_ = zo * ys + (y + m) % ys
            for n in range(1, half_count):
                arrived(s_, (j + n) % half_count)
            build_if(s_)

    def q_lanes(group, pair):
        return pl.ds(pl.multiple_of(group * width + pair * 128, 128), 128)

    fetches = [
        pltpu.make_async_copy(source, target, loads.at[n])
        for n, (source, target) in enumerate(
            (
                (x_hbm, x_ref), (wk_hbm, wkv_ref.at[:, 0:128]), (wv_hbm, wkv_ref.at[:, 128:256]),
                (sums_hbm, sums_ref), (wq_hbm, wq_ref), (wo_hbm, wo_ref),
            )
        )
    ]
    for fetch in fetches:
        fetch.start()

    barrier = pltpu.get_barrier_semaphore()

    def greet(device):
        pl.semaphore_signal(
            barrier, inc=1, device_id=device, device_id_type=pl.DeviceIdType.MESH
        )

    greeted = 0
    for n in range(1, half_count):
        greet((s, g, (j + n) % half_count))
        greeted += 1
    greet((s, partner_x, j))
    greeted += 1
    for z_ in range(zs):
        met = ((z_ < z) & (z_ <= zs - 1 - z)) | ((z < z_) & (z <= zs - 1 - z_))

        @pl.when(met)
        def _():
            greet((z_ * ys + y, g, j))

        greeted = greeted + jnp.where(met, 1, 0)
    for n in range(1, ys):
        greet((z * ys + (y + n) % ys, g, j))
        greeted += 1
    for x_ in range(kv_heads):
        for n in range(half_count):
            greet((s_far, x_, n))
            greeted += 1
    for way in (1, -1):

        @pl.when(inside(z + way))
        def _():
            greet(((z + way) * ys + y, g, j))

        greeted = greeted + jnp.where(inside(z + way), 1, 0)

    def columns(gain):
        wide = jnp.broadcast_to(gain.reshape(1, 64), (64, 64))
        wide = jnp.concatenate([wide, wide], axis=1)
        wide = jnp.concatenate([wide, wide], axis=0).T
        return jnp.concatenate([wide[0:64]] * (rows // 128), axis=1)

    def per_head(turned, gain):
        many = turned.reshape(turned.shape[0] // 64, 64, rows)
        mean = jnp.mean(many * many, axis=1, keepdims=True)
        return (many * lax.rsqrt(mean + epsilon) * gain[None]).reshape(turned.shape)

    fetches[0].wait()
    x = x_ref[...].astype(jnp.float32)
    scale = lax.rsqrt(jnp.mean(x * x, axis=1, keepdims=True) + epsilon)
    normed_ref[...] = (x * scale * in_gain[...].reshape(1, -1)).astype(jnp.bfloat16)
    fetches[1].wait()
    fetches[2].wait()
    both = jnp.dot(normed_ref[...], wkv_ref[...], preferred_element_type=jnp.float32).T
    turned_keys = per_head(both[0:128], columns(key_gain[...])).astype(jnp.bfloat16)
    turned_values = both[128:256].astype(jnp.bfloat16)
    for n in range(kv_heads):
        kvt_ref[n, 0:64] = turned_keys[n * 64 : (n + 1) * 64]
        kvt_ref[n, 64:128] = turned_values[n * 64 : (n + 1) * 64]
    fetches[3].wait()
    decay_ref[...] = sums_ref[...] * LOG2E

    def far_q_copy(group, pair):
        unit = kv_heads * pair + g
        slot = jnp.minimum(pairs + unit, 2 * pairs - 1)
        return remote(
            query_ref.at[q_lanes(group, pair)], in_q.at[slot],
            q_send.at[group * pairs + pair], q_recv.at[slot], (s_far, group, j),
        )

    def near_q_copy(pair):
        return remote(
            query_ref.at[q_lanes(partner_x, pair)], in_q.at[pair],
            q_send.at[partner_x * pairs + pair], q_recv.at[pair], (s, partner_x, j),
        )

    def q_arrived(slot):
        remote(
            query_ref.at[pl.ds(0, 128)], in_q.at[slot], q_send.at[0], q_recv.at[slot], here
        ).wait_recv()

    def is_given(pair, x_):
        return kv_heads * pair + x_ < given

    def far_sends(act):
        for pair in range(pairs):
            for group in range(kv_heads):

                @pl.when(is_given(pair, g))
                def _():
                    act([far_q_copy(group, pair)])

    def near_sends(act):
        for pair in range(pairs):

            @pl.when(jnp.logical_not(is_given(pair, g)))
            def _():
                act([near_q_copy(pair)])

    def far_decay_copies():
        copies = []
        for x_ in range(kv_heads):
            for n in range(half_count):
                source = decay_ref.at[:, pl.ds((x_ * half_count + n) * rows, rows)]
                at = x_ * half_count + n
                copies.append(
                    remote(
                        source, far_decay.at[x_ * half_count + j], far_send.at[at],
                        far_recv.at[x_ * half_count + j], (s_far, g, n),
                    )
                )
        return copies

    own_block = block_at(s, g, j)
    other_block = block_at(s, partner_x, j)
    member = s * half_count + j

    def side_targets():
        targets = [(None, (s, g, (j + n) % half_count)) for n in range(1, half_count)]
        targets.append((inside(z + 1), ((z + 1) * ys + y, g, j)))
        targets += [(None, (z * ys + (y + n) % ys, g, j)) for n in range(1, ys)]
        return targets

    def each_down(act):
        for z_ in range(zh - 1, -1, -1):

            @pl.when((z_ < z) & (z_ <= zs - 1 - z))
            def _():
                act((ys + half_count - 1 + z_) * each, (z_ * ys + y, g, j))

    def each_side(act):
        for slot, (condition, device) in enumerate(side_targets()):
            if condition is None:
                act(slot * each, device)
            else:

                @pl.when(condition)
                def _():
                    act(slot * each, device)

    def own_copies(base, device):
        return [
            kv_copy(kvt_ref.at[g], own_block, own_send.at[base], device),
            decay_copy(decay_ref, member, own_send.at[base + 1], device),
        ]

    def other_copies(base, device):
        return [kv_copy(kvt_all.at[other_block], other_block, own_send.at[base + 2], device)]

    x_copy = kv_copy(kvt_ref.at[partner_x], own_block, x_send, (s, partner_x, j))
    pl.semaphore_wait(barrier, greeted)
    x_copy.start()
    each_side(lambda base, device: start_all(own_copies(base, device)))

    @pl.when(z <= zh)
    def _():
        each_down(lambda base, device: start_all(own_copies(base, device)))

    fetches[4].wait()
    query_columns = columns(query_gain[...] * (LOG2E * 64 ** (-0.5)))

    for n in range(query_ref.shape[0] // 256):
        at = pl.ds(n * 256, 256)
        turned = jnp.dot(
            normed_ref[...], wq_ref[:, at], preferred_element_type=jnp.float32
        ).T
        query_ref[at] = per_head(turned, query_columns).astype(jnp.bfloat16)

    @pl.when(z > zh)
    def _():
        far_sends(start_all)

    near_sends(start_all)
    kvt_all[own_block] = kvt_ref[g]
    decay_all[member] = decay_ref[...]
    acc_ref[...] = jnp.zeros_like(acc_ref)
    vt_all[:, 64:80] = jnp.ones((sp_count, 16, chunk_rows), jnp.bfloat16)

    def prepare(t, slot, source, pair, decays):
        turned = source
        high = decays.astype(jnp.bfloat16).astype(jnp.float32)
        rest = decays - high
        middle = rest.astype(jnp.bfloat16).astype(jnp.float32)
        rest = rest - middle
        row = lax.broadcasted_iota(jnp.int32, (64, rows), 0)
        for n in range(2):
            head = 2 * pair + n
            lanes = pl.ds(slot * span + n * rows, rows)
            picked = (row == head) | (row == 8 + head) | (row == 16 + head)
            extra = jnp.where(picked, 1.0, 0.0)
            for at, part in ((24, high), (25, middle), (26, rest)):
                extra = jnp.where(row == at, part[n : n + 1], extra)
            qt_ref[t, 0:64, lanes] = turned[n * 64 : (n + 1) * 64]
            qt_ref[t, 64:128, lanes] = extra.astype(jnp.bfloat16)

    def own_decays(pair, x_):
        first = (2 * pair) % local
        at = pl.ds(pl.multiple_of((x_ * half_count + j) * rows, rows), rows)
        return decay_all[s * half_count + (2 * pair) // local, first : first + 2, at]

    def far_decays(slot):
        pair, x_ = slot // kv_heads, slot % kv_heads
        first = (2 * pair) % local
        return far_decay[x_ * half_count + (2 * pair) // local, first : first + 2]

    def work(t, at, lanes, chunk, start, size, step, limit=None):
        at = pl.ds(pl.multiple_of(at, span), lanes)
        q = qt_ref[t, :, at]
        total = acc_ref[t, :, at]
        for b in range(size // step):
            where = pl.ds(pl.multiple_of(start + b * step, step), step)
            scores = jnp.dot(kp_all[chunk, where], q, preferred_element_type=jnp.float32)
            if limit is not None:
                key = lax.broadcasted_iota(jnp.int32, (step, lanes), 0)
                row = lax.broadcasted_iota(jnp.int32, (step, lanes), 1) % rows
                scores = jnp.where(key <= row + limit, scores, -1e30)
            weights = jnp.exp2(scores).astype(jnp.bfloat16)
            total = total + jnp.dot(
                vt_all[chunk, :, where], weights, preferred_element_type=jnp.float32
            )
        acc_ref[t, :, at] = total

    def whole(t, at, lanes, chunk):
        work(t, at, lanes, chunk, 0, chunk_rows, chunk_rows if lanes == span else chunk_rows // 2)

    def diagonal(t, at, lanes, chunk, offset):
        def body(i, carry):
            work(t, at, lanes, chunk, i * span, span, span, offset - i * span)
            return carry

        lax.fori_loop(0, offset // span + 1, body, 0)

    def finished(t, slot):
        out = []
        for n in range(2):
            lanes = pl.ds(slot * span + n * rows, rows)
            out.append(acc_ref[t, 0:64, lanes] / acc_ref[t, 64:65, lanes])
        return jnp.concatenate(out, axis=0).T.astype(jnp.bfloat16)

    def back_copy(slot, pair, device):
        return remote(
            res_ref.at[slot], att_ref.at[:, q_lanes(g, pair)], back_send.at[slot],
            back_recv.at[g * pairs + pair], device,
        )

    def back_arrived(group, pair):
        remote(
            res_ref.at[0], att_ref.at[:, q_lanes(group, pair)], back_send.at[0],
            back_recv.at[group * pairs + pair], here,
        ).wait_recv()

    assert MOVED[0] * pairs // MOVED[1] <= kv_heads

    def kept_groups(first, act):
        @pl.when(first == 0)
        def _():
            act(0, pairs * span)

        @pl.when(first > 0)
        def _():
            act(span, (pairs - 1) * span)

    def taken_groups(act):
        @pl.when(taken == 2)
        def _():
            act(0, 2 * span)

        @pl.when(taken == 1)
        def _():
            act(0, span)

    my_first = kept_from(g)
    partner_first = kept_from(partner_x)
    offset = (g * half_count + j) * rows
    partner_offset = (partner_x * half_count + j) * rows

    kv_copy(kvt_ref.at[g], other_block, x_send, here).wait_recv()
    each_side(lambda base, device: start_all(other_copies(base, device)))

    @pl.when(z <= zh)
    def _():
        each_down(lambda base, device: start_all(other_copies(base, device)))

    @pl.when(z == zh)
    def _():
        far_sends(start_all)

    @pl.when(is_high)
    def _():
        start_all(far_decay_copies())

    for n in range(1, half_count):
        arrived(s, (j + n) % half_count)
    build(s)
    for pair in range(pairs):
        prepare(0, pair, query_ref[q_lanes(g, pair)], pair, own_decays(pair, g))
    def at_step(k):
        return s - jnp.where(y == 0, jnp.where(k == 1, ys, jnp.where(k == ys, 1, k)), k)

    def comes(zo):
        return (z < zh) & (zo > z) & (zo <= zs - 1 - z)

    first_steps = 2 * (zs + 1)
    left = jnp.maximum(s - zs + 1, 0)

    def item(f, carry):
        early = f < first_steps
        late_f = f - first_steps
        k = f // 2
        turn = jnp.where(early, f % 2, jnp.where(late_f < left, 1, 0))
        step = jnp.where(
            early, k - turn, jnp.where(late_f < left, zs + late_f, zs + late_f - left)
        )
        idle = early & (turn == 0) & (k == zs) & (s >= zs)

        @pl.when(early & (turn == 0) & (k > 0))
        def _():
            @pl.when((k == 2) & (z > zh))
            def _():
                each_down(
                    lambda base, device: start_all(
                        own_copies(base, device) + other_copies(base, device)
                    )
                )

            @pl.when(k < zs)
            def _():
                lanes_of(k)

            for here_too, when, duty, zo in (
                (z == 0, 1, late, z + 1), (z == 0, 3, late, z + 2),
                (z > 0, 2, late, z + 1), (z > 0, 4, late_across, z + 1),
            ):

                @pl.when(here_too & (k == when) & comes(zo))
                def _():
                    duty(zo, True)

        @pl.when(early & (turn == 1))
        def _():
            @pl.when(k < zs - 1)
            def _():
                round_of(k + 1, True)

            @pl.when(k == 1)
            def _():
                for n in range(pairs):

                    @pl.when(partner_first <= n)
                    def _():
                        q_arrived(n)
                        prepare(1, n, in_q[n], n, own_decays(n, partner_x))

        kept = jnp.where(turn == 0, my_first, partner_first)
        start = jnp.where(turn == 0, offset, partner_offset)

        @pl.when(step == 0)
        def _():
            kept_groups(kept, lambda at, lanes: diagonal(turn, at, lanes, s, start))

        @pl.when((step > 0) & (step <= s) & jnp.logical_not(idle))
        def _():
            kept_groups(kept, lambda at, lanes: whole(turn, at, lanes, at_step(step)))

        @pl.when((step == s) & (turn == 0) & jnp.logical_not(idle))
        def _():
            for pair in range(1, pairs):
                att_ref[:, q_lanes(g, pair)] = finished(0, pair)

            @pl.when(my_first == 0)
            def _():
                att_ref[:, q_lanes(g, 0)] = finished(0, 0)

        @pl.when((step == s) & (turn == 1))
        def _():
            for n in range(1, pairs):
                res_ref[n] = finished(1, n)
            for n in range(1, pairs):
                back_copy(n, n, (s, partner_x, j)).start()

            @pl.when(partner_first == 0)
            def _():
                res_ref[0] = finished(1, 0)
                back_copy(0, 0, (s, partner_x, j)).start()

        @pl.when(early & (turn == 1) & (k == zs - 1))
        def _():
            round_of(zs, True)

        @pl.when(early & (turn == 1) & (k == zs))
        def _():
            lanes_of(zs)

        return carry

    lax.fori_loop(0, first_steps + 2 * left, item, 0)

    def far_phase():
        for n in range(kv_heads * half_count):
            remote(
                decay_ref.at[:, pl.ds(0, rows)], far_decay.at[n], far_send.at[n],
                far_recv.at[n], here,
            ).wait_recv()

        for n in range(pairs):

            @pl.when(n < taken)
            def _():
                q_arrived(pairs + n)
                prepare(2, n, in_q[pairs + n], n // kv_heads, far_decays(n))

        def zone(zo, carry):
            def body(i, carry):
                chunk = zo * ys + i

                @pl.when(chunk < s_far)
                def _():
                    taken_groups(lambda at, lanes: whole(2, at, lanes, chunk))

                for place, ahead, duty, zl in (
                    (0, 0, late_across, z + 1), (0, 1, late, z + 3), (ys - 1, 1, late_across, z + 2),
                    (0, 2, late_across, z + 3),
                ):

                    @pl.when((z == 0) & (i == place) & (zo == ahead) & comes(zl))
                    def _():
                        duty(zl, True)

                return carry

            lax.fori_loop(0, ys, body, 0)

            @pl.when(comes(zo + 1) & (zo > jnp.where(z == 0, 2, z)))
            def _():
                late(zo + 1, True)
                late_across(zo + 1, True)

            @pl.when(comes(zo + 1))
            def _():
                late_lanes(zo + 1)

            return carry

        lax.fori_loop(0, zs - z, zone, 0)

        def close(n, carry):
            unit_x = n % kv_heads
            diagonal(2, n * span, span, s_far, (unit_x * half_count + j) * rows)
            for m in range(pairs):

                @pl.when(n == m)
                def _():
                    res_ref[pairs + m] = finished(2, m)
                    back_copy(
                        pairs + m, m // kv_heads, (s_far, m % kv_heads, j)
                    ).start()

            return carry

        lax.fori_loop(0, taken, close, 0)

    @pl.when(z < zh)
    def _():
        far_phase()

    fetches[5].wait()
    for pair in range(1, pairs):
        back_arrived(partner_x, pair)

    firsts = [pl.ds(n * width, 128) for n in range(kv_heads)]
    others = [pl.ds(n * width + 128, width - 128) for n in range(kv_heads)]
    quarter = wo_ref.shape[1] // 4

    def output(parts, at):
        rows_in = jnp.concatenate([att_ref[:, part] for part in parts], axis=1)
        weights_in = jnp.concatenate([wo_ref[part, at] for part in parts], axis=0)
        return jnp.dot(rows_in, weights_in, preferred_element_type=jnp.float32)

    for n in range(4):
        at = pl.ds(n * quarter, quarter)
        sum_ref[:, at] = output(others, at)

    @pl.when(my_first > 0)
    def _():
        back_arrived(g, 0)

    back_arrived(partner_x, 0)
    puts = []
    for n in range(4):
        at = pl.ds(n * quarter, quarter)
        done_ref[:, at] = (sum_ref[:, at] + output(firsts, at)).astype(jnp.bfloat16)
        puts.append(pltpu.make_async_copy(done_ref.at[:, at], out_ref.at[:, at], loads.at[n]))
        puts[n].start()
    x_copy.wait_send()
    each_side(
        lambda base, device: drain_all(own_copies(base, device) + other_copies(base, device))
    )

    each_down(
        lambda base, device: drain_all(own_copies(base, device) + other_copies(base, device))
    )

    def drain(k, carry):
        round_of(k, False)
        return carry

    lax.fori_loop(1, zs + 1, drain, 0)

    def drain_late(zo, carry):
        late(zo, False)
        late_across(zo, False)
        return carry

    @pl.when(z < zh)
    def _():
        lax.fori_loop(z + 1, zs - z, drain_late, 0)


    @pl.when(is_high)
    def _():
        far_sends(drain_all)
        drain_all(far_decay_copies())

    near_sends(drain_all)
    for pair in range(pairs):

        @pl.when(partner_first <= pair)
        def _():
            back_copy(pair, pair, (s, partner_x, j)).wait_send()

        @pl.when(pair < taken)
        def _():
            back_copy(
                pairs + pair, pair // kv_heads, (s_far, pair % kv_heads, j)
            ).wait_send()
    for put in puts:
        put.wait()


def lines_of(sp_count):
    ys = 1 << ((sp_count.bit_length() - 1) // 2)
    return sp_count // ys, ys


def stream(
    inputs, in_gain, w_query, w_key, w_value, query_gain, key_gain, decay_sums, w_out, sizes
):
    sp_count, kv_heads, half_count = sizes
    rows, model = inputs.shape
    width = w_query.shape[1]
    heads = width // 64 // kv_heads
    local, chunk_rows = decay_sums.shape
    zs, ys = lines_of(sp_count)
    pairs = heads // 2
    count = sp_count * kv_heads * half_count
    members = sp_count * half_count
    per = 1 + (ys - 1) + (half_count - 1) + (ys - 1) * (half_count - 1)
    each = kv_heads + 1
    vmem = pl.BlockSpec(memory_space=pltpu.VMEM)
    hbm = pl.BlockSpec(memory_space=pltpu.MemorySpace.HBM)
    dma = pltpu.SemaphoreType.DMA
    return pl.pallas_call(
        lambda *refs: stream_kernel(
            *refs, sizes=sizes, lines=(zs, ys), rows=rows, heads=heads
        ),
        out_shape=jax.ShapeDtypeStruct((rows, w_out.shape[1]), jnp.bfloat16),
        in_specs=[hbm, vmem, hbm, hbm, hbm, vmem, vmem, hbm, hbm],
        out_specs=hbm,
        scratch_shapes=[
            pltpu.VMEM((rows, model), jnp.bfloat16),
            pltpu.VMEM((model, 256), jnp.bfloat16),
            pltpu.VMEM(w_query.shape, jnp.bfloat16),
            pltpu.VMEM(decay_sums.shape, jnp.float32),
            pltpu.VMEM(w_out.shape, jnp.bfloat16),
            pltpu.VMEM((rows, model), jnp.bfloat16),
            pltpu.VMEM((kv_heads, 128, rows), jnp.bfloat16),
            pltpu.VMEM((width, rows), jnp.bfloat16),
            pltpu.VMEM((local, chunk_rows), jnp.float32),
            pltpu.VMEM((rows, width), jnp.bfloat16),
            pltpu.VMEM((count, 128, rows), jnp.bfloat16),
            pltpu.VMEM((members, local, chunk_rows), jnp.float32),
            pltpu.VMEM((kv_heads * half_count, local, rows), jnp.float32),
            pltpu.VMEM((2 * pairs, 128, rows), jnp.bfloat16),
            pltpu.VMEM((3, 128, heads * rows), jnp.bfloat16),
            pltpu.VMEM((3, 80, heads * rows), jnp.float32),
            pltpu.VMEM((sp_count, chunk_rows, 128), jnp.bfloat16),
            pltpu.VMEM((sp_count, 80, chunk_rows), jnp.bfloat16),
            pltpu.VMEM((2 * pairs, rows, 128), jnp.bfloat16),
            pltpu.VMEM((rows, w_out.shape[1]), jnp.bfloat16),
            pltpu.VMEM((rows, w_out.shape[1]), jnp.float32),
            dma((6,)),
            dma((count,)), dma((members,)), dma, dma(((ys + half_count + zs // 2) * each,)),
            dma((zs * per * each,)), dma((zs * per * each,)),
            dma((kv_heads * half_count,)), dma((kv_heads * half_count,)),
            dma((2 * pairs,)), dma((2 * pairs,)), dma((2 * pairs,)), dma((2 * pairs,)),
        ],
        compiler_params=pltpu.CompilerParams(
            has_side_effects=True, collective_id=0, vmem_limit_bytes=56 * 1024 * 1024
        ),
        name="stream",
    )(inputs, in_gain, w_query, w_key, w_value, query_gain, key_gain, decay_sums, w_out)


def any_scores(queries, kv_blocks, decays, sizes):
    sp_count, kv_heads, half_count = sizes
    group = lax.axis_index("kv")
    me = (lax.axis_index("sp") * kv_heads + group) * half_count + lax.axis_index("half")
    count = sp_count * kv_heads * half_count
    mirror = [(i, count - 1 - i) for i in range(count)]
    rows = queries.shape[0]
    length = rows * count
    heads = queries.shape[1] // 64 // kv_heads
    width = heads * 64
    members = sp_count * half_count
    key_block = math.gcd(length, KEY_BLOCK)

    def choose(a, b):
        return jnp.where(group == 0, a, b)

    decay_rows = decays.reshape(-1, 128)
    own_q = choose(queries[:, :width], queries[:, width:])
    sent_q = choose(queries[:, width:], queries[:, :width])
    vmem = pl.BlockSpec(memory_space=pltpu.VMEM)
    chips = count // 2
    dma = pltpu.SemaphoreType.DMA
    kv, far_q, decay_all = pl.pallas_call(
        lambda *refs: exchange_kernel(*refs, rows=rows, sizes=sizes),
        out_shape=(
            jax.ShapeDtypeStruct((length, 128), jnp.bfloat16),
            jax.ShapeDtypeStruct((rows, width), jnp.bfloat16),
            jax.ShapeDtypeStruct((members, *decay_rows.shape), jnp.float32),
        ),
        in_specs=[vmem] * 3,
        out_specs=(vmem,) * 3,
        scratch_shapes=[
            dma((2,)), dma((chips,)), dma((count,)), dma((chips,)), dma((members // 2,)),
            dma((members,)), dma((members // 2,)), dma, dma,
        ],
        compiler_params=pltpu.CompilerParams(has_side_effects=True),
        name="exchange",
    )(kv_blocks, sent_q, decay_rows)
    decay_all = decay_all.reshape(sp_count, heads, -1, key_block)
    decay_all = decay_all.transpose(0, 2, 1, 3).reshape(length // key_block, heads, key_block)
    firsts = (me * rows, (count - 1 - me) * rows)
    place = jnp.stack(firsts).astype(jnp.int32)
    row_decay = jnp.stack(
        [
            lax.dynamic_slice(
                decay_all, (first // key_block, 0, first % key_block), (1, heads, rows)
            )[0].T
            for first in firsts
        ]
    )
    attended = attend(place, own_q, far_q, row_decay, decay_all, kv, False)
    back = lax.ppermute(attended[1], ALL, mirror)
    return choose(
        jnp.concatenate([attended[0], back], axis=1), jnp.concatenate([back, attended[0]], axis=1)
    )


def any_program(
    inputs, in_gain, w_query, w_key, w_value, query_gain, key_gain, decay_sums, w_out, sizes
):
    kv_heads = sizes[1]
    head_size = query_gain.shape[0]
    rows = inputs.shape[0]
    all_heads = w_query.shape[1] // head_size

    normed = rms_norm(inputs.astype(jnp.float32), in_gain).astype(jnp.bfloat16)
    keys = rms_norm(
        jnp.dot(normed, w_key, preferred_element_type=jnp.float32).reshape(
            rows, kv_heads, head_size
        ),
        key_gain,
    ).astype(jnp.bfloat16)
    values = (
        jnp.dot(normed, w_value, preferred_element_type=jnp.float32)
        .astype(jnp.bfloat16)
        .reshape(rows, kv_heads, head_size)
    )
    kv_blocks = jnp.concatenate([keys, values], axis=2).transpose(1, 0, 2)
    queries = rms_norm(
        jnp.dot(normed, w_query, preferred_element_type=jnp.float32).reshape(
            rows, all_heads, head_size
        ),
        query_gain * (LOG2E * head_size ** (-0.5)),
    ).astype(jnp.bfloat16).reshape(rows, all_heads * head_size)
    whole = any_scores(queries, kv_blocks, decay_sums.T * LOG2E, sizes)
    return jnp.dot(whole, w_out, preferred_element_type=jnp.float32).astype(jnp.bfloat16)


def per_device(*arrays):
    query_gain, key_gain = arrays[5:7]
    sizes = (lax.axis_size("sp"), lax.axis_size("kv"), lax.axis_size("half"))
    most = jnp.max(query_gain[:, None] * key_gain[None, :])
    bound = query_gain.shape[0] ** 0.5 * LOG2E * most
    return lax.cond(
        bound <= SMALL,
        lambda *given: stream(*given[:7], given[7].T, given[8], sizes),
        lambda *given: any_program(*given, sizes),
        *arrays,
    )


def solution(mesh):
    sp_count, tp_count = mesh.devices.shape
    split = Mesh(mesh.devices.reshape(sp_count, 2, tp_count // 2), ALL)
    placed = (P(ALL, None), P(), P(), P(), P(), P(), P(), P("sp", ("kv", "half")), P())
    return jax.shard_map(
        per_device, mesh=split, in_specs=placed, out_specs=P(ALL, None), check_vma=False
    )
```
